32 devices in a mesh: grp: 2 (over x), sp: 4 (over z), tp: 4 (over y, core).
Axes of the slice: x: 2, y: 2, z: 4, core: 2. Of those that a mesh axis runs over, the one named last changes fastest.
Arguments:
- stream: bfloat16 [4096, 2560], P(None, ('grp', 'sp')), parts along dimension 1, may hold values from -6 to 6
- norm_gain: float32 [2, 4096], replicated, may hold values from 0.1 to 1.9
- value_weight: bfloat16 [2, 2048, 4096], P(None, 'tp'), may hold values from -0.09375 to 0.09375
- gate_weight: bfloat16 [2, 2048, 4096], P(None, 'tp'), may hold values from -0.09375 to 0.09375
- conv_kernel: float32 [2, 2048, 31], P(None, 'tp')
- conv_bias: float32 [2, 2048], P(None, 'tp'), may hold values from -3 to 3
- channel_gain: float32 [2, 2048], P(None, 'tp'), may hold values from 0.1 to 1.9
- channel_bias: float32 [2, 2048], P(None, 'tp'), may hold values from -3 to 3
- out_weight: bfloat16 [2, 4096, 2048], P(None, 'tp'), may hold values from -0.25 to 0.25
Outputs:
- result: bfloat16 [4096, 2560], P('tp', ('grp', 'sp')), parts along dimension 1
The draws below stay inside these ranges and needn't reach their ends.
There are 2 independent parts, one for each index of `grp`. The reference program is written for one: setup_inputs(seed, part) draws one part's arguments, and reference() takes and returns one part's arrays. A program takes and returns all parts, laid end to end along the dimension named above; an argument that names none is the same for every part. Nothing has to cross between parts.
All inputs are finite; a program needn't handle non-finite values.
Results may differ from the reference program's by a relative error of at most 0.012.
Values may be sent and summed in bfloat16 or wider, within the bound.
A program may use at most 128 MiB of HBM per device.

```python
import math
import jax
import jax.numpy as jnp
from jax import lax

D = 4096
C = 2048
K = 31
LAYERS = 2
TOKENS = 1280


def draw_conv_kernel(key, part):
    normal_key, factor_key = jax.random.split(key)
    samples = jax.random.truncated_normal(normal_key, -4.0, 4.0, (LAYERS, C, K), jnp.float32)
    rising = 10.0 ** (jnp.arange(C, dtype=jnp.float32) / (C - 1))
    jitter = jnp.exp(jax.random.uniform(factor_key, (LAYERS, C, 1), jnp.float32, -0.35, 0.35))
    return samples * rising[None, :, None] * jitter * (0.5 / math.sqrt(K))


def steps_of(stream_key, shape, cuts, smallest, top_value):
    factor_of = 1.0
    for position, blocks in cuts:
        heights = jax.random.uniform(jax.random.fold_in(jax.random.fold_in(stream_key, 6), position), (blocks,), jnp.float32, smallest / len(cuts), top_value / len(cuts))
        factor_of = factor_of * jnp.repeat(jnp.exp(heights), shape[position] // blocks).reshape((-1,) + (1,) * (len(shape) - 1 - position))
    return factor_of


def gaussian(rng, shape, scale, most, pieces=(), kind=jnp.bfloat16):
    loudness = steps_of(rng, shape, pieces, -0.22, 0.18) if pieces else 1.0
    entries = jax.random.normal(rng, shape, jnp.float32) * scale * loudness
    return jnp.minimum(jnp.maximum(entries, -most), most).astype(kind)


def setup_inputs(seed: int = 0, part: int = 0) -> dict:
    keys = jax.random.split(jax.random.key(seed), 10)
    own_keys = jax.random.split(jax.random.fold_in(keys[9], part), 10)
    return {
        "stream": gaussian(own_keys[0], (D, TOKENS), 1.0, 6.0, ((1, 4),)),
        "norm_gain": jnp.clip(1.0 + 0.18 * jax.random.normal(keys[1], (LAYERS, D), jnp.float32), 0.1, 1.9),
        "value_weight": gaussian(keys[2], (LAYERS, C, D), D ** -0.5, 0.09375, ((1, 4),)),
        "gate_weight": gaussian(keys[3], (LAYERS, C, D), D ** -0.5, 0.09375, ((1, 4),)),
        "conv_kernel": draw_conv_kernel(jax.random.fold_in(keys[9], 71), part),
        "conv_bias": gaussian(keys[5], (LAYERS, C), 0.5, 3.0, ((1, 4),), jnp.float32),
        "channel_gain": jnp.clip(1.0 + 0.18 * jax.random.normal(keys[6], (LAYERS, C), jnp.float32), 0.1, 1.9),
        "channel_bias": gaussian(keys[7], (LAYERS, C), 0.5, 3.0, ((1, 4),), jnp.float32),
        "out_weight": gaussian(keys[8], (LAYERS, D, C), (C // 4) ** -0.5, 0.25, ((1, 4),)),
    }


epsilon = 1e-06

def depthwise(signal, kernel):
    length = signal.shape[0]
    padded = jnp.pad(signal, ((K - 1, 0), (0, 0)))
    total = jnp.zeros_like(signal)
    for tap in range(K):
        total = total + padded[tap:tap + length] * kernel[:, tap][None, :]
    return total

def reference(stream, norm_gain, value_weight, gate_weight, conv_kernel, conv_bias, channel_gain, channel_bias, out_weight):
    rows = stream.T
    for layer in range(LAYERS):
        current = rows.astype(jnp.float32)
        scaling = lax.rsqrt(lax.optimization_barrier(jnp.mean(current * current, axis=1, keepdims=True)) + epsilon)
        normed = (current * scaling * norm_gain[layer]).astype(jnp.bfloat16)
        value = jnp.dot(normed, value_weight[layer].T, preferred_element_type=jnp.float32)
        gate_part = jnp.dot(normed, gate_weight[layer].T, preferred_element_type=jnp.float32)
        gated = (value * jax.nn.sigmoid(gate_part)).astype(jnp.bfloat16)
        filtered = depthwise(gated.astype(jnp.float32), conv_kernel[layer]) + conv_bias[layer]
        row_mean = lax.optimization_barrier(jnp.mean(filtered, axis=1, keepdims=True))
        centred = filtered - row_mean
        spread = lax.optimization_barrier(jnp.mean(centred * centred, axis=1, keepdims=True))
        activated = jax.nn.silu(centred * lax.rsqrt(spread + epsilon) * channel_gain[layer] + channel_bias[layer]).astype(jnp.bfloat16)
        branch = jnp.dot(activated, out_weight[layer].T, preferred_element_type=jnp.float32)
        rows = (current + branch).astype(jnp.bfloat16)
    return rows.T
```

```python
import functools

import jax
import jax.numpy as jnp
from jax import lax
from jax.experimental import pallas as pl
from jax.experimental.pallas import tpu as pltpu
from jax.sharding import PartitionSpec as P

K = 31
LAYERS = 2


epsilon = 1e-06


def shifted(value, axis, steps):
    count = lax.axis_size(axis)
    initial, last = (max(0, -steps), min(count, count - steps))
    return lax.ppermute(value, axis, [(source, source + steps) for source in range(initial, last)])


def depthwise(signal, kernel):
    out = lax.conv_general_dilated(
        signal[None],
        kernel[:, None, :],
        (1,),
        [(0, 0)],
        dimension_numbers=("NCW", "OIW", "NCW"),
        feature_group_count=kernel.shape[0],
        precision=lax.Precision.HIGHEST,
    )
    return out[0]


def norm_project(whole, gain, weights):
    scaling = lax.rsqrt(jnp.mean(whole * whole, axis=0, keepdims=True) + epsilon)
    normed = (whole * scaling * gain[:, None]).astype(jnp.bfloat16)
    return jnp.dot(weights, normed, preferred_element_type=jnp.float32)


def local(
    stream,
    norm_gain,
    value_weight,
    gate_weight,
    conv_kernel,
    conv_bias,
    channel_gain,
    channel_bias,
    out_weight,
):
    shard_channels = value_weight.shape[1]
    total_channels = shard_channels * lax.axis_size("tp")
    shard_features = out_weight.shape[1]
    tokens_here = stream.shape[1]
    row_start = lax.axis_index("tp") * shard_features
    whole = stream.astype(jnp.float32)
    current = lax.dynamic_slice_in_dim(whole, row_start, shard_features, 0)
    layer_out = stream
    for layer in range(LAYERS):
        both_weights = jnp.concatenate((value_weight[layer], gate_weight[layer]), axis=0)
        if layer == 0:
            projected = norm_project(whole, norm_gain[layer], both_weights)
        else:
            gathered = lax.all_gather(layer_out, "tp", axis=0, tiled=True).astype(jnp.float32)
            projected = norm_project(gathered, norm_gain[layer], both_weights)
        gated = (projected[:shard_channels] * jax.nn.sigmoid(projected[shard_channels:])).astype(
            jnp.bfloat16
        )
        earlier = shifted(gated[:, tokens_here - (K - 1) :], "sp", 1)
        extended = jnp.concatenate((earlier, gated), axis=1).astype(jnp.float32)
        filtered = depthwise(extended, conv_kernel[layer]) + conv_bias[layer][:, None]
        first_sum, square_sum = lax.psum(
            (
                jnp.sum(filtered, axis=0, keepdims=True),
                jnp.sum(filtered * filtered, axis=0, keepdims=True),
            ),
            "tp",
        )
        row_mean = first_sum / total_channels
        centred = filtered - row_mean
        spread = square_sum / total_channels - row_mean * row_mean
        activated = jax.nn.silu(
            centred * lax.rsqrt(spread + epsilon) * channel_gain[layer][:, None]
            + channel_bias[layer][:, None]
        ).astype(jnp.bfloat16)

        def accumulate(total, piece, start, weights=out_weight[layer]):
            weight_cols = lax.dynamic_slice_in_dim(weights, start, piece.shape[0], 1)
            return total + jnp.dot(weight_cols, piece, preferred_element_type=jnp.float32)

        zero_branch = jnp.zeros((shard_features, tokens_here), jnp.float32)
        branch = accumulate(
            zero_branch, lax.all_gather(activated, "tp", axis=0, tiled=True), jnp.int32(0)
        )
        layer_out = (current + branch).astype(jnp.bfloat16)
        current = layer_out.astype(jnp.float32)
    return layer_out


MESH = pl.DeviceIdType.MESH
LANES = 128
SUBLANES = 8
CHUNK = 256
HALO = 32
ROWS = 64
CORES = 2
PIECES = 4


def dot_nt(left, right):
    return lax.dot_general(
        left, right, (((1,), (1,)), ((), ())), preferred_element_type=jnp.float32
    )


def kernel(
    n_tp,
    n_sp,
    split,
    x_hbm,
    gain_hbm,
    taps_hbm,
    bias_hbm,
    chan_gain_hbm,
    chan_bias_hbm,
    wv_ref,
    wg_ref,
    ow_ref,
    out_ref,
    gain_ref,
    raw_taps,
    bias_ref,
    chan,
    wp,
    wo,
    x_in,
    xg,
    ext,
    filt,
    taps,
    norm_squares,
    scale,
    part,
    columns,
    halo_out,
    halo_in,
    stat,
    square,
    cf,
    ag,
    sg,
    accp,
    acco,
    res,
    small_sem,
    x_sem,
    wp_sem,
    wo_sem,
    chan_send,
    chan_recv,
    halo_send,
    halo_recv,
    stat_send,
    stat_recv,
    square_send,
    square_recv,
    y_send,
    y_recv,
    f_send,
    f_recv,
):
    tokens, width = x_in.shape
    chans = wv_ref.shape[1]
    feats = ow_ref.shape[1]
    total_chans = chans * n_tp
    n_y = n_tp // CORES
    piece = width // PIECES
    padded = stat.shape[-1]
    n_a, n_f = chans // CHUNK, feats // CHUNK
    groups = CHUNK // LANES
    spans = (
        ((split, tokens), (0, split)),
        ((split + HALO, tokens), (0, split + HALO)),
    )
    me = lax.axis_index("tp")
    sp = lax.axis_index("sp")
    my_y, core = me // CORES, me % CORES
    sibling = my_y * CORES + (1 - core)

    def tp_id(index):
        return {"tp": index}

    smalls = [
        pltpu.make_async_copy(source, target, small_sem.at[index])
        for index, (source, target) in enumerate(
            (
                (gain_hbm, gain_ref),
                (taps_hbm, raw_taps),
                (bias_hbm, bias_ref),
                (chan_gain_hbm, chan.at[my_y, 0]),
                (chan_bias_hbm, chan.at[my_y, 1]),
            )
        )
    ]

    def x_copy(index):
        cols = pl.ds(index * piece, piece)
        return pltpu.make_async_copy(x_hbm.at[:, cols], x_in.at[:, cols], x_sem.at[index])

    def proj_copies(layer, chunk, index=None):
        rows = pl.ds(chunk * CHUNK, CHUNK)
        cols = slice(None) if index is None else pl.ds(index * piece, piece)
        return [
            pltpu.make_async_copy(
                ref.at[layer, rows, cols],
                wp.at[layer, chunk, pl.ds(half * CHUNK, CHUNK), cols],
                wp_sem.at[layer, chunk, index or 0],
            )
            for half, ref in enumerate((wv_ref, wg_ref))
        ]

    def out_copy(layer):
        return pltpu.make_async_copy(ow_ref.at[layer], wo.at[layer], wo_sem.at[layer])

    smalls[0].start()
    for index in range(PIECES):
        x_copy(index).start()
        for copy in proj_copies(0, 0, index):
            copy.start()
    for copy in smalls[1:]:
        copy.start()
    for layer in range(LAYERS):
        for chunk in range(n_a):
            if layer or chunk:
                for copy in proj_copies(layer, chunk):
                    copy.start()
        out_copy(layer).start()

    barrier = pltpu.get_barrier_semaphore()
    for step in range(1, n_tp):
        pl.semaphore_signal(
            barrier, inc=1, device_id=tp_id(lax.rem(me + step, n_tp)), device_id_type=MESH
        )

    @pl.when(sp > 0)
    def _():
        pl.semaphore_signal(barrier, inc=1, device_id={"sp": sp - 1}, device_id_type=MESH)

    @pl.when(sp < n_sp - 1)
    def _():
        pl.semaphore_signal(barrier, inc=1, device_id={"sp": sp + 1}, device_id_type=MESH)

    part[...] = jnp.zeros(part.shape, jnp.float32)
    columns[...] = jnp.zeros(columns.shape, jnp.float32)

    pending = []

    def remote(source, target, send, recv, device):
        return pltpu.make_async_remote_copy(
            src_ref=source,
            dst_ref=target,
            send_sem=send,
            recv_sem=recv,
            device_id=tp_id(device),
            device_id_type=MESH,
        )

    def launch(copy):
        copy.start()
        pending.append(copy)

    def rows_of(span):
        return pl.ds(span[0], span[1] - span[0])

    def y_peer(step):
        return lax.rem(my_y + step, n_y)

    def y_origin(step):
        return lax.rem(my_y + n_y - step, n_y)

    def y_copy(phase, ref, step, chunk):
        target = y_peer(step) * CORES + core
        return remote(
            ref, ref, y_send.at[phase, step, chunk], y_recv.at[phase, step, chunk], target
        )

    def f_copy(phase, buf, step, chunk, owner, span):
        ref = buf.at[owner, chunk, rows_of(span)]
        return remote(
            ref, ref, f_send.at[phase, step, chunk], f_recv.at[phase, step, chunk], sibling
        )

    def chan_copy(step, slot):
        target = y_peer(step) * CORES + core
        return remote(chan.at[slot], chan.at[slot], chan_send.at[step], chan_recv.at[step], target)

    def prepare(index):
        gains = gain_ref[0:1, index * piece : (index + 1) * piece]

        @pl.loop(0, tokens // ROWS)
        def _(block):
            rows = pl.ds(pl.multiple_of(block * ROWS, ROWS), ROWS)
            squares = jnp.zeros((ROWS, LANES), jnp.float32)
            if index:
                squares = norm_squares[rows, :]
            for lane in range(piece // LANES):
                here = slice(index * piece + lane * LANES, index * piece + (lane + 1) * LANES)
                values = x_in[rows, here].astype(jnp.float32)
                squares = squares + values * values
                xg[rows, here] = (values * gains[:, lane * LANES : (lane + 1) * LANES]).astype(
                    jnp.bfloat16
                )
            norm_squares[rows, :] = squares

    def held(chunk):
        return slice(chunk * 2 * CHUNK, (chunk + 1) * 2 * CHUNK)

    def gate(chunk, first_row, count):
        rows = pl.ds(first_row, count)
        scaling = scale[rows, :]
        start = chunk * 2 * CHUNK
        pieces = []
        for lane in range(groups):
            at = start + lane * LANES
            value = accp[rows, at : at + LANES] * scaling
            gates = accp[rows, at + CHUNK : at + CHUNK + LANES] * scaling
            gated = (value * jax.nn.sigmoid(gates)).astype(jnp.bfloat16)
            ext[chunk * groups + lane, pl.ds(first_row + HALO, count), :] = gated.astype(
                jnp.float32
            )
            pieces.append(gated)
        return pieces

    def gate_rows(chunk, start, stop):
        @pl.loop(0, (stop - start) // HALO)
        def _(block):
            gate(chunk, pl.multiple_of(start + block * HALO, HALO), HALO)

    def halo_copy(layer, chunk):
        return pltpu.make_async_remote_copy(
            src_ref=halo_out.at[layer, chunk],
            dst_ref=halo_in.at[layer, chunk],
            send_sem=halo_send.at[layer, chunk],
            recv_sem=halo_recv.at[layer, chunk],
            device_id={"sp": lax.rem(sp + 1, n_sp)},
            device_id_type=MESH,
        )

    def send_halo(layer, chunk):
        for lane, gated in enumerate(gate(chunk, tokens - HALO, HALO)):
            halo_out[layer, chunk, :, lane * LANES : (lane + 1) * LANES] = gated

        @pl.when(sp < n_sp - 1)
        def _():
            halo_copy(layer, chunk).start()

    def receive_halo(layer, chunk):
        @pl.when(sp > 0)
        def _():
            halo_copy(layer, chunk).wait_recv()
            for lane in range(groups):
                ext[chunk * groups + lane, :HALO, :] = halo_in[
                    layer, chunk, :, lane * LANES : (lane + 1) * LANES
                ].astype(jnp.float32)

        @pl.when(sp == 0)
        def _():
            for lane in range(groups):
                ext[chunk * groups + lane, :HALO, :] = jnp.zeros((HALO, LANES), jnp.float32)

    def convolve(layer, half, chunk, start, stop):
        base = spans[layer][half][0]
        blocks = []
        while start < stop:
            count = min(ROWS, stop - start)
            blocks.append((start, count))
            start += count

        @pl.loop(chunk * groups, (chunk + 1) * groups)
        def _(lane):
            here = pl.ds(pl.multiple_of(lane * LANES, LANES), LANES)
            bias = bias_ref[layer : layer + 1, here]
            for first_row, count in blocks:
                tiles = count // SUBLANES
                sums = [jnp.broadcast_to(bias, (SUBLANES, LANES))] * tiles
                for residue in range(SUBLANES):
                    begin = first_row + HALO - K + 1 + residue
                    held_taps = range(residue, K, SUBLANES)
                    weights = [taps[layer, tap : tap + 1, here] for tap in held_taps]
                    for index in range(tiles + len(weights) - 1):
                        at = begin + index * SUBLANES
                        window = ext[lane, at : at + SUBLANES, :]
                        for step, weight in enumerate(weights):
                            tile = index - step
                            if 0 <= tile < tiles:
                                sums[tile] = sums[tile] + window * weight
                total = jnp.concatenate(sums, axis=0)
                filt[first_row : first_row + count, here] = total
                inner = slice(first_row - base, first_row - base + count)
                part[half, chunk, 0, inner, :] += total
                part[half, chunk, 1, inner, :] += total * total

    lane_index = lax.broadcasted_iota(jnp.int32, (HALO, LANES), 1)

    def centre(layer, half, chunk):
        start, stop = spans[layer][half]

        @pl.loop(0, (stop - start) // HALO)
        def _(block):
            inner = pl.ds(pl.multiple_of(block * HALO, HALO), HALO)
            rows = pl.ds(pl.multiple_of(start + block * HALO, HALO), HALO)
            mean = jnp.sum(part[half, chunk, 0, inner, :], axis=1, keepdims=True) / CHUNK
            squares = jnp.sum(part[half, chunk, 1, inner, :], axis=1, keepdims=True)
            for lane in range(groups):
                at = chunk * CHUNK + lane * LANES
                cf[layer, my_y, chunk, rows, lane * LANES : (lane + 1) * LANES] = (
                    filt[rows, at : at + LANES] - mean
                ).astype(jnp.bfloat16)
            packed = jnp.where(
                lane_index == chunk, mean, jnp.where(lane_index == n_a + chunk, squares, 0.0)
            )
            if chunk:
                packed = packed + columns[half, inner, :]
            columns[half, inner, :] = packed

    def send_centred(layer, half, phase, chunk):
        ref = cf.at[layer, my_y, chunk, rows_of(spans[layer][half])]
        for step in range(1, n_y):
            launch(y_copy(phase, ref, step, chunk))

    def stat_copy(layer, half, step, owner, target):
        ref = stat.at[layer, half, owner]
        index = layer * 2 + half
        return remote(ref, ref, stat_send.at[index, step], stat_recv.at[index, step], target)

    def send_stats(layer, half):
        stat[layer, half, me] = jnp.transpose(columns[half])[:SUBLANES]
        for step in range(1, n_tp):
            launch(stat_copy(layer, half, step, me, lax.rem(me + step, n_tp)))

    def to_columns(rows):
        fill = jnp.zeros((LANES - rows.shape[0], padded), jnp.float32)
        return jnp.transpose(jnp.concatenate((rows, fill), axis=0))

    def settle(layer, half):
        for step in range(1, n_tp):
            origin = lax.rem(me + n_tp - step, n_tp)
            stat_copy(layer, half, step, origin, origin).wait_recv()
        totals = jnp.sum(stat[layer, half], axis=0)
        mean_row = jnp.sum(totals[:n_a], axis=0, keepdims=True) * CHUNK / total_chans
        square_row = jnp.sum(totals[n_a : 2 * n_a], axis=0, keepdims=True) / total_chans
        rstd_row = lax.rsqrt(square_row - mean_row * mean_row + epsilon)
        rows = [rstd_row]
        for step in range(n_y):
            means = stat[layer, half, y_origin(step) * CORES + core]
            rows.append((means[:n_a] - mean_row) * rstd_row)
        columns[half] = to_columns(jnp.concatenate(rows, axis=0))

    def activate(layer, half, step, chunk):
        start, stop = spans[layer][half]
        origin = y_origin(step)
        owner = origin * CORES + core

        @pl.loop(0, (stop - start) // HALO)
        def _(block):
            inner = pl.ds(pl.multiple_of(block * HALO, HALO), HALO)
            rows = pl.ds(pl.multiple_of(start + block * HALO, HALO), HALO)
            at = 1 + step * n_a + chunk
            rstd = jnp.broadcast_to(columns[half, inner, 0:1], (HALO, LANES))
            shift = jnp.broadcast_to(columns[half, inner, at : at + 1], (HALO, LANES))
            for lane in range(groups):
                cols = slice(lane * LANES, (lane + 1) * LANES)
                here = slice(chunk * CHUNK + lane * LANES, chunk * CHUNK + (lane + 1) * LANES)
                values = cf[layer, origin, chunk, rows, cols].astype(jnp.float32) * rstd + shift
                values = (
                    values * chan[origin, 0, layer : layer + 1, here]
                    + chan[origin, 1, layer : layer + 1, here]
                )
                ag[layer, owner, chunk, rows, cols] = jax.nn.silu(values).astype(jnp.bfloat16)

    def own_activated(layer, half, phase):
        for chunk in range(n_a):
            activate(layer, half, 0, chunk)
            launch(f_copy(phase, ag.at[layer], 0, chunk, me, spans[layer][half]))

    def arrived_activated(layer, half, phase):
        for step in range(1, n_y):
            owner = y_origin(step) * CORES + core
            for chunk in range(n_a):
                ref = cf.at[layer, y_origin(step), chunk, rows_of(spans[layer][half])]
                y_copy(phase, ref, step, chunk).wait_recv()
                activate(layer, half, step, chunk)
                launch(f_copy(phase, ag.at[layer], step, chunk, owner, spans[layer][half]))

    def mix(layer, half, owner, first=False):
        rows = slice(*spans[layer][half])
        if not first:
            total = acco[rows, :]
        elif layer == 0:
            total = x_in[rows, pl.ds(pl.multiple_of(me * feats, LANES), feats)].astype(jnp.float32)
        else:
            total = res[rows, :]
        for chunk in range(n_a):
            start = pl.multiple_of(owner * chans + chunk * CHUNK, LANES)
            total = total + dot_nt(
                ag[layer, owner, chunk, rows, :], wo[layer, :, pl.ds(start, CHUNK)]
            )
        acco[rows, :] = total

    def mix_own(layer, half):
        mix(layer, half, me, True)

    def mix_arrived(layer, half):
        for step in range(1, n_y):
            mix(layer, half, y_origin(step) * CORES + core)

    def mix_sibling(layer, half, phase):
        for chunk in range(n_a):
            f_copy(phase, ag.at[layer], 0, chunk, sibling, spans[layer][half]).wait_recv()
        mix(layer, half, sibling)

    def mix_relayed(layer, half, phase):
        for step in range(1, n_y):
            owner = y_origin(step) * CORES + 1 - core
            for chunk in range(n_a):
                f_copy(phase, ag.at[layer], step, chunk, owner, spans[layer][half]).wait_recv()
            mix(layer, half, owner)

    def square_copy(half, step, owner, target):
        ref = square.at[half, owner]
        return remote(ref, ref, square_send.at[half, step], square_recv.at[half, step], target)

    def send_stream(half):
        span = spans[0][half]
        rows = slice(*span)
        squares = jnp.zeros((span[1] - span[0], LANES), jnp.float32)
        for chunk in range(n_f):
            first = pl.multiple_of(me * feats + chunk * CHUNK, LANES)
            gains = gain_ref[1:2, pl.ds(first, CHUNK)]
            for lane in range(groups):
                cols = slice(lane * LANES, (lane + 1) * LANES)
                here = slice(chunk * CHUNK + lane * LANES, chunk * CHUNK + (lane + 1) * LANES)
                rounded = acco[rows, here].astype(jnp.bfloat16).astype(jnp.float32)
                sg[me, chunk, rows, cols] = (rounded * gains[:, cols]).astype(jnp.bfloat16)
                res[rows, here] = rounded
                squares = squares + rounded * rounded
            ref = sg.at[me, chunk, rows_of(span)]
            for step in range(1, n_y):
                launch(y_copy(2 + half, ref, step, chunk))
            launch(f_copy(2 + half, sg, 0, chunk, me, span))
        norm_squares[rows, :] = squares

    def send_squares(half):
        span = spans[0][half]
        count = span[1] - span[0]
        squares = norm_squares[slice(*span), :]
        if count < padded:
            fill = jnp.zeros((padded - count, LANES), jnp.float32)
            squares = jnp.concatenate((squares, fill), axis=0)
        row = jnp.sum(jnp.transpose(squares), axis=0, keepdims=True)
        square[half, me] = jnp.broadcast_to(row, (SUBLANES, padded))
        for step in range(1, n_tp):
            launch(square_copy(half, step, me, lax.rem(me + step, n_tp)))

    def rescale(half):
        for step in range(1, n_tp):
            origin = lax.rem(me + n_tp - step, n_tp)
            square_copy(half, step, origin, origin).wait_recv()
        totals = jnp.sum(square[half], axis=0)[0:1] / width
        start, stop = spans[0][half]
        spread = jnp.transpose(
            jnp.broadcast_to(lax.rsqrt(totals + epsilon), (LANES, padded))
        )
        scale[start:stop, :] = spread[: stop - start]

    def project(half, owner, chunks, first):
        rows = slice(*spans[0][half])
        for block in range(n_a):
            total = None if first else accp[rows, held(block)]
            for chunk in chunks:
                start = pl.multiple_of(owner * feats + chunk * CHUNK, LANES)
                product = dot_nt(
                    sg[owner, chunk, rows, :], wp[1, block, :, pl.ds(start, CHUNK)]
                )
                total = product if total is None else total + product
            accp[rows, held(block)] = total

    def near_stream(half):
        project(half, me, range(n_f), True)
        for chunk in range(n_f):
            f_copy(2 + half, sg, 0, chunk, sibling, spans[0][half]).wait_recv()
        project(half, sibling, range(n_f), False)

    def arrive_stream(half, chunk):
        for step in range(1, n_y):
            origin = y_origin(step)
            owner = origin * CORES + core
            ref = sg.at[owner, chunk, rows_of(spans[0][half])]
            y_copy(2 + half, ref, step, chunk).wait_recv()
            launch(f_copy(2 + half, sg, step, chunk, owner, spans[0][half]))
            project(half, owner, (chunk,), False)

    def relayed_stream(half, chunk):
        for step in range(1, n_y):
            owner = y_origin(step) * CORES + 1 - core
            f_copy(2 + half, sg, step, chunk, owner, spans[0][half]).wait_recv()
            project(half, owner, (chunk,), False)

    def far_stream(half, chunks):
        for chunk in chunks:
            arrive_stream(half, chunk)
            if chunk:
                relayed_stream(half, chunk - 1)

    smalls[0].wait()
    for index in range(PIECES):
        cols = slice(index * piece, (index + 1) * piece)
        x_copy(index).wait()
        prepare(index)
        for copy in proj_copies(0, 0, index):
            copy.wait()
        product = dot_nt(xg[:, cols], wp[0, 0, :, cols])
        if index:
            accp[:, held(0)] += product
        else:
            accp[:, held(0)] = product

    @pl.loop(0, tokens // ROWS)
    def _(block):
        rows = pl.ds(pl.multiple_of(block * ROWS, ROWS), ROWS)
        scaling = lax.rsqrt(jnp.sum(norm_squares[rows, :], axis=1, keepdims=True) / width + epsilon)
        scale[rows, :] = jnp.broadcast_to(scaling, (ROWS, LANES))

    for copy in smalls[1:]:
        copy.wait()
    for layer in range(LAYERS):
        taps[layer] = raw_taps[:, layer, :]
    pl.semaphore_wait(
        barrier,
        n_tp - 1 + jnp.where(sp > 0, 1, 0) + jnp.where(sp < n_sp - 1, 1, 0),
    )
    for step in range(1, n_y):
        launch(chan_copy(step, my_y))

    for chunk in range(n_a):
        if chunk:
            for copy in proj_copies(0, chunk):
                copy.wait()
            accp[:, held(chunk)] = dot_nt(xg[...], wp[0, chunk])
        send_halo(0, chunk)
        gate_rows(chunk, 0, tokens - HALO)
        convolve(0, 0, chunk, *spans[0][0])
        centre(0, 0, chunk)
        send_centred(0, 0, 0, chunk)
    send_stats(0, 0)
    for chunk in range(n_a):
        convolve(0, 1, chunk, ROWS, spans[0][1][1])
        receive_halo(0, chunk)
        convolve(0, 1, chunk, 0, ROWS)
        centre(0, 1, chunk)
        send_centred(0, 1, 1, chunk)
    send_stats(0, 1)
    for step in range(1, n_y):
        chan_copy(step, y_origin(step)).wait_recv()
    settle(0, 0)
    own_activated(0, 0, 0)
    out_copy(0).wait()
    mix_own(0, 0)
    arrived_activated(0, 0, 0)
    mix_arrived(0, 0)
    mix_sibling(0, 0, 0)
    settle(0, 1)
    own_activated(0, 1, 1)
    mix_relayed(0, 0, 0)
    send_stream(0)
    send_squares(0)
    mix_own(0, 1)
    arrived_activated(0, 1, 1)
    mix_arrived(0, 1)
    mix_sibling(0, 1, 1)
    mix_relayed(0, 1, 1)
    send_stream(1)
    send_squares(1)
    part[...] = jnp.zeros(part.shape, jnp.float32)
    for chunk in range(n_a):
        for copy in proj_copies(1, chunk):
            copy.wait()
    near_stream(0)
    far_stream(0, range(n_f))
    near_stream(1)
    relayed_stream(0, n_f - 1)
    rescale(0)
    for chunk in range(n_a):
        send_halo(1, chunk)
        gate_rows(chunk, split, tokens - HALO)
        convolve(1, 0, chunk, *spans[1][0])
        centre(1, 0, chunk)
        send_centred(1, 0, 4, chunk)
    send_stats(1, 0)
    far_stream(1, range(n_f // 2))
    settle(1, 0)
    own_activated(1, 0, 4)
    far_stream(1, range(n_f // 2, n_f))
    relayed_stream(1, n_f - 1)
    rescale(1)
    for chunk in range(n_a):
        gate_rows(chunk, 0, split)
        convolve(1, 1, chunk, HALO, spans[1][1][1])
        receive_halo(1, chunk)
        convolve(1, 1, chunk, 0, HALO)
        centre(1, 1, chunk)
        send_centred(1, 1, 5, chunk)
    send_stats(1, 1)
    out_copy(1).wait()
    mix_own(1, 0)
    mix_sibling(1, 0, 4)
    arrived_activated(1, 0, 4)
    mix_arrived(1, 0)
    settle(1, 1)
    own_activated(1, 1, 5)
    mix_own(1, 1)
    mix_relayed(1, 0, 4)
    mix_sibling(1, 1, 5)
    arrived_activated(1, 1, 5)
    mix_arrived(1, 1)
    mix_relayed(1, 1, 5)
    out_ref[...] = acco[...].astype(jnp.bfloat16)

    @pl.when(sp < n_sp - 1)
    def _():
        for layer in range(LAYERS):
            for chunk in range(n_a):
                halo_copy(layer, chunk).wait_send()

    for copy in pending:
        copy.wait_send()


def fused(mesh, stream, norm_gain, value_weight, gate_weight, conv_kernel, conv_bias,
          channel_gain, channel_bias, out_weight):
    n_tp, n_sp = mesh.shape["tp"], mesh.shape["sp"]
    width, tokens = stream.shape
    chans, feats = value_weight.shape[1], out_weight.shape[1]
    split = (tokens // 2 - HALO) // HALO * HALO
    n_y = n_tp // CORES
    n_a, n_f = chans // CHUNK, feats // CHUNK
    fits = (
        n_tp % CORES == 0
        and chans % CHUNK == 0
        and feats % CHUNK == 0
        and width % (PIECES * CHUNK) == 0
        and tokens % ROWS == 0
        and split % ROWS == 0
        and tokens >= 4 * ROWS
        and LAYERS == 2
        and n_tp <= 8
        and 2 * n_a <= SUBLANES
        and 1 + n_y * n_a <= LANES
    )
    if not fits:
        return local(stream, norm_gain, value_weight, gate_weight, conv_kernel, conv_bias,
                     channel_gain, channel_bias, out_weight)
    padded = -(-(tokens - split) // LANES) * LANES
    most = max(n_a, n_f)
    f32, bf16 = jnp.float32, jnp.bfloat16
    dma = pltpu.SemaphoreType.DMA
    out = pl.pallas_call(
        functools.partial(kernel, n_tp, n_sp, split),
        out_shape=jax.ShapeDtypeStruct((tokens, feats), bf16),
        in_specs=[pl.BlockSpec(memory_space=pl.ANY)] * 9,
        out_specs=pl.BlockSpec(memory_space=pltpu.VMEM),
        scratch_shapes=[
            pltpu.VMEM((LAYERS, width), f32),
            pltpu.VMEM((K, LAYERS, chans), f32),
            pltpu.VMEM((LAYERS, chans), f32),
            pltpu.VMEM((n_y, 2, LAYERS, chans), f32),
            pltpu.VMEM((LAYERS, n_a, 2 * CHUNK, width), bf16),
            pltpu.VMEM((LAYERS, feats, chans * n_tp), bf16),
            pltpu.VMEM((tokens, width), bf16),
            pltpu.VMEM((tokens, width), bf16),
            pltpu.VMEM((chans // LANES, HALO + tokens, LANES), f32),
            pltpu.VMEM((tokens, chans), f32),
            pltpu.VMEM((LAYERS, K, chans), f32),
            pltpu.VMEM((tokens, LANES), f32),
            pltpu.VMEM((tokens, LANES), f32),
            pltpu.VMEM((2, n_a, 2, padded, LANES), f32),
            pltpu.VMEM((2, padded, LANES), f32),
            pltpu.VMEM((LAYERS, n_a, HALO, CHUNK), bf16),
            pltpu.VMEM((LAYERS, n_a, HALO, CHUNK), bf16),
            pltpu.VMEM((LAYERS, 2, n_tp, SUBLANES, padded), f32),
            pltpu.VMEM((2, n_tp, SUBLANES, padded), f32),
            pltpu.VMEM((LAYERS, n_y, n_a, tokens, CHUNK), bf16),
            pltpu.VMEM((LAYERS, n_tp, n_a, tokens, CHUNK), bf16),
            pltpu.VMEM((n_tp, n_f, tokens, CHUNK), bf16),
            pltpu.VMEM((tokens, 2 * chans), f32),
            pltpu.VMEM((tokens, feats), f32),
            pltpu.VMEM((tokens, feats), f32),
            dma((5,)),
            dma((PIECES,)),
            dma((LAYERS, n_a, PIECES)),
            dma((LAYERS,)),
            dma((n_y,)),
            dma((n_y,)),
            dma((LAYERS, n_a)),
            dma((LAYERS, n_a)),
            dma((LAYERS * 2, n_tp)),
            dma((LAYERS * 2, n_tp)),
            dma((2, n_tp)),
            dma((2, n_tp)),
            dma((6, n_y, most)),
            dma((6, n_y, most)),
            dma((6, n_y, most)),
            dma((6, n_y, most)),
        ],
        compiler_params=pltpu.CompilerParams(
            collective_id=0, has_side_effects=True, vmem_limit_bytes=60 * 1024 * 1024
        ),
    )(stream.T, norm_gain, jnp.transpose(conv_kernel, (2, 0, 1)), conv_bias, channel_gain, channel_bias,
       value_weight, gate_weight, out_weight)
    return out.T


def solution(mesh):
    placed = (
        P(None, ("grp", "sp")),
        P(),
        P(None, "tp", None),
        P(None, "tp", None),
        P(None, "tp", None),
        P(None, "tp"),
        P(None, "tp"),
        P(None, "tp"),
        P(None, "tp", None),
    )
    return jax.shard_map(
        functools.partial(fused, mesh), mesh=mesh, in_specs=placed, out_specs=P("tp", ("grp", "sp")), check_vma=False
    )
```

```python
import functools

import jax
import jax.numpy as jnp
from jax import lax
from jax.experimental import pallas as pl
from jax.experimental.pallas import tpu as pltpu
from jax.sharding import PartitionSpec as P

K = 31
LAYERS = 2


epsilon = 1e-06


def shifted(value, axis, steps):
    count = lax.axis_size(axis)
    initial, last = (max(0, -steps), min(count, count - steps))
    return lax.ppermute(value, axis, [(source, source + steps) for source in range(initial, last)])


def depthwise(signal, kernel):
    out = lax.conv_general_dilated(
        signal[None],
        kernel[:, None, :],
        (1,),
        [(0, 0)],
        dimension_numbers=("NCW", "OIW", "NCW"),
        feature_group_count=kernel.shape[0],
        precision=lax.Precision.HIGHEST,
    )
    return out[0]


def norm_project(whole, gain, weights):
    scaling = lax.rsqrt(jnp.mean(whole * whole, axis=0, keepdims=True) + epsilon)
    normed = (whole * scaling * gain[:, None]).astype(jnp.bfloat16)
    return jnp.dot(weights, normed, preferred_element_type=jnp.float32)


def local(
    stream,
    norm_gain,
    value_weight,
    gate_weight,
    conv_kernel,
    conv_bias,
    channel_gain,
    channel_bias,
    out_weight,
):
    shard_channels = value_weight.shape[1]
    total_channels = shard_channels * lax.axis_size("tp")
    shard_features = out_weight.shape[1]
    tokens_here = stream.shape[1]
    row_start = lax.axis_index("tp") * shard_features
    whole = stream.astype(jnp.float32)
    current = lax.dynamic_slice_in_dim(whole, row_start, shard_features, 0)
    layer_out = stream
    for layer in range(LAYERS):
        both_weights = jnp.concatenate((value_weight[layer], gate_weight[layer]), axis=0)
        if layer == 0:
            projected = norm_project(whole, norm_gain[layer], both_weights)
        else:
            gathered = lax.all_gather(layer_out, "tp", axis=0, tiled=True).astype(jnp.float32)
            projected = norm_project(gathered, norm_gain[layer], both_weights)
        gated = (projected[:shard_channels] * jax.nn.sigmoid(projected[shard_channels:])).astype(
            jnp.bfloat16
        )
        earlier = shifted(gated[:, tokens_here - (K - 1) :], "sp", 1)
        extended = jnp.concatenate((earlier, gated), axis=1).astype(jnp.float32)
        filtered = depthwise(extended, conv_kernel[layer]) + conv_bias[layer][:, None]
        first_sum, square_sum = lax.psum(
            (
                jnp.sum(filtered, axis=0, keepdims=True),
                jnp.sum(filtered * filtered, axis=0, keepdims=True),
            ),
            "tp",
        )
        row_mean = first_sum / total_channels
        centred = filtered - row_mean
        spread = square_sum / total_channels - row_mean * row_mean
        activated = jax.nn.silu(
            centred * lax.rsqrt(spread + epsilon) * channel_gain[layer][:, None]
            + channel_bias[layer][:, None]
        ).astype(jnp.bfloat16)

        def accumulate(total, piece, start, weights=out_weight[layer]):
            weight_cols = lax.dynamic_slice_in_dim(weights, start, piece.shape[0], 1)
            return total + jnp.dot(weight_cols, piece, preferred_element_type=jnp.float32)

        zero_branch = jnp.zeros((shard_features, tokens_here), jnp.float32)
        branch = accumulate(
            zero_branch, lax.all_gather(activated, "tp", axis=0, tiled=True), jnp.int32(0)
        )
        layer_out = (current + branch).astype(jnp.bfloat16)
        current = layer_out.astype(jnp.float32)
    return layer_out


MESH = pl.DeviceIdType.MESH
LANES = 128
SUBLANES = 8
CHUNK = 256
HALO = 32
ROWS = 64
CORES = 2
PIECES = 4


def dot_nt(left, right):
    return lax.dot_general(
        left, right, (((1,), (1,)), ((), ())), preferred_element_type=jnp.float32
    )


def kernel(
    n_tp,
    n_sp,
    split,
    x_hbm,
    gain_hbm,
    taps_hbm,
    bias_hbm,
    chan_gain_hbm,
    chan_bias_hbm,
    wv_ref,
    wg_ref,
    ow_ref,
    out_ref,
    gain_ref,
    raw_taps,
    bias_ref,
    chan,
    wp,
    wo,
    x_in,
    xg,
    ext,
    filt,
    taps,
    norm_squares,
    scale,
    part,
    columns,
    halo_out,
    halo_in,
    stat,
    square,
    cf,
    ag,
    sg,
    accp,
    acco,
    res,
    small_sem,
    x_sem,
    wp_sem,
    wo_sem,
    chan_send,
    chan_recv,
    halo_send,
    halo_recv,
    stat_send,
    stat_recv,
    square_send,
    square_recv,
    y_send,
    y_recv,
    f_send,
    f_recv,
):
    tokens, width = x_in.shape
    chans = wv_ref.shape[1]
    feats = ow_ref.shape[1]
    total_chans = chans * n_tp
    n_y = n_tp // CORES
    piece = width // PIECES
    padded = stat.shape[-1]
    n_a, n_f = chans // CHUNK, feats // CHUNK
    groups = CHUNK // LANES
    spans = (
        ((split, tokens), (0, split)),
        ((split + HALO, tokens), (0, split + HALO)),
    )
    me = lax.axis_index("tp")
    sp = lax.axis_index("sp")
    my_y, core = me // CORES, me % CORES
    sibling = my_y * CORES + (1 - core)

    def tp_id(index):
        return {"tp": index}

    smalls = [
        pltpu.make_async_copy(source, target, small_sem.at[index])
        for index, (source, target) in enumerate(
            (
                (gain_hbm, gain_ref),
                (taps_hbm, raw_taps),
                (bias_hbm, bias_ref),
                (chan_gain_hbm, chan.at[my_y, 0]),
                (chan_bias_hbm, chan.at[my_y, 1]),
            )
        )
    ]

    def x_copy(index):
        cols = pl.ds(index * piece, piece)
        return pltpu.make_async_copy(x_hbm.at[:, cols], x_in.at[:, cols], x_sem.at[index])

    def proj_copies(layer, chunk, index=None):
        rows = pl.ds(chunk * CHUNK, CHUNK)
        cols = slice(None) if index is None else pl.ds(index * piece, piece)
        return [
            pltpu.make_async_copy(
                ref.at[layer, rows, cols],
                wp.at[layer, chunk, pl.ds(half * CHUNK, CHUNK), cols],
                wp_sem.at[layer, chunk, index or 0],
            )
            for half, ref in enumerate((wv_ref, wg_ref))
        ]

    def out_copy(layer):
        return pltpu.make_async_copy(ow_ref.at[layer], wo.at[layer], wo_sem.at[layer])

    smalls[0].start()
    for index in range(PIECES):
        x_copy(index).start()
        for copy in proj_copies(0, 0, index):
            copy.start()
    for copy in smalls[1:]:
        copy.start()

    barrier = pltpu.get_barrier_semaphore()
    for step in range(1, n_tp):
        pl.semaphore_signal(
            barrier, inc=1, device_id=tp_id(lax.rem(me + step, n_tp)), device_id_type=MESH
        )

    @pl.when(sp > 0)
    def _():
        pl.semaphore_signal(barrier, inc=1, device_id={"sp": sp - 1}, device_id_type=MESH)

    @pl.when(sp < n_sp - 1)
    def _():
        pl.semaphore_signal(barrier, inc=1, device_id={"sp": sp + 1}, device_id_type=MESH)

    part[...] = jnp.zeros(part.shape, jnp.float32)
    columns[...] = jnp.zeros(columns.shape, jnp.float32)

    pending = []

    def remote(source, target, send, recv, device):
        return pltpu.make_async_remote_copy(
            src_ref=source,
            dst_ref=target,
            send_sem=send,
            recv_sem=recv,
            device_id=tp_id(device),
            device_id_type=MESH,
        )

    def launch(copy):
        copy.start()
        pending.append(copy)

    def rows_of(span):
        return pl.ds(span[0], span[1] - span[0])

    def y_peer(step):
        return lax.rem(my_y + step, n_y)

    def y_origin(step):
        return lax.rem(my_y + n_y - step, n_y)

    def y_copy(phase, ref, step, chunk):
        target = y_peer(step) * CORES + core
        return remote(
            ref, ref, y_send.at[phase, step, chunk], y_recv.at[phase, step, chunk], target
        )

    def f_copy(phase, buf, step, chunk, owner, span):
        ref = buf.at[owner, chunk, rows_of(span)]
        return remote(
            ref, ref, f_send.at[phase, step, chunk], f_recv.at[phase, step, chunk], sibling
        )

    def chan_copy(step, slot):
        target = y_peer(step) * CORES + core
        return remote(chan.at[slot], chan.at[slot], chan_send.at[step], chan_recv.at[step], target)

    def prepare(index):
        gains = gain_ref[0:1, index * piece : (index + 1) * piece]

        @pl.loop(0, tokens // ROWS)
        def _(block):
            rows = pl.ds(pl.multiple_of(block * ROWS, ROWS), ROWS)
            squares = jnp.zeros((ROWS, LANES), jnp.float32)
            if index:
                squares = norm_squares[rows, :]
            for lane in range(piece // LANES):
                here = slice(index * piece + lane * LANES, index * piece + (lane + 1) * LANES)
                values = x_in[rows, here].astype(jnp.float32)
                squares = squares + values * values
                xg[rows, here] = (values * gains[:, lane * LANES : (lane + 1) * LANES]).astype(
                    jnp.bfloat16
                )
            norm_squares[rows, :] = squares

    def held(chunk):
        return slice(chunk * 2 * CHUNK, (chunk + 1) * 2 * CHUNK)

    def gate(chunk, first_row, count):
        rows = pl.ds(first_row, count)
        halved = scale[rows, :]
        start = chunk * 2 * CHUNK
        pieces = []
        for lane in range(groups):
            at = start + lane * LANES
            value = accp[rows, at : at + LANES] * halved
            gates = accp[rows, at + CHUNK : at + CHUNK + LANES] * halved
            gated = (value + value * jnp.tanh(gates)).astype(jnp.bfloat16)
            ext[chunk * groups + lane, pl.ds(first_row + HALO, count), :] = gated.astype(
                jnp.float32
            )
            pieces.append(gated)
        return pieces

    def gate_rows(chunk, start, stop):
        @pl.loop(0, (stop - start) // HALO)
        def _(block):
            gate(chunk, pl.multiple_of(start + block * HALO, HALO), HALO)

    def halo_copy(layer, chunk):
        return pltpu.make_async_remote_copy(
            src_ref=halo_out.at[layer, chunk],
            dst_ref=halo_in.at[layer, chunk],
            send_sem=halo_send.at[layer, chunk],
            recv_sem=halo_recv.at[layer, chunk],
            device_id={"sp": lax.rem(sp + 1, n_sp)},
            device_id_type=MESH,
        )

    def send_halo(layer, chunk):
        for lane, gated in enumerate(gate(chunk, tokens - HALO, HALO)):
            halo_out[layer, chunk, :, lane * LANES : (lane + 1) * LANES] = gated

        @pl.when(sp < n_sp - 1)
        def _():
            halo_copy(layer, chunk).start()

    def receive_halo(layer, chunk):
        @pl.when(sp > 0)
        def _():
            halo_copy(layer, chunk).wait_recv()
            for lane in range(groups):
                ext[chunk * groups + lane, :HALO, :] = halo_in[
                    layer, chunk, :, lane * LANES : (lane + 1) * LANES
                ].astype(jnp.float32)

        @pl.when(sp == 0)
        def _():
            for lane in range(groups):
                ext[chunk * groups + lane, :HALO, :] = jnp.zeros((HALO, LANES), jnp.float32)

    def convolve(layer, half, chunk, start, stop):
        base = spans[layer][half][0]
        blocks = []
        while start < stop:
            count = min(ROWS, stop - start)
            blocks.append((start, count))
            start += count

        @pl.loop(chunk * groups, (chunk + 1) * groups)
        def _(lane):
            here = pl.ds(pl.multiple_of(lane * LANES, LANES), LANES)
            bias = bias_ref[layer : layer + 1, here]
            for first_row, count in blocks:
                tiles = count // SUBLANES
                sums = [jnp.broadcast_to(bias, (SUBLANES, LANES))] * tiles
                for residue in range(SUBLANES):
                    begin = first_row + HALO - K + 1 + residue
                    held_taps = range(residue, K, SUBLANES)
                    weights = [taps[layer, tap : tap + 1, here] for tap in held_taps]
                    for index in range(tiles + len(weights) - 1):
                        at = begin + index * SUBLANES
                        window = ext[lane, at : at + SUBLANES, :]
                        for step, weight in enumerate(weights):
                            tile = index - step
                            if 0 <= tile < tiles:
                                sums[tile] = sums[tile] + window * weight
                total = jnp.concatenate(sums, axis=0)
                filt[first_row : first_row + count, here] = total
                inner = slice(first_row - base, first_row - base + count)
                part[half, chunk, 0, inner, :] += total
                part[half, chunk, 1, inner, :] += total * total

    lane_index = lax.broadcasted_iota(jnp.int32, (HALO, LANES), 1)

    def centre(layer, half, chunk):
        start, stop = spans[layer][half]

        for block in range((stop - start) // HALO):
            inner = slice(block * HALO, (block + 1) * HALO)
            rows = slice(start + block * HALO, start + (block + 1) * HALO)
            mean = jnp.sum(part[half, chunk, 0, inner, :], axis=1, keepdims=True) / CHUNK
            squares = jnp.sum(part[half, chunk, 1, inner, :], axis=1, keepdims=True)
            for lane in range(groups):
                at = chunk * CHUNK + lane * LANES
                cf[layer, my_y, chunk, rows, lane * LANES : (lane + 1) * LANES] = (
                    filt[rows, at : at + LANES] - mean
                ).astype(jnp.bfloat16)
            packed = jnp.where(
                lane_index == chunk, mean, jnp.where(lane_index == n_a + chunk, squares, 0.0)
            )
            if chunk:
                packed = packed + columns[half, inner, :]
            columns[half, inner, :] = packed

    def send_centred(layer, half, phase, chunk):
        ref = cf.at[layer, my_y, chunk, rows_of(spans[layer][half])]
        for step in range(1, n_y):
            launch(y_copy(phase, ref, step, chunk))

    def stat_copy(layer, half, step, owner, target):
        ref = stat.at[layer, half, owner]
        index = layer * 2 + half
        return remote(ref, ref, stat_send.at[index, step], stat_recv.at[index, step], target)

    def send_stats(layer, half):
        stat[layer, half, me] = jnp.transpose(columns[half])[:SUBLANES]
        for step in range(1, n_tp):
            launch(stat_copy(layer, half, step, me, lax.rem(me + step, n_tp)))

    def to_columns(rows):
        fill = jnp.zeros((LANES - rows.shape[0], padded), jnp.float32)
        return jnp.transpose(jnp.concatenate((rows, fill), axis=0))

    def settle(layer, half):
        for step in range(1, n_tp):
            origin = lax.rem(me + n_tp - step, n_tp)
            stat_copy(layer, half, step, origin, origin).wait_recv()
        totals = jnp.sum(stat[layer, half], axis=0)
        mean_row = jnp.sum(totals[:n_a], axis=0, keepdims=True) * CHUNK / total_chans
        square_row = jnp.sum(totals[n_a : 2 * n_a], axis=0, keepdims=True) / total_chans
        rstd_row = lax.rsqrt(square_row - mean_row * mean_row + epsilon)
        rows = [rstd_row]
        for step in range(n_y):
            means = stat[layer, half, y_origin(step) * CORES + core]
            rows.append((means[:n_a] - mean_row) * rstd_row)
        columns[half] = to_columns(jnp.concatenate(rows, axis=0))

    def activate(layer, half, step, chunk):
        start, stop = spans[layer][half]
        origin = y_origin(step)
        owner = origin * CORES + core

        at = 1 + step * n_a + chunk
        gains = 0.5 * chan[origin, 0, layer : layer + 1, chunk * CHUNK : (chunk + 1) * CHUNK]
        biases = 0.5 * chan[origin, 1, layer : layer + 1, chunk * CHUNK : (chunk + 1) * CHUNK]
        for block in range((stop - start) // HALO):
            inner = slice(block * HALO, (block + 1) * HALO)
            rows = slice(start + block * HALO, start + (block + 1) * HALO)
            rstd = jnp.broadcast_to(columns[half, inner, 0:1], (HALO, LANES))
            shift = jnp.broadcast_to(columns[half, inner, at : at + 1], (HALO, LANES))
            for lane in range(groups):
                cols = slice(lane * LANES, (lane + 1) * LANES)
                values = cf[layer, origin, chunk, rows, cols].astype(jnp.float32) * rstd + shift
                values = values * gains[:, cols] + biases[:, cols]
                ag[layer, owner, chunk, rows, cols] = (values + values * jnp.tanh(values)).astype(
                    jnp.bfloat16
                )

    def own_activated(layer, half, phase):
        for chunk in range(n_a):
            activate(layer, half, 0, chunk)
            launch(f_copy(phase, ag.at[layer], 0, chunk, me, spans[layer][half]))

    def arrived_activated(layer, half, phase):
        for step in range(1, n_y):
            owner = y_origin(step) * CORES + core
            for chunk in range(n_a):
                ref = cf.at[layer, y_origin(step), chunk, rows_of(spans[layer][half])]
                y_copy(phase, ref, step, chunk).wait_recv()
                activate(layer, half, step, chunk)
                launch(f_copy(phase, ag.at[layer], step, chunk, owner, spans[layer][half]))

    def mix(layer, half, owner, chunks, first=False, last=False):
        rows = slice(*spans[layer][half])
        if not first:
            total = acco[rows, :]
        elif layer == 0:
            total = x_in[rows, pl.ds(pl.multiple_of(me * feats, LANES), feats)].astype(jnp.float32)
        else:
            total = res[rows, :]
        for chunk in chunks:
            start = pl.multiple_of(owner * chans + chunk * CHUNK, LANES)
            total = total + dot_nt(
                ag[layer, owner, chunk, rows, :], wo[layer, :, pl.ds(start, CHUNK)]
            )
        if last:
            out_ref[rows, :] = total.astype(jnp.bfloat16)
        else:
            acco[rows, :] = total

    def mix_own(layer, half):
        mix(layer, half, me, range(n_a), True)

    def mix_arrived(layer, half):
        for step in range(1, n_y):
            mix(layer, half, y_origin(step) * CORES + core, range(n_a))

    def mix_sibling(layer, half, phase):
        for chunk in range(n_a):
            f_copy(phase, ag.at[layer], 0, chunk, sibling, spans[layer][half]).wait_recv()
        mix(layer, half, sibling, range(n_a))

    def mix_relayed(layer, half, phase, groups_of):
        for step in range(1, n_y):
            owner = y_origin(step) * CORES + 1 - core
            for chunks in groups_of:
                for chunk in chunks:
                    f_copy(phase, ag.at[layer], step, chunk, owner, spans[layer][half]).wait_recv()
                final = step == n_y - 1 and chunks[-1] == n_a - 1
                mix(layer, half, owner, chunks, False, layer == LAYERS - 1 and final)

    def square_copy(half, step, owner, target):
        ref = square.at[half, owner]
        return remote(ref, ref, square_send.at[half, step], square_recv.at[half, step], target)

    def send_stream(half):
        span = spans[0][half]
        rows = slice(*span)
        squares = jnp.zeros((span[1] - span[0], LANES), jnp.float32)
        for chunk in range(n_f):
            first = pl.multiple_of(me * feats + chunk * CHUNK, LANES)
            gains = gain_ref[1:2, pl.ds(first, CHUNK)]
            for lane in range(groups):
                cols = slice(lane * LANES, (lane + 1) * LANES)
                here = slice(chunk * CHUNK + lane * LANES, chunk * CHUNK + (lane + 1) * LANES)
                rounded = acco[rows, here].astype(jnp.bfloat16).astype(jnp.float32)
                sg[me, chunk, rows, cols] = (rounded * gains[:, cols]).astype(jnp.bfloat16)
                res[rows, here] = rounded
                squares = squares + rounded * rounded
            if chunk == n_f - 1:
                send_squares(half, squares)
            ref = sg.at[me, chunk, rows_of(span)]
            for step in range(1, n_y):
                launch(y_copy(2 + half, ref, step, chunk))
            launch(f_copy(2 + half, sg, 0, chunk, me, span))

    def send_squares(half, squares):
        span = spans[0][half]
        count = span[1] - span[0]
        if count < padded:
            fill = jnp.zeros((padded - count, LANES), jnp.float32)
            squares = jnp.concatenate((squares, fill), axis=0)
        row = jnp.sum(jnp.transpose(squares), axis=0, keepdims=True)
        square[half, me] = jnp.broadcast_to(row, (SUBLANES, padded))
        for step in range(1, n_tp):
            launch(square_copy(half, step, me, lax.rem(me + step, n_tp)))

    def rescale(half):
        for step in range(1, n_tp):
            origin = lax.rem(me + n_tp - step, n_tp)
            square_copy(half, step, origin, origin).wait_recv()
        totals = jnp.sum(square[half], axis=0)[0:1] / width
        start, stop = spans[0][half]
        spread = jnp.transpose(
            jnp.broadcast_to(0.5 * lax.rsqrt(totals + epsilon), (LANES, padded))
        )
        scale[start:stop, :] = spread[: stop - start]

    def project(half, owner, chunks, first):
        rows = slice(*spans[0][half])
        for block in range(n_a):
            total = None if first else accp[rows, held(block)]
            for chunk in chunks:
                start = pl.multiple_of(owner * feats + chunk * CHUNK, LANES)
                product = dot_nt(
                    sg[owner, chunk, rows, :], wp[1, block, :, pl.ds(start, CHUNK)]
                )
                total = product if total is None else total + product
            accp[rows, held(block)] = total

    def near_stream(half):
        project(half, me, range(n_f), True)
        for chunk in range(n_f):
            f_copy(2 + half, sg, 0, chunk, sibling, spans[0][half]).wait_recv()
        project(half, sibling, range(n_f), False)

    def arrive_stream(half, chunk):
        for step in range(1, n_y):
            origin = y_origin(step)
            owner = origin * CORES + core
            ref = sg.at[owner, chunk, rows_of(spans[0][half])]
            y_copy(2 + half, ref, step, chunk).wait_recv()
            launch(f_copy(2 + half, sg, step, chunk, owner, spans[0][half]))
            project(half, owner, (chunk,), False)

    def relayed_stream(half, chunk):
        for step in range(1, n_y):
            owner = y_origin(step) * CORES + 1 - core
            f_copy(2 + half, sg, step, chunk, owner, spans[0][half]).wait_recv()
            project(half, owner, (chunk,), False)

    def far_stream(half, chunks):
        for chunk in chunks:
            arrive_stream(half, chunk)
            if chunk:
                relayed_stream(half, chunk - 1)

    everything = range(n_a)
    smalls[0].wait()
    for index in range(PIECES):
        cols = slice(index * piece, (index + 1) * piece)
        x_copy(index).wait()
        prepare(index)
        for copy in proj_copies(0, 0, index):
            copy.wait()
        if index == PIECES - 1:
            for chunk in range(1, n_a):
                for copy in proj_copies(0, chunk):
                    copy.start()
        product = dot_nt(xg[:, cols], wp[0, 0, :, cols])
        if index:
            accp[:, held(0)] += product
        else:
            accp[:, held(0)] = product

    @pl.loop(0, tokens // ROWS)
    def _(block):
        rows = pl.ds(pl.multiple_of(block * ROWS, ROWS), ROWS)
        scaling = lax.rsqrt(jnp.sum(norm_squares[rows, :], axis=1, keepdims=True) / width + epsilon)
        scale[rows, :] = jnp.broadcast_to(0.5 * scaling, (ROWS, LANES))

    for copy in smalls[1:]:
        copy.wait()
    for layer in range(LAYERS):
        taps[layer] = raw_taps[:, layer, :]
    pl.semaphore_wait(
        barrier,
        n_tp - 1 + jnp.where(sp > 0, 1, 0) + jnp.where(sp < n_sp - 1, 1, 0),
    )
    for step in range(1, n_y):
        launch(chan_copy(step, my_y))

    for chunk in range(n_a):
        if chunk:
            for copy in proj_copies(0, chunk):
                copy.wait()
            accp[:, held(chunk)] = dot_nt(xg[...], wp[0, chunk])
        send_halo(0, chunk)
        gate_rows(chunk, 0, tokens - HALO)
        convolve(0, 0, chunk, *spans[0][0])
        centre(0, 0, chunk)
        if chunk == n_a - 1:
            send_stats(0, 0)
        send_centred(0, 0, 0, chunk)
    out_copy(0).start()
    for chunk in range(n_a):
        convolve(0, 1, chunk, ROWS, spans[0][1][1])
        receive_halo(0, chunk)
        convolve(0, 1, chunk, 0, ROWS)
        centre(0, 1, chunk)
        if chunk == n_a - 1:
            send_stats(0, 1)
        send_centred(0, 1, 1, chunk)
    for chunk in range(n_a):
        for copy in proj_copies(1, chunk):
            copy.start()
    out_copy(1).start()
    for step in range(1, n_y):
        chan_copy(step, y_origin(step)).wait_recv()
    settle(0, 0)
    own_activated(0, 0, 0)
    out_copy(0).wait()
    mix_own(0, 0)
    arrived_activated(0, 0, 0)
    mix_arrived(0, 0)
    mix_sibling(0, 0, 0)
    settle(0, 1)
    own_activated(0, 1, 1)
    mix_relayed(0, 0, 0, [everything])
    send_stream(0)
    mix_own(0, 1)
    arrived_activated(0, 1, 1)
    mix_arrived(0, 1)
    mix_sibling(0, 1, 1)
    mix_relayed(0, 1, 1, [everything])
    send_stream(1)
    part[...] = jnp.zeros(part.shape, jnp.float32)
    for chunk in range(n_a):
        for copy in proj_copies(1, chunk):
            copy.wait()
    near_stream(0)
    far_stream(0, range(n_f))
    near_stream(1)
    relayed_stream(0, n_f - 1)
    rescale(0)
    for chunk in range(n_a):
        send_halo(1, chunk)
        gate_rows(chunk, split, tokens - HALO)
        convolve(1, 0, chunk, *spans[1][0])
        centre(1, 0, chunk)
    send_stats(1, 0)
    for chunk in range(n_a):
        send_centred(1, 0, 4, chunk)
    far_stream(1, range(n_f // 2))
    settle(1, 0)
    own_activated(1, 0, 4)
    far_stream(1, range(n_f // 2, n_f))
    relayed_stream(1, n_f - 1)
    rescale(1)
    for chunk in range(n_a):
        gate_rows(chunk, 0, split)
        convolve(1, 1, chunk, HALO, spans[1][1][1])
        receive_halo(1, chunk)
        convolve(1, 1, chunk, 0, HALO)
        centre(1, 1, chunk)
        if chunk == n_a - 1:
            send_stats(1, 1)
        send_centred(1, 1, 5, chunk)
    out_copy(1).wait()
    mix_own(1, 0)
    mix_sibling(1, 0, 4)
    arrived_activated(1, 0, 4)
    mix_arrived(1, 0)
    settle(1, 1)
    own_activated(1, 1, 5)
    mix_own(1, 1)
    mix_relayed(1, 0, 4, [everything])
    mix_sibling(1, 1, 5)
    arrived_activated(1, 1, 5)
    mix_arrived(1, 1)
    mix_relayed(1, 1, 5, [(chunk,) for chunk in everything])

    @pl.when(sp < n_sp - 1)
    def _():
        for layer in range(LAYERS):
            for chunk in range(n_a):
                halo_copy(layer, chunk).wait_send()

    for copy in pending:
        copy.wait_send()


def fused(mesh, stream, norm_gain, value_weight, gate_weight, conv_kernel, conv_bias,
          channel_gain, channel_bias, out_weight):
    n_tp, n_sp = mesh.shape["tp"], mesh.shape["sp"]
    width, tokens = stream.shape
    chans, feats = value_weight.shape[1], out_weight.shape[1]
    split = (tokens // 2 - HALO) // HALO * HALO
    n_y = n_tp // CORES
    n_a, n_f = chans // CHUNK, feats // CHUNK
    fits = (
        n_tp % CORES == 0
        and chans % CHUNK == 0
        and feats % CHUNK == 0
        and width % (PIECES * CHUNK) == 0
        and tokens % ROWS == 0
        and split % ROWS == 0
        and tokens >= 4 * ROWS
        and LAYERS == 2
        and n_tp <= 8
        and 2 * n_a <= SUBLANES
        and 1 + n_y * n_a <= LANES
    )
    if not fits:
        return local(stream, norm_gain, value_weight, gate_weight, conv_kernel, conv_bias,
                     channel_gain, channel_bias, out_weight)
    padded = -(-(tokens - split) // LANES) * LANES
    most = max(n_a, n_f)
    f32, bf16 = jnp.float32, jnp.bfloat16
    dma = pltpu.SemaphoreType.DMA
    out = pl.pallas_call(
        functools.partial(kernel, n_tp, n_sp, split),
        out_shape=jax.ShapeDtypeStruct((tokens, feats), bf16),
        in_specs=[pl.BlockSpec(memory_space=pl.ANY)] * 9,
        out_specs=pl.BlockSpec(memory_space=pltpu.VMEM),
        scratch_shapes=[
            pltpu.VMEM((LAYERS, width), f32),
            pltpu.VMEM((K, LAYERS, chans), f32),
            pltpu.VMEM((LAYERS, chans), f32),
            pltpu.VMEM((n_y, 2, LAYERS, chans), f32),
            pltpu.VMEM((LAYERS, n_a, 2 * CHUNK, width), bf16),
            pltpu.VMEM((LAYERS, feats, chans * n_tp), bf16),
            pltpu.VMEM((tokens, width), bf16),
            pltpu.VMEM((tokens, width), bf16),
            pltpu.VMEM((chans // LANES, HALO + tokens, LANES), f32),
            pltpu.VMEM((tokens, chans), f32),
            pltpu.VMEM((LAYERS, K, chans), f32),
            pltpu.VMEM((tokens, LANES), f32),
            pltpu.VMEM((tokens, LANES), f32),
            pltpu.VMEM((2, n_a, 2, padded, LANES), f32),
            pltpu.VMEM((2, padded, LANES), f32),
            pltpu.VMEM((LAYERS, n_a, HALO, CHUNK), bf16),
            pltpu.VMEM((LAYERS, n_a, HALO, CHUNK), bf16),
            pltpu.VMEM((LAYERS, 2, n_tp, SUBLANES, padded), f32),
            pltpu.VMEM((2, n_tp, SUBLANES, padded), f32),
            pltpu.VMEM((LAYERS, n_y, n_a, tokens, CHUNK), bf16),
            pltpu.VMEM((LAYERS, n_tp, n_a, tokens, CHUNK), bf16),
            pltpu.VMEM((n_tp, n_f, tokens, CHUNK), bf16),
            pltpu.VMEM((tokens, 2 * chans), f32),
            pltpu.VMEM((tokens, feats), f32),
            pltpu.VMEM((tokens, feats), f32),
            dma((5,)),
            dma((PIECES,)),
            dma((LAYERS, n_a, PIECES)),
            dma((LAYERS,)),
            dma((n_y,)),
            dma((n_y,)),
            dma((LAYERS, n_a)),
            dma((LAYERS, n_a)),
            dma((LAYERS * 2, n_tp)),
            dma((LAYERS * 2, n_tp)),
            dma((2, n_tp)),
            dma((2, n_tp)),
            dma((6, n_y, most)),
            dma((6, n_y, most)),
            dma((6, n_y, most)),
            dma((6, n_y, most)),
        ],
        compiler_params=pltpu.CompilerParams(
            collective_id=0, has_side_effects=True, vmem_limit_bytes=50 * 1024 * 1024
        ),
    )(*(
        pltpu.with_memory_space_constraint(value, pltpu.HBM)
        for value in (
            stream.T, norm_gain, jnp.transpose(conv_kernel, (2, 0, 1)), conv_bias, channel_gain,
            channel_bias, value_weight, gate_weight, out_weight,
        )
    ))
    return out.T


def solution(mesh):
    placed = (
        P(None, ("grp", "sp")),
        P(),
        P(None, "tp", None),
        P(None, "tp", None),
        P(None, "tp", None),
        P(None, "tp"),
        P(None, "tp"),
        P(None, "tp"),
        P(None, "tp", None),
    )
    return jax.shard_map(
        functools.partial(fused, mesh), mesh=mesh, in_specs=placed, out_specs=P("tp", ("grp", "sp")), check_vma=False
    )
```

```python
import functools

import jax
import jax.numpy as jnp
from jax import lax
from jax.experimental import pallas as pl
from jax.experimental.pallas import tpu as pltpu
from jax.sharding import PartitionSpec as P

K = 31
LAYERS = 2


epsilon = 1e-06


def shifted(value, axis, steps):
    count = lax.axis_size(axis)
    initial, last = (max(0, -steps), min(count, count - steps))
    return lax.ppermute(value, axis, [(source, source + steps) for source in range(initial, last)])


def depthwise(signal, kernel):
    out = lax.conv_general_dilated(
        signal[None],
        kernel[:, None, :],
        (1,),
        [(0, 0)],
        dimension_numbers=("NCW", "OIW", "NCW"),
        feature_group_count=kernel.shape[0],
        precision=lax.Precision.HIGHEST,
    )
    return out[0]


def norm_project(whole, gain, weights):
    scaling = lax.rsqrt(jnp.mean(whole * whole, axis=0, keepdims=True) + epsilon)
    normed = (whole * scaling * gain[:, None]).astype(jnp.bfloat16)
    return jnp.dot(weights, normed, preferred_element_type=jnp.float32)


def local(
    stream,
    norm_gain,
    value_weight,
    gate_weight,
    conv_kernel,
    conv_bias,
    channel_gain,
    channel_bias,
    out_weight,
):
    shard_channels = value_weight.shape[1]
    total_channels = shard_channels * lax.axis_size("tp")
    shard_features = out_weight.shape[1]
    tokens_here = stream.shape[1]
    row_start = lax.axis_index("tp") * shard_features
    whole = stream.astype(jnp.float32)
    current = lax.dynamic_slice_in_dim(whole, row_start, shard_features, 0)
    layer_out = stream
    for layer in range(LAYERS):
        both_weights = jnp.concatenate((value_weight[layer], gate_weight[layer]), axis=0)
        if layer == 0:
            projected = norm_project(whole, norm_gain[layer], both_weights)
        else:
            gathered = lax.all_gather(layer_out, "tp", axis=0, tiled=True).astype(jnp.float32)
            projected = norm_project(gathered, norm_gain[layer], both_weights)
        gated = (projected[:shard_channels] * jax.nn.sigmoid(projected[shard_channels:])).astype(
            jnp.bfloat16
        )
        earlier = shifted(gated[:, tokens_here - (K - 1) :], "sp", 1)
        extended = jnp.concatenate((earlier, gated), axis=1).astype(jnp.float32)
        filtered = depthwise(extended, conv_kernel[layer]) + conv_bias[layer][:, None]
        first_sum, square_sum = lax.psum(
            (
                jnp.sum(filtered, axis=0, keepdims=True),
                jnp.sum(filtered * filtered, axis=0, keepdims=True),
            ),
            "tp",
        )
        row_mean = first_sum / total_channels
        centred = filtered - row_mean
        spread = square_sum / total_channels - row_mean * row_mean
        activated = jax.nn.silu(
            centred * lax.rsqrt(spread + epsilon) * channel_gain[layer][:, None]
            + channel_bias[layer][:, None]
        ).astype(jnp.bfloat16)

        def accumulate(total, piece, start, weights=out_weight[layer]):
            weight_cols = lax.dynamic_slice_in_dim(weights, start, piece.shape[0], 1)
            return total + jnp.dot(weight_cols, piece, preferred_element_type=jnp.float32)

        zero_branch = jnp.zeros((shard_features, tokens_here), jnp.float32)
        branch = accumulate(
            zero_branch, lax.all_gather(activated, "tp", axis=0, tiled=True), jnp.int32(0)
        )
        layer_out = (current + branch).astype(jnp.bfloat16)
        current = layer_out.astype(jnp.float32)
    return layer_out


MESH = pl.DeviceIdType.MESH
LANES = 128
SUBLANES = 8
CHUNK = 256
HALO = 32
ROWS = 64
CORES = 2
PIECES = 4


def dot_nt(left, right):
    return lax.dot_general(
        left, right, (((1,), (1,)), ((), ())), preferred_element_type=jnp.float32
    )


def kernel(
    n_tp,
    n_sp,
    split,
    x_hbm,
    gain_hbm,
    taps_hbm,
    bias_hbm,
    chan_gain_hbm,
    chan_bias_hbm,
    wv_ref,
    wg_ref,
    ow_ref,
    out_ref,
    gain_ref,
    raw_taps,
    bias_ref,
    chan,
    wp,
    wo,
    x_in,
    xg,
    ext,
    filt,
    taps,
    norm_squares,
    scale,
    part,
    columns,
    halo_out,
    halo_in,
    stat,
    square,
    cf,
    ag,
    sg,
    accp,
    acco,
    res,
    small_sem,
    x_sem,
    wp_sem,
    wo_sem,
    chan_send,
    chan_recv,
    halo_send,
    halo_recv,
    stat_send,
    stat_recv,
    square_send,
    square_recv,
    y_send,
    y_recv,
    f_send,
    f_recv,
):
    tokens, width = x_in.shape
    chans = wv_ref.shape[1]
    feats = ow_ref.shape[1]
    total_chans = chans * n_tp
    n_y = n_tp // CORES
    piece = width // PIECES
    padded = stat.shape[-1]
    n_a, n_f = chans // CHUNK, feats // CHUNK
    groups = CHUNK // LANES
    spans = (
        ((split, tokens), (0, split)),
        ((split + HALO, tokens), (0, split + HALO)),
    )
    me = lax.axis_index("tp")
    sp = lax.axis_index("sp")
    my_y, core = me // CORES, me % CORES
    sibling = my_y * CORES + (1 - core)

    def tp_id(index):
        return {"tp": index}

    smalls = [
        pltpu.make_async_copy(source, target, small_sem.at[index])
        for index, (source, target) in enumerate(
            (
                (gain_hbm, gain_ref),
                (taps_hbm, raw_taps),
                (bias_hbm, bias_ref),
                (chan_gain_hbm, chan.at[my_y, 0]),
                (chan_bias_hbm, chan.at[my_y, 1]),
            )
        )
    ]

    def x_copy(index):
        cols = pl.ds(index * piece, piece)
        return pltpu.make_async_copy(x_hbm.at[:, cols], x_in.at[:, cols], x_sem.at[index])

    def proj_copies(layer, chunk, index=None):
        rows = pl.ds(chunk * CHUNK, CHUNK)
        cols = slice(None) if index is None else pl.ds(index * piece, piece)
        return [
            pltpu.make_async_copy(
                ref.at[layer, rows, cols],
                wp.at[layer, chunk, pl.ds(half * CHUNK, CHUNK), cols],
                wp_sem.at[layer, chunk, index or 0],
            )
            for half, ref in enumerate((wv_ref, wg_ref))
        ]

    def out_copy(layer):
        return pltpu.make_async_copy(ow_ref.at[layer], wo.at[layer], wo_sem.at[layer])

    for copy in smalls:
        copy.start()
    for index in range(PIECES):
        x_copy(index).start()
        for copy in proj_copies(0, 0, index):
            copy.start()

    barrier = pltpu.get_barrier_semaphore()
    for step in range(1, n_tp):
        pl.semaphore_signal(
            barrier, inc=1, device_id=tp_id(lax.rem(me + step, n_tp)), device_id_type=MESH
        )

    @pl.when(sp > 0)
    def _():
        pl.semaphore_signal(barrier, inc=1, device_id={"sp": sp - 1}, device_id_type=MESH)

    @pl.when(sp < n_sp - 1)
    def _():
        pl.semaphore_signal(barrier, inc=1, device_id={"sp": sp + 1}, device_id_type=MESH)

    part[...] = jnp.zeros(part.shape, jnp.float32)
    columns[...] = jnp.zeros(columns.shape, jnp.float32)

    pending = []

    def remote(source, target, send, recv, device):
        return pltpu.make_async_remote_copy(
            src_ref=source,
            dst_ref=target,
            send_sem=send,
            recv_sem=recv,
            device_id=tp_id(device),
            device_id_type=MESH,
        )

    def launch(copy):
        copy.start()
        pending.append(copy)

    def drain(keep=0):
        while len(pending) > keep:
            pending.pop(0).wait_send()

    def rows_of(span):
        return pl.ds(span[0], span[1] - span[0])

    def y_peer(step):
        return lax.rem(my_y + step, n_y)

    def y_origin(step):
        return lax.rem(my_y + n_y - step, n_y)

    def y_copy(phase, ref, step, chunk):
        target = y_peer(step) * CORES + core
        return remote(
            ref, ref, y_send.at[phase, step, chunk], y_recv.at[phase, step, chunk], target
        )

    def f_copy(phase, buf, step, chunk, owner, span):
        ref = buf.at[owner, chunk, rows_of(span)]
        return remote(
            ref, ref, f_send.at[phase, step, chunk], f_recv.at[phase, step, chunk], sibling
        )

    def chan_copy(step, slot):
        target = y_peer(step) * CORES + core
        return remote(chan.at[slot], chan.at[slot], chan_send.at[step], chan_recv.at[step], target)

    def prepare(index):
        gains = gain_ref[0:1, index * piece : (index + 1) * piece]
        for first_row in range(0, tokens, ROWS):
            rows = slice(first_row, first_row + ROWS)
            squares = norm_squares[rows, :] if index else None
            for lane in range(piece // LANES):
                here = slice(index * piece + lane * LANES, index * piece + (lane + 1) * LANES)
                values = x_in[rows, here].astype(jnp.float32)
                squares = values * values if squares is None else squares + values * values
                xg[rows, here] = (values * gains[:, lane * LANES : (lane + 1) * LANES]).astype(
                    jnp.bfloat16
                )
            norm_squares[rows, :] = squares

    def held(chunk):
        return slice(chunk * 2 * CHUNK, (chunk + 1) * 2 * CHUNK)

    def gate(chunk, first_row, count):
        rows = pl.ds(first_row, count)
        halved = scale[rows, :]
        start = chunk * 2 * CHUNK
        pieces = []
        for lane in range(groups):
            at = start + lane * LANES
            value = accp[rows, at : at + LANES] * halved
            gates = accp[rows, at + CHUNK : at + CHUNK + LANES] * halved
            gated = (value + value * jnp.tanh(gates)).astype(jnp.bfloat16)
            ext[chunk * groups + lane, pl.ds(first_row + HALO, count), :] = gated.astype(
                jnp.float32
            )
            pieces.append(gated)
        return pieces

    def gate_rows(chunk, start, stop):
        @pl.loop(0, (stop - start) // HALO)
        def _(block):
            gate(chunk, pl.multiple_of(start + block * HALO, HALO), HALO)

    def halo_copy(layer, chunk):
        return pltpu.make_async_remote_copy(
            src_ref=halo_out.at[layer, chunk],
            dst_ref=halo_in.at[layer, chunk],
            send_sem=halo_send.at[layer, chunk],
            recv_sem=halo_recv.at[layer, chunk],
            device_id={"sp": lax.rem(sp + 1, n_sp)},
            device_id_type=MESH,
        )

    def send_halo(layer, chunk):
        for lane, gated in enumerate(gate(chunk, tokens - HALO, HALO)):
            halo_out[layer, chunk, :, lane * LANES : (lane + 1) * LANES] = gated

        @pl.when(sp < n_sp - 1)
        def _():
            halo_copy(layer, chunk).start()

    def receive_halo(layer, chunk):
        @pl.when(sp > 0)
        def _():
            halo_copy(layer, chunk).wait_recv()
            for lane in range(groups):
                ext[chunk * groups + lane, :HALO, :] = halo_in[
                    layer, chunk, :, lane * LANES : (lane + 1) * LANES
                ].astype(jnp.float32)

        @pl.when(sp == 0)
        def _():
            for lane in range(groups):
                ext[chunk * groups + lane, :HALO, :] = jnp.zeros((HALO, LANES), jnp.float32)

    def convolve(layer, half, chunk, start, stop):
        base = spans[layer][half][0]
        blocks = []
        while start < stop:
            count = min(ROWS, stop - start)
            blocks.append((start, count))
            start += count

        @pl.loop(chunk * groups, (chunk + 1) * groups)
        def _(lane):
            here = pl.ds(pl.multiple_of(lane * LANES, LANES), LANES)
            bias = bias_ref[layer : layer + 1, here]
            for first_row, count in blocks:
                tiles = count // SUBLANES
                sums = [jnp.broadcast_to(bias, (SUBLANES, LANES))] * tiles
                for residue in range(SUBLANES):
                    begin = first_row + HALO - K + 1 + residue
                    held_taps = range(residue, K, SUBLANES)
                    weights = [taps[layer, tap : tap + 1, here] for tap in held_taps]
                    for index in range(tiles + len(weights) - 1):
                        at = begin + index * SUBLANES
                        window = ext[lane, at : at + SUBLANES, :]
                        for step, weight in enumerate(weights):
                            tile = index - step
                            if 0 <= tile < tiles:
                                sums[tile] = sums[tile] + window * weight
                total = jnp.concatenate(sums, axis=0)
                filt[first_row : first_row + count, here] = total
                inner = slice(first_row - base, first_row - base + count)
                part[half, chunk, 0, inner, :] += total
                part[half, chunk, 1, inner, :] += total * total

    lane_index = lax.broadcasted_iota(jnp.int32, (HALO, LANES), 1)

    def centre(layer, half, chunk):
        start, stop = spans[layer][half]

        for block in range((stop - start) // HALO):
            inner = slice(block * HALO, (block + 1) * HALO)
            rows = slice(start + block * HALO, start + (block + 1) * HALO)
            mean = jnp.sum(part[half, chunk, 0, inner, :], axis=1, keepdims=True) / CHUNK
            squares = jnp.sum(part[half, chunk, 1, inner, :], axis=1, keepdims=True)
            for lane in range(groups):
                at = chunk * CHUNK + lane * LANES
                cf[layer, my_y, chunk, rows, lane * LANES : (lane + 1) * LANES] = (
                    filt[rows, at : at + LANES] - mean
                ).astype(jnp.bfloat16)
            packed = jnp.where(
                lane_index == chunk, mean, jnp.where(lane_index == n_a + chunk, squares, 0.0)
            )
            if chunk:
                packed = packed + columns[half, inner, :]
            columns[half, inner, :] = packed

    def send_centred(layer, half, phase, chunk):
        ref = cf.at[layer, my_y, chunk, rows_of(spans[layer][half])]
        for step in range(1, n_y):
            launch(y_copy(phase, ref, step, chunk))

    def stat_copy(layer, half, step, owner, target):
        ref = stat.at[layer, half, owner]
        index = layer * 2 + half
        return remote(ref, ref, stat_send.at[index, step], stat_recv.at[index, step], target)

    def send_stats(layer, half):
        stat[layer, half, me] = jnp.transpose(columns[half])[:SUBLANES]
        for step in range(1, n_tp):
            launch(stat_copy(layer, half, step, me, lax.rem(me + step, n_tp)))

    def to_columns(rows):
        fill = jnp.zeros((LANES - rows.shape[0], padded), jnp.float32)
        return jnp.transpose(jnp.concatenate((rows, fill), axis=0))

    def settle(layer, half):
        for step in range(1, n_tp):
            origin = lax.rem(me + n_tp - step, n_tp)
            stat_copy(layer, half, step, origin, origin).wait_recv()
        totals = jnp.sum(stat[layer, half], axis=0)
        mean_row = jnp.sum(totals[:n_a], axis=0, keepdims=True) * CHUNK / total_chans
        square_row = jnp.sum(totals[n_a : 2 * n_a], axis=0, keepdims=True) / total_chans
        rstd_row = lax.rsqrt(square_row - mean_row * mean_row + epsilon)
        rows = [rstd_row]
        for step in range(n_y):
            means = stat[layer, half, y_origin(step) * CORES + core]
            rows.append((means[:n_a] - mean_row) * rstd_row)
        columns[half] = to_columns(jnp.concatenate(rows, axis=0))

    def activate(layer, half, step, chunk):
        start, stop = spans[layer][half]
        origin = y_origin(step)
        owner = origin * CORES + core

        at = 1 + step * n_a + chunk
        gains = 0.5 * chan[origin, 0, layer : layer + 1, chunk * CHUNK : (chunk + 1) * CHUNK]
        biases = 0.5 * chan[origin, 1, layer : layer + 1, chunk * CHUNK : (chunk + 1) * CHUNK]
        for block in range((stop - start) // HALO):
            inner = slice(block * HALO, (block + 1) * HALO)
            rows = slice(start + block * HALO, start + (block + 1) * HALO)
            rstd = jnp.broadcast_to(columns[half, inner, 0:1], (HALO, LANES))
            shift = jnp.broadcast_to(columns[half, inner, at : at + 1], (HALO, LANES))
            for lane in range(groups):
                cols = slice(lane * LANES, (lane + 1) * LANES)
                values = cf[layer, origin, chunk, rows, cols].astype(jnp.float32) * rstd + shift
                values = values * gains[:, cols] + biases[:, cols]
                ag[layer, owner, chunk, rows, cols] = (values + values * jnp.tanh(values)).astype(
                    jnp.bfloat16
                )

    def own_activated(layer, half, phase):
        for chunk in range(n_a):
            activate(layer, half, 0, chunk)
            launch(f_copy(phase, ag.at[layer], 0, chunk, me, spans[layer][half]))

    def arrive(layer, half, phase, chunk):
        for step in range(1, n_y):
            owner = y_origin(step) * CORES + core
            ref = cf.at[layer, y_origin(step), chunk, rows_of(spans[layer][half])]
            y_copy(phase, ref, step, chunk).wait_recv()
            activate(layer, half, step, chunk)
            launch(f_copy(phase, ag.at[layer], step, chunk, owner, spans[layer][half]))

    def from_sibling(layer, half, phase, chunk, step=0):
        owner = y_origin(step) * CORES + 1 - core
        f_copy(phase, ag.at[layer], step, chunk, owner, spans[layer][half]).wait_recv()

    def mix(layer, half, parts, first=False, last=False):
        rows = slice(*spans[layer][half])
        if not first:
            total = acco[rows, :]
        elif layer == 0:
            total = x_in[rows, pl.ds(pl.multiple_of(me * feats, LANES), feats)].astype(jnp.float32)
        else:
            total = res[rows, :]
        for owner, chunk in parts:
            start = pl.multiple_of(owner * chans + chunk * CHUNK, LANES)
            total = total + dot_nt(
                ag[layer, owner, chunk, rows, :], wo[layer, :, pl.ds(start, CHUNK)]
            )
        if last:
            out_ref[rows, :] = total.astype(jnp.bfloat16)
        else:
            acco[rows, :] = total

    everything = range(n_a)
    others = range(1, n_y)

    def own(chunks):
        return [(me, chunk) for chunk in chunks]

    def next_door(chunks):
        return [(sibling, chunk) for chunk in chunks]

    def across(chunks):
        return [(y_origin(step) * CORES + core, chunk) for step in others for chunk in chunks]

    def relayed(chunks):
        return [(y_origin(step) * CORES + 1 - core, chunk) for step in others for chunk in chunks]

    def branch(layer, half, phase, ahead=None):
        own_activated(layer, half, phase)
        mix(layer, half, own(everything), True)
        for chunk in everything[:-1]:
            arrive(layer, half, phase, chunk)
        for chunk in everything:
            from_sibling(layer, half, phase, chunk)
        mix(layer, half, next_door(everything) + across(everything[:-1]))
        if ahead is not None:
            ahead()
        arrive(layer, half, phase, n_a - 1)
        for step in others:
            for chunk in everything[:-1]:
                from_sibling(layer, half, phase, chunk, step)
        mix(layer, half, across(everything[-1:]) + relayed(everything[:-1]))
        for step in others:
            from_sibling(layer, half, phase, n_a - 1, step)
        mix(layer, half, relayed(everything[-1:]), False, layer == LAYERS - 1)

    def square_copy(half, step, owner, target):
        ref = square.at[half, owner]
        return remote(ref, ref, square_send.at[half, step], square_recv.at[half, step], target)

    def send_stream(half):
        span = spans[0][half]
        rows = slice(*span)
        squares = jnp.zeros((span[1] - span[0], LANES), jnp.float32)
        for chunk in range(n_f):
            first = pl.multiple_of(me * feats + chunk * CHUNK, LANES)
            gains = gain_ref[1:2, pl.ds(first, CHUNK)]
            for lane in range(groups):
                cols = slice(lane * LANES, (lane + 1) * LANES)
                here = slice(chunk * CHUNK + lane * LANES, chunk * CHUNK + (lane + 1) * LANES)
                rounded = acco[rows, here].astype(jnp.bfloat16).astype(jnp.float32)
                sg[me, chunk, rows, cols] = (rounded * gains[:, cols]).astype(jnp.bfloat16)
                res[rows, here] = rounded
                squares = squares + rounded * rounded
            if chunk == n_f - 1:
                send_squares(half, squares)
            ref = sg.at[me, chunk, rows_of(span)]
            for step in range(1, n_y):
                launch(y_copy(2 + half, ref, step, chunk))
            launch(f_copy(2 + half, sg, 0, chunk, me, span))

    def send_squares(half, squares):
        span = spans[0][half]
        count = span[1] - span[0]
        if count < padded:
            fill = jnp.zeros((padded - count, LANES), jnp.float32)
            squares = jnp.concatenate((squares, fill), axis=0)
        row = jnp.sum(jnp.transpose(squares), axis=0, keepdims=True)
        square[half, me] = jnp.broadcast_to(row, (SUBLANES, padded))
        for step in range(1, n_tp):
            launch(square_copy(half, step, me, lax.rem(me + step, n_tp)))

    def rescale(half):
        for step in range(1, n_tp):
            origin = lax.rem(me + n_tp - step, n_tp)
            square_copy(half, step, origin, origin).wait_recv()
        totals = jnp.sum(square[half], axis=0)[0:1] / width
        start, stop = spans[0][half]
        spread = jnp.transpose(
            jnp.broadcast_to(0.5 * lax.rsqrt(totals + epsilon), (LANES, padded))
        )
        scale[start:stop, :] = spread[: stop - start]

    def project(half, owner, chunks, first):
        rows = slice(*spans[0][half])
        for block in range(n_a):
            total = None if first else accp[rows, held(block)]
            for chunk in chunks:
                start = pl.multiple_of(owner * feats + chunk * CHUNK, LANES)
                product = dot_nt(
                    sg[owner, chunk, rows, :], wp[1, block, :, pl.ds(start, CHUNK)]
                )
                total = product if total is None else total + product
            accp[rows, held(block)] = total

    def own_stream(half):
        project(half, me, range(n_f), True)

    def sibling_stream(half):
        for chunk in range(n_f):
            f_copy(2 + half, sg, 0, chunk, sibling, spans[0][half]).wait_recv()
        project(half, sibling, range(n_f), False)

    def arrive_stream(half, chunk):
        for step in range(1, n_y):
            origin = y_origin(step)
            owner = origin * CORES + core
            ref = sg.at[owner, chunk, rows_of(spans[0][half])]
            y_copy(2 + half, ref, step, chunk).wait_recv()
            launch(f_copy(2 + half, sg, step, chunk, owner, spans[0][half]))
            project(half, owner, (chunk,), False)

    def relayed_stream(half, chunk):
        for step in range(1, n_y):
            owner = y_origin(step) * CORES + 1 - core
            f_copy(2 + half, sg, step, chunk, owner, spans[0][half]).wait_recv()
            project(half, owner, (chunk,), False)

    for copy in smalls:
        copy.wait()
    for layer in range(LAYERS):
        taps[layer] = raw_taps[:, layer, :]
    x_copy(0).wait()
    prepare(0)
    for index in range(PIECES):
        cols = slice(index * piece, (index + 1) * piece)
        for copy in proj_copies(0, 0, index):
            copy.wait()
        if index < PIECES - 1:
            x_copy(index + 1).wait()
        if index == PIECES // 2:
            for chunk in range(1, n_a):
                for copy in proj_copies(0, chunk):
                    copy.start()
        product = dot_nt(xg[:, cols], wp[0, 0, :, cols])
        if index < PIECES - 1:
            prepare(index + 1)
        if index:
            accp[:, held(0)] += product
        else:
            accp[:, held(0)] = product

    for first_row in range(0, tokens, ROWS):
        rows = slice(first_row, first_row + ROWS)
        scaling = lax.rsqrt(jnp.sum(norm_squares[rows, :], axis=1, keepdims=True) / width + epsilon)
        scale[rows, :] = jnp.broadcast_to(0.5 * scaling, (ROWS, LANES))

    pl.semaphore_wait(
        barrier,
        n_tp - 1 + jnp.where(sp > 0, 1, 0) + jnp.where(sp < n_sp - 1, 1, 0),
    )

    for chunk in everything:
        if chunk:
            for copy in proj_copies(0, chunk):
                copy.wait()
            accp[:, held(chunk)] = dot_nt(xg[...], wp[0, chunk])
        send_halo(0, chunk)
        gate_rows(chunk, 0, tokens - HALO)
        convolve(0, 0, chunk, *spans[0][0])
        centre(0, 0, chunk)
        if chunk == n_a - 1:
            send_stats(0, 0)
        send_centred(0, 0, 0, chunk)
        if chunk == 0:
            for step in others:
                launch(chan_copy(step, my_y))
    out_copy(0).start()
    for chunk in everything:
        convolve(0, 1, chunk, ROWS, spans[0][1][1])
        receive_halo(0, chunk)
        convolve(0, 1, chunk, 0, ROWS)
        centre(0, 1, chunk)
        if chunk == n_a - 1:
            send_stats(0, 1)
        send_centred(0, 1, 1, chunk)
    for chunk in everything:
        for copy in proj_copies(1, chunk):
            copy.start()
    out_copy(1).start()
    for step in others:
        chan_copy(step, y_origin(step)).wait_recv()
    out_copy(0).wait()
    settle(0, 0)
    branch(0, 0, 0)
    send_stream(0)
    settle(0, 1)
    branch(0, 1, 1)
    settled = len(pending)
    send_stream(1)
    part[...] = jnp.zeros(part.shape, jnp.float32)
    for chunk in everything:
        for copy in proj_copies(1, chunk):
            copy.wait()
    own_stream(0)
    sibling_stream(0)
    for chunk in range(n_f):
        if chunk == 1:
            own_stream(1)
        if chunk == 2:
            sibling_stream(1)
        if chunk == n_f - 1:
            drain(len(pending) - settled)
        arrive_stream(0, chunk)
        if chunk:
            relayed_stream(0, chunk - 1)
    relayed_stream(0, n_f - 1)
    rescale(0)
    for chunk in everything:
        send_halo(1, chunk)
        gate_rows(chunk, split, tokens - HALO)
        convolve(1, 0, chunk, *spans[1][0])
        centre(1, 0, chunk)
    streamed = len(pending)
    send_stats(1, 0)
    for chunk in everything:
        send_centred(1, 0, 4, chunk)
    for chunk in range(n_f):
        arrive_stream(1, chunk)
        if chunk:
            relayed_stream(1, chunk - 1)
    relayed_stream(1, n_f - 1)
    rescale(1)
    for chunk in everything:
        gate_rows(chunk, 0, split)
        convolve(1, 1, chunk, HALO, spans[1][1][1])
        receive_halo(1, chunk)
        convolve(1, 1, chunk, 0, HALO)
        centre(1, 1, chunk)
        if chunk == n_a - 1:
            send_stats(1, 1)
        send_centred(1, 1, 5, chunk)
    out_copy(1).wait()
    settle(1, 0)
    drain(len(pending) - streamed)
    branch(1, 0, 4)
    settle(1, 1)
    sent = len(pending)
    branch(1, 1, 5, lambda: drain(len(pending) - sent))

    @pl.when(sp < n_sp - 1)
    def _():
        for layer in range(LAYERS):
            for chunk in range(n_a):
                halo_copy(layer, chunk).wait_send()

    drain()


def fused(mesh, stream, norm_gain, value_weight, gate_weight, conv_kernel, conv_bias,
          channel_gain, channel_bias, out_weight):
    n_tp, n_sp = mesh.shape["tp"], mesh.shape["sp"]
    width, tokens = stream.shape
    chans, feats = value_weight.shape[1], out_weight.shape[1]
    split = (tokens // 2 - HALO) // HALO * HALO
    n_y = n_tp // CORES
    n_a, n_f = chans // CHUNK, feats // CHUNK
    fits = (
        n_tp % CORES == 0
        and chans % CHUNK == 0
        and feats % CHUNK == 0
        and width % (PIECES * CHUNK) == 0
        and tokens % ROWS == 0
        and split % ROWS == 0
        and tokens >= 4 * ROWS
        and LAYERS == 2
        and n_tp <= 8
        and 2 * n_a <= SUBLANES
        and 1 + n_y * n_a <= LANES
    )
    if not fits:
        return local(stream, norm_gain, value_weight, gate_weight, conv_kernel, conv_bias,
                     channel_gain, channel_bias, out_weight)
    padded = -(-(tokens - split) // LANES) * LANES
    most = max(n_a, n_f)
    f32, bf16 = jnp.float32, jnp.bfloat16
    dma = pltpu.SemaphoreType.DMA
    out = pl.pallas_call(
        functools.partial(kernel, n_tp, n_sp, split),
        out_shape=jax.ShapeDtypeStruct((tokens, feats), bf16),
        in_specs=[pl.BlockSpec(memory_space=pl.ANY)] * 9,
        out_specs=pl.BlockSpec(memory_space=pltpu.VMEM),
        scratch_shapes=[
            pltpu.VMEM((LAYERS, width), f32),
            pltpu.VMEM((K, LAYERS, chans), f32),
            pltpu.VMEM((LAYERS, chans), f32),
            pltpu.VMEM((n_y, 2, LAYERS, chans), f32),
            pltpu.VMEM((LAYERS, n_a, 2 * CHUNK, width), bf16),
            pltpu.VMEM((LAYERS, feats, chans * n_tp), bf16),
            pltpu.VMEM((tokens, width), bf16),
            pltpu.VMEM((tokens, width), bf16),
            pltpu.VMEM((chans // LANES, HALO + tokens, LANES), f32),
            pltpu.VMEM((tokens, chans), f32),
            pltpu.VMEM((LAYERS, K, chans), f32),
            pltpu.VMEM((tokens, LANES), f32),
            pltpu.VMEM((tokens, LANES), f32),
            pltpu.VMEM((2, n_a, 2, padded, LANES), f32),
            pltpu.VMEM((2, padded, LANES), f32),
            pltpu.VMEM((LAYERS, n_a, HALO, CHUNK), bf16),
            pltpu.VMEM((LAYERS, n_a, HALO, CHUNK), bf16),
            pltpu.VMEM((LAYERS, 2, n_tp, SUBLANES, padded), f32),
            pltpu.VMEM((2, n_tp, SUBLANES, padded), f32),
            pltpu.VMEM((LAYERS, n_y, n_a, tokens, CHUNK), bf16),
            pltpu.VMEM((LAYERS, n_tp, n_a, tokens, CHUNK), bf16),
            pltpu.VMEM((n_tp, n_f, tokens, CHUNK), bf16),
            pltpu.VMEM((tokens, 2 * chans), f32),
            pltpu.VMEM((tokens, feats), f32),
            pltpu.VMEM((tokens, feats), f32),
            dma((5,)),
            dma((PIECES,)),
            dma((LAYERS, n_a, PIECES)),
            dma((LAYERS,)),
            dma((n_y,)),
            dma((n_y,)),
            dma((LAYERS, n_a)),
            dma((LAYERS, n_a)),
            dma((LAYERS * 2, n_tp)),
            dma((LAYERS * 2, n_tp)),
            dma((2, n_tp)),
            dma((2, n_tp)),
            dma((6, n_y, most)),
            dma((6, n_y, most)),
            dma((6, n_y, most)),
            dma((6, n_y, most)),
        ],
        compiler_params=pltpu.CompilerParams(
            collective_id=0, has_side_effects=True, vmem_limit_bytes=50 * 1024 * 1024
        ),
    )(*(
        pltpu.with_memory_space_constraint(value, pltpu.HBM)
        for value in (
            stream.T, norm_gain, jnp.transpose(conv_kernel, (2, 0, 1)), conv_bias, channel_gain,
            channel_bias, value_weight, gate_weight, out_weight,
        )
    ))
    return out.T


def solution(mesh):
    placed = (
        P(None, ("grp", "sp")),
        P(),
        P(None, "tp", None),
        P(None, "tp", None),
        P(None, "tp", None),
        P(None, "tp"),
        P(None, "tp"),
        P(None, "tp"),
        P(None, "tp", None),
    )
    return jax.shard_map(
        functools.partial(fused, mesh), mesh=mesh, in_specs=placed, out_specs=P("tp", ("grp", "sp")), check_vma=False
    )
```

```python
import functools

import jax
import jax.numpy as jnp
from jax import lax
from jax.experimental import pallas as pl
from jax.experimental.pallas import tpu as pltpu
from jax.sharding import PartitionSpec as P

K = 31
LAYERS = 2


epsilon = 1e-06


def shifted(value, axis, steps):
    count = lax.axis_size(axis)
    initial, last = (max(0, -steps), min(count, count - steps))
    return lax.ppermute(value, axis, [(source, source + steps) for source in range(initial, last)])


def depthwise(signal, kernel):
    out = lax.conv_general_dilated(
        signal[None],
        kernel[:, None, :],
        (1,),
        [(0, 0)],
        dimension_numbers=("NCW", "OIW", "NCW"),
        feature_group_count=kernel.shape[0],
        precision=lax.Precision.HIGHEST,
    )
    return out[0]


def norm_project(whole, gain, weights):
    scaling = lax.rsqrt(jnp.mean(whole * whole, axis=0, keepdims=True) + epsilon)
    normed = (whole * scaling * gain[:, None]).astype(jnp.bfloat16)
    return jnp.dot(weights, normed, preferred_element_type=jnp.float32)


def local(
    stream,
    norm_gain,
    value_weight,
    gate_weight,
    conv_kernel,
    conv_bias,
    channel_gain,
    channel_bias,
    out_weight,
):
    shard_channels = value_weight.shape[1]
    total_channels = shard_channels * lax.axis_size("tp")
    shard_features = out_weight.shape[1]
    tokens_here = stream.shape[1]
    row_start = lax.axis_index("tp") * shard_features
    whole = stream.astype(jnp.float32)
    current = lax.dynamic_slice_in_dim(whole, row_start, shard_features, 0)
    layer_out = stream
    for layer in range(LAYERS):
        both_weights = jnp.concatenate((value_weight[layer], gate_weight[layer]), axis=0)
        if layer == 0:
            projected = norm_project(whole, norm_gain[layer], both_weights)
        else:
            gathered = lax.all_gather(layer_out, "tp", axis=0, tiled=True).astype(jnp.float32)
            projected = norm_project(gathered, norm_gain[layer], both_weights)
        gated = (projected[:shard_channels] * jax.nn.sigmoid(projected[shard_channels:])).astype(
            jnp.bfloat16
        )
        earlier = shifted(gated[:, tokens_here - (K - 1) :], "sp", 1)
        extended = jnp.concatenate((earlier, gated), axis=1).astype(jnp.float32)
        filtered = depthwise(extended, conv_kernel[layer]) + conv_bias[layer][:, None]
        first_sum, square_sum = lax.psum(
            (
                jnp.sum(filtered, axis=0, keepdims=True),
                jnp.sum(filtered * filtered, axis=0, keepdims=True),
            ),
            "tp",
        )
        row_mean = first_sum / total_channels
        centred = filtered - row_mean
        spread = square_sum / total_channels - row_mean * row_mean
        activated = jax.nn.silu(
            centred * lax.rsqrt(spread + epsilon) * channel_gain[layer][:, None]
            + channel_bias[layer][:, None]
        ).astype(jnp.bfloat16)

        def accumulate(total, piece, start, weights=out_weight[layer]):
            weight_cols = lax.dynamic_slice_in_dim(weights, start, piece.shape[0], 1)
            return total + jnp.dot(weight_cols, piece, preferred_element_type=jnp.float32)

        zero_branch = jnp.zeros((shard_features, tokens_here), jnp.float32)
        branch = accumulate(
            zero_branch, lax.all_gather(activated, "tp", axis=0, tiled=True), jnp.int32(0)
        )
        layer_out = (current + branch).astype(jnp.bfloat16)
        current = layer_out.astype(jnp.float32)
    return layer_out


MESH = pl.DeviceIdType.MESH
LANES = 128
SUBLANES = 8
CHUNK = 256
HALO = 32
ROWS = 64
CORES = 2
PIECES = 4


def dot_nt(left, right):
    return lax.dot_general(
        left, right, (((1,), (1,)), ((), ())), preferred_element_type=jnp.float32
    )


def kernel(
    n_tp,
    n_sp,
    split,
    x_hbm,
    gain_hbm,
    taps_hbm,
    bias_hbm,
    chan_gain_hbm,
    chan_bias_hbm,
    wv_ref,
    wg_ref,
    ow_ref,
    out_ref,
    gain_ref,
    taps,
    bias_ref,
    chan,
    wp,
    wo,
    x_in,
    xg,
    ext,
    filt,
    norm_squares,
    scale,
    part,
    columns,
    halo_out,
    halo_in,
    stat,
    square,
    cf,
    ag,
    sg,
    accp,
    acco,
    res,
    small_sem,
    x_sem,
    wp_sem,
    wo_sem,
    y_sent,
    own_sent,
    f_sent,
    stat_sent,
    square_sent,
    chan_sent,
    halo_sent,
    chan_recv,
    halo_recv,
    stat_recv,
    square_recv,
    y_recv,
    own_recv,
    f_recv,
):
    tokens, width = x_in.shape
    chans = wv_ref.shape[1]
    feats = ow_ref.shape[1]
    total_chans = chans * n_tp
    n_y = n_tp // CORES
    piece = width // PIECES
    padded = stat.shape[-1]
    n_a, n_f = chans // CHUNK, feats // CHUNK
    groups = CHUNK // LANES
    spans = (
        ((split, tokens), (0, split)),
        ((split + HALO, tokens), (0, split + HALO)),
    )
    me = lax.axis_index("tp")
    sp = lax.axis_index("sp")
    my_y, core = me // CORES, me % CORES
    sibling = my_y * CORES + (1 - core)

    def tp_id(index):
        return {"tp": index}

    smalls = [
        pltpu.make_async_copy(source, target, small_sem.at[index])
        for index, (source, target) in enumerate((
            (gain_hbm, gain_ref),
            (taps_hbm, taps),
            (bias_hbm, bias_ref),
            (chan_gain_hbm, chan.at[my_y, 0]),
            (chan_bias_hbm, chan.at[my_y, 1]),
        ))
    ]

    def x_copy(index):
        cols = pl.ds(index * piece, piece)
        return pltpu.make_async_copy(x_hbm.at[:, cols], x_in.at[:, cols], x_sem.at[index])

    def proj_copies(layer, chunk, index=None):
        rows = pl.ds(chunk * CHUNK, CHUNK)
        cols = slice(None) if index is None else pl.ds(index * piece, piece)
        return [
            pltpu.make_async_copy(
                ref.at[layer, rows, cols],
                wp.at[layer, chunk, pl.ds(half * CHUNK, CHUNK), cols],
                wp_sem.at[layer * n_a + chunk] if index is None else x_sem.at[PIECES + index],
            )
            for half, ref in enumerate((wv_ref, wg_ref))
        ]

    def out_copy(layer):
        return pltpu.make_async_copy(ow_ref.at[layer], wo.at[layer], wo_sem.at[layer])

    smalls[0].start()
    for index in range(PIECES):
        x_copy(index).start()
        for copy in proj_copies(0, 0, index):
            copy.start()
    for copy in smalls[1:]:
        copy.start()

    barrier = pltpu.get_barrier_semaphore()
    for step in range(1, n_tp):
        pl.semaphore_signal(
            barrier, inc=1, device_id=tp_id(lax.rem(me + step, n_tp)), device_id_type=MESH
        )

    @pl.when(sp > 0)
    def _():
        pl.semaphore_signal(barrier, inc=1, device_id={"sp": sp - 1}, device_id_type=MESH)

    @pl.when(sp < n_sp - 1)
    def _():
        pl.semaphore_signal(barrier, inc=1, device_id={"sp": sp + 1}, device_id_type=MESH)

    part[...] = jnp.zeros(part.shape, jnp.float32)
    columns[...] = jnp.zeros(columns.shape, jnp.float32)

    def remote(source, target, send, recv, device):
        return pltpu.make_async_remote_copy(
            src_ref=source,
            dst_ref=target,
            send_sem=send,
            recv_sem=recv,
            device_id=tp_id(device),
            device_id_type=MESH,
        )

    def launch(copy):
        copy.start()

    def wait_bytes(ref, semaphore):
        pltpu.make_async_copy(ref, ref, semaphore).wait()

    def rows_of(span):
        return pl.ds(span[0], span[1] - span[0])

    def y_peer(step):
        return lax.rem(my_y + step, n_y)

    def y_origin(step):
        return lax.rem(my_y + n_y - step, n_y)

    def slot(phase, chunk):
        return phase * n_a + max(0, min(phase, 4) - 2) * (n_f - n_a) + chunk

    def y_copy(phase, ref, step, chunk):
        target = y_peer(step) * CORES + core
        return remote(
            ref, ref, y_sent.at[phase, step - 1], y_recv.at[slot(phase, chunk), step - 1], target
        )

    def f_copy(phase, buf, step, chunk, owner, span):
        ref = buf.at[owner, chunk, rows_of(span)]
        if step == 0:
            return remote(ref, ref, own_sent.at[phase], own_recv.at[phase], sibling)
        index = slot(phase, chunk)
        return remote(
            ref, ref, f_sent.at[phase, step - 1], f_recv.at[index, step - 1], sibling
        )

    def chan_copy(step, slot):
        target = y_peer(step) * CORES + core
        return remote(chan.at[slot], chan.at[slot], chan_sent.at[step - 1], chan_recv.at[step - 1], target)

    def prepare(index):
        gains = gain_ref[0:1, index * piece : (index + 1) * piece]
        for first_row in range(0, tokens, ROWS):
            rows = slice(first_row, first_row + ROWS)
            squares = norm_squares[rows, :] if index else None
            for lane in range(piece // LANES):
                here = slice(index * piece + lane * LANES, index * piece + (lane + 1) * LANES)
                values = x_in[rows, here].astype(jnp.float32)
                squares = values * values if squares is None else squares + values * values
                xg[rows, here] = (values * gains[:, lane * LANES : (lane + 1) * LANES]).astype(
                    jnp.bfloat16
                )
            norm_squares[rows, :] = squares

    def held(chunk):
        return slice(chunk * 2 * CHUNK, (chunk + 1) * 2 * CHUNK)

    def gate(chunk, first_row, count):
        rows = pl.ds(first_row, count)
        halved = scale[rows, :]
        start = chunk * 2 * CHUNK
        pieces = []
        for lane in range(groups):
            at = start + lane * LANES
            value = accp[rows, at : at + LANES] * halved
            gates = accp[rows, at + CHUNK : at + CHUNK + LANES] * halved
            gated = (value + value * jnp.tanh(gates)).astype(jnp.bfloat16)
            ext[chunk * groups + lane, pl.ds(first_row + HALO, count), :] = gated.astype(
                jnp.float32
            )
            pieces.append(gated)
        return pieces

    def gate_rows(chunk, start, stop):
        @pl.loop(0, (stop - start) // HALO)
        def _(block):
            gate(chunk, pl.multiple_of(start + block * HALO, HALO), HALO)

    def halo_copy(layer, chunk):
        return pltpu.make_async_remote_copy(
            src_ref=halo_out.at[layer, chunk],
            dst_ref=halo_in.at[layer, chunk],
            send_sem=halo_sent.at[layer],
            recv_sem=halo_recv.at[layer, chunk],
            device_id={"sp": lax.rem(sp + 1, n_sp)},
            device_id_type=MESH,
        )

    def send_halo(layer, chunk):
        for lane, gated in enumerate(gate(chunk, tokens - HALO, HALO)):
            halo_out[layer, chunk, :, lane * LANES : (lane + 1) * LANES] = gated

        @pl.when(sp < n_sp - 1)
        def _():
            halo_copy(layer, chunk).start()

    def receive_halo(layer, chunk):
        @pl.when(sp > 0)
        def _():
            halo_copy(layer, chunk).wait_recv()
            for lane in range(groups):
                ext[chunk * groups + lane, :HALO, :] = halo_in[
                    layer, chunk, :, lane * LANES : (lane + 1) * LANES
                ].astype(jnp.float32)

        @pl.when(sp == 0)
        def _():
            for lane in range(groups):
                ext[chunk * groups + lane, :HALO, :] = jnp.zeros((HALO, LANES), jnp.float32)

    def convolve(layer, half, chunk, start, stop):
        base = spans[layer][half][0]
        blocks = []
        while start < stop:
            count = min(ROWS, stop - start)
            blocks.append((start, count))
            start += count

        @pl.loop(chunk * groups, (chunk + 1) * groups)
        def _(lane):
            here = pl.ds(pl.multiple_of(lane * LANES, LANES), LANES)
            bias = bias_ref[layer : layer + 1, here]
            for first_row, count in blocks:
                tiles = count // SUBLANES
                sums = [jnp.broadcast_to(bias, (SUBLANES, LANES))] * tiles
                for residue in range(SUBLANES):
                    begin = first_row + HALO - K + 1 + residue
                    held_taps = range(residue, K, SUBLANES)
                    weights = [taps[tap, layer : layer + 1, here] for tap in held_taps]
                    for index in range(tiles + len(weights) - 1):
                        at = begin + index * SUBLANES
                        window = ext[lane, at : at + SUBLANES, :]
                        for step, weight in enumerate(weights):
                            tile = index - step
                            if 0 <= tile < tiles:
                                sums[tile] = sums[tile] + window * weight
                total = jnp.concatenate(sums, axis=0)
                filt[first_row : first_row + count, here] = total
                inner = slice(first_row - base, first_row - base + count)
                part[half, chunk, 0, inner, :] += total
                part[half, chunk, 1, inner, :] += total * total

    lane_index = lax.broadcasted_iota(jnp.int32, (HALO, LANES), 1)

    def centre(layer, half, chunk):
        start, stop = spans[layer][half]

        for block in range((stop - start) // HALO):
            inner = slice(block * HALO, (block + 1) * HALO)
            rows = slice(start + block * HALO, start + (block + 1) * HALO)
            mean = jnp.sum(part[half, chunk, 0, inner, :], axis=1, keepdims=True) / CHUNK
            squares = jnp.sum(part[half, chunk, 1, inner, :], axis=1, keepdims=True)
            for lane in range(groups):
                at = chunk * CHUNK + lane * LANES
                cf[layer, my_y, chunk, rows, lane * LANES : (lane + 1) * LANES] = (
                    filt[rows, at : at + LANES] - mean
                ).astype(jnp.bfloat16)
            packed = jnp.where(
                lane_index == chunk, mean, jnp.where(lane_index == n_a + chunk, squares, 0.0)
            )
            if chunk:
                packed = packed + columns[half, inner, :]
            columns[half, inner, :] = packed

    def send_centred(layer, half, phase, chunk):
        ref = cf.at[layer, my_y, chunk, rows_of(spans[layer][half])]
        for step in range(1, n_y):
            launch(y_copy(phase, ref, step, chunk))

    def stat_copy(layer, half, step, owner, target):
        ref = stat.at[layer, half, owner]
        index = layer * 2 + half
        return remote(ref, ref, stat_sent.at[index], stat_recv.at[index], target)

    def send_stats(layer, half):
        stat[layer, half, me] = jnp.transpose(columns[half])[:SUBLANES]
        for step in range(1, n_tp):
            launch(stat_copy(layer, half, step, me, lax.rem(me + step, n_tp)))

    def to_columns(rows):
        fill = jnp.zeros((LANES - rows.shape[0], padded), jnp.float32)
        return jnp.transpose(jnp.concatenate((rows, fill), axis=0))

    def settle(layer, half):
        wait_bytes(stat.at[layer, half, pl.ds(0, n_tp - 1)], stat_recv.at[layer * 2 + half])
        totals = jnp.sum(stat[layer, half], axis=0)
        mean_row = jnp.sum(totals[:n_a], axis=0, keepdims=True) * CHUNK / total_chans
        square_row = jnp.sum(totals[n_a : 2 * n_a], axis=0, keepdims=True) / total_chans
        rstd_row = lax.rsqrt(square_row - mean_row * mean_row + epsilon)
        rows = [rstd_row]
        for step in range(n_y):
            means = stat[layer, half, y_origin(step) * CORES + core]
            rows.append((means[:n_a] - mean_row) * rstd_row)
        columns[half] = to_columns(jnp.concatenate(rows, axis=0))

    def activate(layer, half, step, chunk):
        start, stop = spans[layer][half]
        origin = y_origin(step)
        owner = origin * CORES + core

        at = 1 + step * n_a + chunk
        gains = 0.5 * chan[origin, 0, layer : layer + 1, chunk * CHUNK : (chunk + 1) * CHUNK]
        biases = 0.5 * chan[origin, 1, layer : layer + 1, chunk * CHUNK : (chunk + 1) * CHUNK]
        for block in range((stop - start) // HALO):
            inner = slice(block * HALO, (block + 1) * HALO)
            rows = slice(start + block * HALO, start + (block + 1) * HALO)
            rstd = jnp.broadcast_to(columns[half, inner, 0:1], (HALO, LANES))
            shift = jnp.broadcast_to(columns[half, inner, at : at + 1], (HALO, LANES))
            for lane in range(groups):
                cols = slice(lane * LANES, (lane + 1) * LANES)
                values = cf[layer, origin, chunk, rows, cols].astype(jnp.float32) * rstd + shift
                values = values * gains[:, cols] + biases[:, cols]
                ag[layer, owner, chunk, rows, cols] = (values + values * jnp.tanh(values)).astype(
                    jnp.bfloat16
                )

    def own_activated(layer, half, phase):
        for chunk in range(n_a):
            activate(layer, half, 0, chunk)
            launch(f_copy(phase, ag.at[layer], 0, chunk, me, spans[layer][half]))

    def arrive(layer, half, phase, chunk):
        for step in range(1, n_y):
            owner = y_origin(step) * CORES + core
            ref = cf.at[layer, y_origin(step), chunk, rows_of(spans[layer][half])]
            y_copy(phase, ref, step, chunk).wait_recv()
            activate(layer, half, step, chunk)
            launch(f_copy(phase, ag.at[layer], step, chunk, owner, spans[layer][half]))

    def from_next_door(layer, half, phase):
        rows = rows_of(spans[layer][half])
        wait_bytes(ag.at[layer, sibling, :, rows], own_recv.at[phase])

    def from_sibling(layer, half, phase, chunk, step):
        owner = y_origin(step) * CORES + 1 - core
        f_copy(phase, ag.at[layer], step, chunk, owner, spans[layer][half]).wait_recv()

    def mix(layer, half, parts, first=False, last=False):
        rows = slice(*spans[layer][half])
        if not first:
            total = acco[rows, :]
        elif layer == 0:
            total = x_in[rows, pl.ds(pl.multiple_of(me * feats, LANES), feats)].astype(jnp.float32)
        else:
            total = res[rows, :]
        for owner, chunk in parts:
            start = pl.multiple_of(owner * chans + chunk * CHUNK, LANES)
            total = total + dot_nt(
                ag[layer, owner, chunk, rows, :], wo[layer, :, pl.ds(start, CHUNK)]
            )
        if last:
            out_ref[rows, :] = total.astype(jnp.bfloat16)
        else:
            acco[rows, :] = total

    everything = range(n_a)
    others = range(1, n_y)

    def own(chunks):
        return [(me, chunk) for chunk in chunks]

    def next_door(chunks):
        return [(sibling, chunk) for chunk in chunks]

    def across(chunks):
        return [(y_origin(step) * CORES + core, chunk) for step in others for chunk in chunks]

    def relayed(chunks):
        return [(y_origin(step) * CORES + 1 - core, chunk) for step in others for chunk in chunks]

    def branch_start(layer, half, phase):
        own_activated(layer, half, phase)
        for chunk in everything[:-1]:
            arrive(layer, half, phase, chunk)
        mix(layer, half, own(everything) + across(everything[:-1]), True)
        from_next_door(layer, half, phase)

    def branch_end(layer, half, phase):
        mix(layer, half, next_door(everything))
        arrive(layer, half, phase, n_a - 1)
        for step in others:
            for chunk in everything[:-1]:
                from_sibling(layer, half, phase, chunk, step)
        mix(layer, half, across(everything[-1:]) + relayed(everything[:-1]))
        for step in others:
            from_sibling(layer, half, phase, n_a - 1, step)

    def sent_branch(layer, half, phase):
        rows = rows_of(spans[layer][half])
        wait_bytes(ag.at[layer, me, :, rows], own_sent.at[phase])
        wait_bytes(stat.at[layer, half, pl.ds(0, n_tp - 1)], stat_sent.at[layer * 2 + half])
        for step in others:
            owner = y_origin(step) * CORES + core
            wait_bytes(cf.at[layer, my_y, :, rows], y_sent.at[phase, step - 1])
            wait_bytes(ag.at[layer, owner, :, rows], f_sent.at[phase, step - 1])

    def sent_stream(half):
        rows = rows_of(spans[0][half])
        wait_bytes(sg.at[me, :, rows], own_sent.at[2 + half])
        wait_bytes(square.at[half, pl.ds(0, n_tp - 1)], square_sent.at[half])
        for step in others:
            owner = y_origin(step) * CORES + core
            wait_bytes(sg.at[me, :, rows], y_sent.at[2 + half, step - 1])
            wait_bytes(sg.at[owner, :, rows], f_sent.at[2 + half, step - 1])

    def square_copy(half, step, owner, target):
        ref = square.at[half, owner]
        return remote(ref, ref, square_sent.at[half], square_recv.at[half], target)

    def send_stream(half):
        span = spans[0][half]
        rows = slice(*span)
        squares = jnp.zeros((span[1] - span[0], LANES), jnp.float32)
        for lead in ((0, 1), (1, n_f)):
            block = slice(lead[0] * CHUNK, lead[1] * CHUNK)
            total = acco[rows, block]
            for owner, last in relayed(everything[-1:]):
                start = pl.multiple_of(owner * chans + last * CHUNK, LANES)
                total = total + dot_nt(
                    ag[0, owner, last, rows, :], wo[0, block, pl.ds(start, CHUNK)]
                )
            rounded = total.astype(jnp.bfloat16).astype(jnp.float32)
            res[rows, block] = rounded
            for chunk in range(*lead):
                first = pl.multiple_of(me * feats + chunk * CHUNK, LANES)
                at = (chunk - lead[0]) * CHUNK
                values = rounded[:, at : at + CHUNK]
                sg[me, chunk, rows, :] = (values * gain_ref[1:2, pl.ds(first, CHUNK)]).astype(
                    jnp.bfloat16
                )
                for lane in range(groups):
                    part = values[:, lane * LANES : (lane + 1) * LANES]
                    squares = squares + part * part
                if chunk == n_f - 1:
                    send_squares(half, squares)
                ref = sg.at[me, chunk, rows_of(span)]
                for step in others:
                    launch(y_copy(2 + half, ref, step, chunk))
                launch(f_copy(2 + half, sg, 0, chunk, me, span))

    def send_squares(half, squares):
        span = spans[0][half]
        count = span[1] - span[0]
        if count < padded:
            fill = jnp.zeros((padded - count, LANES), jnp.float32)
            squares = jnp.concatenate((squares, fill), axis=0)
        row = jnp.sum(jnp.transpose(squares), axis=0, keepdims=True)
        square[half, me] = jnp.broadcast_to(row, (SUBLANES, padded))
        for step in range(1, n_tp):
            launch(square_copy(half, step, me, lax.rem(me + step, n_tp)))

    def rescale(half):
        wait_bytes(square.at[half, pl.ds(0, n_tp - 1)], square_recv.at[half])
        totals = jnp.sum(square[half], axis=0)[0:1] / width
        start, stop = spans[0][half]
        spread = jnp.transpose(
            jnp.broadcast_to(0.5 * lax.rsqrt(totals + epsilon), (LANES, padded))
        )
        scale[start:stop, :] = spread[: stop - start]

    def project(half, owner, chunks, first, blocks=None):
        rows = slice(*spans[0][half])
        for block in range(n_a) if blocks is None else blocks:
            total = None if first else accp[rows, held(block)]
            for chunk in chunks:
                start = pl.multiple_of(owner * feats + chunk * CHUNK, LANES)
                product = dot_nt(
                    sg[owner, chunk, rows, :], wp[1, block, :, pl.ds(start, CHUNK)]
                )
                total = product if total is None else total + product
            accp[rows, held(block)] = total

    def own_stream(half):
        project(half, me, range(n_f), True)

    def sibling_stream(half):
        wait_bytes(sg.at[sibling, :, rows_of(spans[0][half])], own_recv.at[2 + half])
        project(half, sibling, range(n_f), False)

    def arrive_stream(half, chunk):
        for step in range(1, n_y):
            origin = y_origin(step)
            owner = origin * CORES + core
            ref = sg.at[owner, chunk, rows_of(spans[0][half])]
            y_copy(2 + half, ref, step, chunk).wait_recv()
            launch(f_copy(2 + half, sg, step, chunk, owner, spans[0][half]))
            project(half, owner, (chunk,), False)

    def relayed_stream(half, chunk, blocks=None):
        for step in others:
            owner = y_origin(step) * CORES + 1 - core
            if blocks is None or blocks[0] == 0:
                f_copy(2 + half, sg, step, chunk, owner, spans[0][half]).wait_recv()
            project(half, owner, (chunk,), False, blocks)

    smalls[0].wait()
    x_copy(0).wait()
    prepare(0)
    for index in range(PIECES):
        cols = slice(index * piece, (index + 1) * piece)
        for copy in proj_copies(0, 0, index):
            copy.wait()
        if index < PIECES - 1:
            x_copy(index + 1).wait()
        if index == PIECES // 2:
            for chunk in range(1, n_a):
                for copy in proj_copies(0, chunk):
                    copy.start()
        product = dot_nt(xg[:, cols], wp[0, 0, :, cols])
        if index < PIECES - 1:
            prepare(index + 1)
        if index:
            accp[:, held(0)] += product
        else:
            accp[:, held(0)] = product

    for first_row in range(0, tokens, ROWS):
        rows = slice(first_row, first_row + ROWS)
        scaling = lax.rsqrt(jnp.sum(norm_squares[rows, :], axis=1, keepdims=True) / width + epsilon)
        scale[rows, :] = jnp.broadcast_to(0.5 * scaling, (ROWS, LANES))

    for copy in smalls[1:]:
        copy.wait()
    pl.semaphore_wait(
        barrier,
        n_tp - 1 + jnp.where(sp > 0, 1, 0) + jnp.where(sp < n_sp - 1, 1, 0),
    )

    for chunk in everything:
        if chunk:
            for copy in proj_copies(0, chunk):
                copy.wait()
            accp[:, held(chunk)] = dot_nt(xg[...], wp[0, chunk])
        send_halo(0, chunk)
        gate_rows(chunk, 0, tokens - HALO)
        convolve(0, 0, chunk, *spans[0][0])
        centre(0, 0, chunk)
        if chunk == n_a - 1:
            send_stats(0, 0)
        send_centred(0, 0, 0, chunk)
        if chunk == 0:
            for step in others:
                launch(chan_copy(step, my_y))
    out_copy(0).start()
    for chunk in everything:
        convolve(0, 1, chunk, ROWS, spans[0][1][1])
        receive_halo(0, chunk)
        convolve(0, 1, chunk, 0, ROWS)
        centre(0, 1, chunk)
        if chunk == n_a - 1:
            send_stats(0, 1)
        send_centred(0, 1, 1, chunk)
    for chunk in everything:
        for copy in proj_copies(1, chunk):
            copy.start()
    out_copy(1).start()
    for step in others:
        chan_copy(step, y_origin(step)).wait_recv()
    out_copy(0).wait()
    settle(0, 0)
    branch_start(0, 0, 0)
    branch_end(0, 0, 0)
    send_stream(0)
    settle(0, 1)
    branch_start(0, 1, 1)
    branch_end(0, 1, 1)
    send_stream(1)
    part[...] = jnp.zeros(part.shape, jnp.float32)
    for chunk in everything:
        for copy in proj_copies(1, chunk):
            copy.wait()
    own_stream(0)
    sibling_stream(0)
    for chunk in range(n_f):
        if chunk == 1:
            own_stream(1)
        if chunk == 2:
            sibling_stream(1)
        if chunk == n_f - 1:
            sent_branch(0, 0, 0)
            sent_branch(0, 1, 1)
            rescale(0)
        arrive_stream(0, chunk)
        if chunk:
            relayed_stream(0, chunk - 1)
    for chunk in everything:
        relayed_stream(0, n_f - 1, (chunk,))
        send_halo(1, chunk)
        gate_rows(chunk, split, tokens - HALO)
        convolve(1, 0, chunk, *spans[1][0])
        centre(1, 0, chunk)
    send_stats(1, 0)
    for chunk in everything:
        send_centred(1, 0, 4, chunk)
    for chunk in range(n_f):
        if chunk == n_f - 1:
            rescale(1)
        arrive_stream(1, chunk)
        if chunk:
            relayed_stream(1, chunk - 1)
    for chunk in everything:
        relayed_stream(1, n_f - 1, (chunk,))
        gate_rows(chunk, 0, split)
        convolve(1, 1, chunk, HALO, spans[1][1][1])
        receive_halo(1, chunk)
        convolve(1, 1, chunk, 0, HALO)
        centre(1, 1, chunk)
        if chunk == n_a - 1:
            send_stats(1, 1)
        send_centred(1, 1, 5, chunk)
    out_copy(1).wait()
    settle(1, 0)
    own_activated(1, 0, 4)
    for chunk in everything:
        arrive(1, 0, 4, chunk)
    mix(1, 0, own(everything) + across(everything), True)
    from_next_door(1, 0, 4)
    for chunk in everything:
        for step in others:
            from_sibling(1, 0, 4, chunk, step)
    mix(1, 0, next_door(everything) + relayed(everything), False, True)
    sent_stream(0)
    sent_stream(1)
    settle(1, 1)
    branch_start(1, 1, 5)
    sent_branch(1, 0, 4)
    branch_end(1, 1, 5)
    mix(1, 1, relayed(everything[-1:]), False, True)

    @pl.when(sp < n_sp - 1)
    def _():
        for layer in range(LAYERS):
            wait_bytes(halo_out.at[layer], halo_sent.at[layer])

    sent_branch(1, 1, 5)
    for step in others:
        wait_bytes(chan.at[my_y], chan_sent.at[step - 1])


def fused(mesh, stream, norm_gain, value_weight, gate_weight, conv_kernel, conv_bias,
          channel_gain, channel_bias, out_weight):
    n_tp, n_sp = mesh.shape["tp"], mesh.shape["sp"]
    width, tokens = stream.shape
    chans, feats = value_weight.shape[1], out_weight.shape[1]
    split = (tokens // 2 - HALO) // HALO * HALO
    n_y = n_tp // CORES
    n_a, n_f = chans // CHUNK, feats // CHUNK
    fits = (
        n_tp % CORES == 0
        and chans % CHUNK == 0
        and feats % CHUNK == 0
        and width % (PIECES * CHUNK) == 0
        and tokens % ROWS == 0
        and split % ROWS == 0
        and tokens >= 4 * ROWS
        and LAYERS == 2
        and n_tp <= 8
        and 2 * n_a <= SUBLANES
        and 1 + n_y * n_a <= LANES
    )
    if not fits:
        return local(stream, norm_gain, value_weight, gate_weight, conv_kernel, conv_bias,
                     channel_gain, channel_bias, out_weight)
    padded = -(-(tokens - split) // LANES) * LANES
    f32, bf16 = jnp.float32, jnp.bfloat16
    dma = pltpu.SemaphoreType.DMA
    out = pl.pallas_call(
        functools.partial(kernel, n_tp, n_sp, split),
        out_shape=jax.ShapeDtypeStruct((tokens, feats), bf16),
        in_specs=[pl.BlockSpec(memory_space=pl.ANY)] * 9,
        out_specs=pl.BlockSpec(memory_space=pltpu.VMEM),
        scratch_shapes=[
            pltpu.VMEM((LAYERS, width), f32),
            pltpu.VMEM((K, LAYERS, chans), f32),
            pltpu.VMEM((LAYERS, chans), f32),
            pltpu.VMEM((n_y, 2, LAYERS, chans), f32),
            pltpu.VMEM((LAYERS, n_a, 2 * CHUNK, width), bf16),
            pltpu.VMEM((LAYERS, feats, chans * n_tp), bf16),
            pltpu.VMEM((tokens, width), bf16),
            pltpu.VMEM((tokens, width), bf16),
            pltpu.VMEM((chans // LANES, HALO + tokens, LANES), f32),
            pltpu.VMEM((tokens, chans), f32),
            pltpu.VMEM((tokens, LANES), f32),
            pltpu.VMEM((tokens, LANES), f32),
            pltpu.VMEM((2, n_a, 2, padded, LANES), f32),
            pltpu.VMEM((2, padded, LANES), f32),
            pltpu.VMEM((LAYERS, n_a, HALO, CHUNK), bf16),
            pltpu.VMEM((LAYERS, n_a, HALO, CHUNK), bf16),
            pltpu.VMEM((LAYERS, 2, n_tp, SUBLANES, padded), f32),
            pltpu.VMEM((2, n_tp, SUBLANES, padded), f32),
            pltpu.VMEM((LAYERS, n_y, n_a, tokens, CHUNK), bf16),
            pltpu.VMEM((LAYERS, n_tp, n_a, tokens, CHUNK), bf16),
            pltpu.VMEM((n_tp, n_f, tokens, CHUNK), bf16),
            pltpu.VMEM((tokens, 2 * chans), f32),
            pltpu.VMEM((tokens, feats), f32),
            pltpu.VMEM((tokens, feats), f32),
            dma((5,)),
            dma((2 * PIECES,)),
            dma((LAYERS * n_a,)),
            dma((LAYERS,)),
            dma((6, n_y - 1)),
            dma((6,)),
            dma((6, n_y - 1)),
            dma((LAYERS * 2,)),
            dma((2,)),
            dma((n_y - 1,)),
            dma((LAYERS,)),
            dma((n_y - 1,)),
            dma((LAYERS, n_a)),
            dma((LAYERS * 2,)),
            dma((2,)),
            dma((4 * n_a + 2 * n_f, n_y - 1)),
            dma((6,)),
            dma((4 * n_a + 2 * n_f, n_y - 1)),
        ],
        compiler_params=pltpu.CompilerParams(
            collective_id=0, has_side_effects=True, vmem_limit_bytes=50 * 1024 * 1024
        ),
    )(*(
        pltpu.with_memory_space_constraint(value, pltpu.HBM)
        for value in (
            stream.T, norm_gain, jnp.transpose(conv_kernel, (2, 0, 1)), conv_bias, channel_gain,
            channel_bias, value_weight, gate_weight, out_weight,
        )
    ))
    return out.T


def solution(mesh):
    placed = (
        P(None, ("grp", "sp")),
        P(),
        P(None, "tp", None),
        P(None, "tp", None),
        P(None, "tp", None),
        P(None, "tp"),
        P(None, "tp"),
        P(None, "tp"),
        P(None, "tp", None),
    )
    return jax.shard_map(
        functools.partial(fused, mesh), mesh=mesh, in_specs=placed, out_specs=P("tp", ("grp", "sp")), check_vma=False
    )
```

```python
import functools

import jax
import jax.numpy as jnp
from jax import lax
from jax.experimental import pallas as pl
from jax.experimental.pallas import tpu as pltpu
from jax.sharding import PartitionSpec as P

K = 31
LAYERS = 2


epsilon = 1e-06


def shifted(value, axis, steps):
    count = lax.axis_size(axis)
    initial, last = (max(0, -steps), min(count, count - steps))
    return lax.ppermute(value, axis, [(source, source + steps) for source in range(initial, last)])


def depthwise(signal, kernel):
    out = lax.conv_general_dilated(
        signal[None],
        kernel[:, None, :],
        (1,),
        [(0, 0)],
        dimension_numbers=("NCW", "OIW", "NCW"),
        feature_group_count=kernel.shape[0],
        precision=lax.Precision.HIGHEST,
    )
    return out[0]


def norm_project(whole, gain, weights):
    scaling = lax.rsqrt(jnp.mean(whole * whole, axis=0, keepdims=True) + epsilon)
    normed = (whole * scaling * gain[:, None]).astype(jnp.bfloat16)
    return jnp.dot(weights, normed, preferred_element_type=jnp.float32)


def local(
    stream,
    norm_gain,
    value_weight,
    gate_weight,
    conv_kernel,
    conv_bias,
    channel_gain,
    channel_bias,
    out_weight,
):
    shard_channels = value_weight.shape[1]
    total_channels = shard_channels * lax.axis_size("tp")
    shard_features = out_weight.shape[1]
    tokens_here = stream.shape[1]
    row_start = lax.axis_index("tp") * shard_features
    whole = stream.astype(jnp.float32)
    current = lax.dynamic_slice_in_dim(whole, row_start, shard_features, 0)
    layer_out = stream
    for layer in range(LAYERS):
        both_weights = jnp.concatenate((value_weight[layer], gate_weight[layer]), axis=0)
        if layer == 0:
            projected = norm_project(whole, norm_gain[layer], both_weights)
        else:
            gathered = lax.all_gather(layer_out, "tp", axis=0, tiled=True).astype(jnp.float32)
            projected = norm_project(gathered, norm_gain[layer], both_weights)
        gated = (projected[:shard_channels] * jax.nn.sigmoid(projected[shard_channels:])).astype(
            jnp.bfloat16
        )
        earlier = shifted(gated[:, tokens_here - (K - 1) :], "sp", 1)
        extended = jnp.concatenate((earlier, gated), axis=1).astype(jnp.float32)
        filtered = depthwise(extended, conv_kernel[layer]) + conv_bias[layer][:, None]
        first_sum, square_sum = lax.psum(
            (
                jnp.sum(filtered, axis=0, keepdims=True),
                jnp.sum(filtered * filtered, axis=0, keepdims=True),
            ),
            "tp",
        )
        row_mean = first_sum / total_channels
        centred = filtered - row_mean
        spread = square_sum / total_channels - row_mean * row_mean
        activated = jax.nn.silu(
            centred * lax.rsqrt(spread + epsilon) * channel_gain[layer][:, None]
            + channel_bias[layer][:, None]
        ).astype(jnp.bfloat16)

        def accumulate(total, piece, start, weights=out_weight[layer]):
            weight_cols = lax.dynamic_slice_in_dim(weights, start, piece.shape[0], 1)
            return total + jnp.dot(weight_cols, piece, preferred_element_type=jnp.float32)

        zero_branch = jnp.zeros((shard_features, tokens_here), jnp.float32)
        branch = accumulate(
            zero_branch, lax.all_gather(activated, "tp", axis=0, tiled=True), jnp.int32(0)
        )
        layer_out = (current + branch).astype(jnp.bfloat16)
        current = layer_out.astype(jnp.float32)
    return layer_out


MESH = pl.DeviceIdType.MESH
LANES = 128
SUBLANES = 8
CHUNK = 256
HALO = 32
ROWS = 64
CORES = 2
PIECES = 4


def dot_nt(left, right):
    return lax.dot_general(
        left, right, (((1,), (1,)), ((), ())), preferred_element_type=jnp.float32
    )


def kernel(
    n_tp,
    n_sp,
    split,
    x_hbm,
    gain_hbm,
    taps_hbm,
    bias_hbm,
    chan_gain_hbm,
    chan_bias_hbm,
    wv_ref,
    wg_ref,
    ow_ref,
    out_ref,
    gain_ref,
    taps,
    bias_ref,
    chan,
    wp,
    wo,
    x_in,
    xg,
    ext,
    filt,
    norm_squares,
    scale,
    part,
    columns,
    halo_out,
    halo_in,
    stat,
    square,
    cf,
    ag,
    sg,
    accp,
    acco,
    res,
    small_sem,
    x_sem,
    wp_sem,
    wo_sem,
    sent,
    stat_sent,
    square_sent,
    chan_sent,
    halo_sent,
    chan_recv,
    halo_recv,
    stat_recv,
    square_recv,
    y_recv,
    own_recv,
    f_recv,
):
    tokens, width = x_in.shape
    chans = wv_ref.shape[1]
    feats = ow_ref.shape[1]
    total_chans = chans * n_tp
    n_y = n_tp // CORES
    piece = width // PIECES
    padded = stat.shape[-1]
    stat_rows = stat.shape[-2]
    n_a, n_f = chans // CHUNK, feats // CHUNK
    groups = CHUNK // LANES
    spans = (
        ((split, tokens), (0, split)),
        ((split + HALO, tokens), (0, split + HALO)),
    )
    me = lax.axis_index("tp")
    sp = lax.axis_index("sp")
    my_y, core = me // CORES, me % CORES
    sibling = my_y * CORES + (1 - core)

    def tp_id(index):
        return {"tp": index}

    smalls = [
        pltpu.make_async_copy(source, target, small_sem.at[index])
        for index, (source, target) in enumerate((
            (gain_hbm, gain_ref),
            (taps_hbm, taps),
            (bias_hbm, bias_ref),
            (chan_gain_hbm, chan.at[my_y, 0]),
            (chan_bias_hbm, chan.at[my_y, 1]),
        ))
    ]

    def x_copy(index):
        cols = pl.ds(index * piece, piece)
        return pltpu.make_async_copy(x_hbm.at[:, cols], x_in.at[:, cols], x_sem.at[index])

    def proj_copies(layer, chunk, index=None):
        rows = pl.ds(chunk * CHUNK, CHUNK)
        cols = slice(None) if index is None else pl.ds(index * piece, piece)
        return [
            pltpu.make_async_copy(
                ref.at[layer, rows, cols],
                wp.at[layer, chunk, pl.ds(half * CHUNK, CHUNK), cols],
                wp_sem.at[layer * n_a + chunk] if index is None else x_sem.at[PIECES + index],
            )
            for half, ref in enumerate((wv_ref, wg_ref))
        ]

    def out_copy(layer):
        return pltpu.make_async_copy(ow_ref.at[layer], wo.at[layer], wo_sem.at[layer])

    smalls[0].start()
    for index in range(PIECES):
        x_copy(index).start()
        for copy in proj_copies(0, 0, index):
            copy.start()
    for copy in smalls[1:]:
        copy.start()

    barrier = pltpu.get_barrier_semaphore()
    for step in range(1, n_tp):
        pl.semaphore_signal(
            barrier, inc=1, device_id=tp_id(lax.rem(me + step, n_tp)), device_id_type=MESH
        )

    @pl.when(sp > 0)
    def _():
        pl.semaphore_signal(barrier, inc=1, device_id={"sp": sp - 1}, device_id_type=MESH)

    @pl.when(sp < n_sp - 1)
    def _():
        pl.semaphore_signal(barrier, inc=1, device_id={"sp": sp + 1}, device_id_type=MESH)

    part[...] = jnp.zeros(part.shape, jnp.float32)
    columns[...] = jnp.zeros(columns.shape, jnp.float32)

    def remote(source, target, send, recv, device):
        return pltpu.make_async_remote_copy(
            src_ref=source,
            dst_ref=target,
            send_sem=send,
            recv_sem=recv,
            device_id=tp_id(device),
            device_id_type=MESH,
        )

    def launch(copy):
        copy.start()

    def wait_bytes(ref, semaphore):
        pltpu.make_async_copy(ref, ref, semaphore).wait()

    def rows_of(span):
        return pl.ds(span[0], span[1] - span[0])

    def columns_of(span):
        return pl.ds(0, -(-(span[1] - span[0]) // LANES) * LANES)

    def stats_of(layer, half):
        return stat.at[layer, half, pl.ds(0, n_tp - 1), :, columns_of(spans[layer][half])]

    def squares_of(half):
        return square.at[half, pl.ds(0, n_tp - 1), :, columns_of(spans[0][half])]

    def y_peer(step):
        return lax.rem(my_y + step, n_y)

    def y_origin(step):
        return lax.rem(my_y + n_y - step, n_y)

    def slot(phase, chunk):
        return phase * n_a + max(0, min(phase, 4) - 2) * (n_f - n_a) + chunk

    def y_copy(phase, ref, step, chunk):
        target = y_peer(step) * CORES + core
        return remote(
            ref, ref, sent.at[phase], y_recv.at[slot(phase, chunk), step - 1], target
        )

    def f_copy(phase, buf, step, chunk, owner, span):
        ref = buf.at[owner, chunk, rows_of(span)]
        if step == 0:
            return remote(ref, ref, sent.at[phase], own_recv.at[phase], sibling)
        index = slot(phase, chunk)
        return remote(
            ref, ref, sent.at[phase], f_recv.at[index, step - 1], sibling
        )

    def chan_copy(step, slot):
        target = y_peer(step) * CORES + core
        return remote(chan.at[slot], chan.at[slot], chan_sent.at[step - 1], chan_recv.at[step - 1], target)

    def prepare(index):
        gains = gain_ref[0:1, index * piece : (index + 1) * piece]
        for first_row in range(0, tokens, ROWS):
            rows = slice(first_row, first_row + ROWS)
            squares = norm_squares[rows, :] if index else None
            for lane in range(piece // LANES):
                here = slice(index * piece + lane * LANES, index * piece + (lane + 1) * LANES)
                values = x_in[rows, here].astype(jnp.float32)
                squares = values * values if squares is None else squares + values * values
                xg[rows, here] = (values * gains[:, lane * LANES : (lane + 1) * LANES]).astype(
                    jnp.bfloat16
                )
            norm_squares[rows, :] = squares

    def held(chunk):
        return slice(chunk * 2 * CHUNK, (chunk + 1) * 2 * CHUNK)

    def gate(chunk, first_row, count):
        rows = pl.ds(first_row, count)
        halved = scale[rows, :]
        start = chunk * 2 * CHUNK
        pieces = []
        for lane in range(groups):
            at = start + lane * LANES
            value = accp[rows, at : at + LANES] * halved
            gates = accp[rows, at + CHUNK : at + CHUNK + LANES] * halved
            gated = (value + value * jnp.tanh(gates)).astype(jnp.bfloat16)
            ext[chunk * groups + lane, pl.ds(first_row + HALO, count), :] = gated.astype(
                jnp.float32
            )
            pieces.append(gated)
        return pieces

    def gate_rows(chunk, start, stop):
        @pl.loop(0, (stop - start) // HALO)
        def _(block):
            gate(chunk, pl.multiple_of(start + block * HALO, HALO), HALO)

    def halo_copy(layer, chunk):
        return pltpu.make_async_remote_copy(
            src_ref=halo_out.at[layer, chunk],
            dst_ref=halo_in.at[layer, chunk],
            send_sem=halo_sent.at[layer],
            recv_sem=halo_recv.at[layer, chunk],
            device_id={"sp": lax.rem(sp + 1, n_sp)},
            device_id_type=MESH,
        )

    def send_halo(layer, chunk):
        for lane, gated in enumerate(gate(chunk, tokens - HALO, HALO)):
            halo_out[layer, chunk, :, lane * LANES : (lane + 1) * LANES] = gated

        @pl.when(sp < n_sp - 1)
        def _():
            halo_copy(layer, chunk).start()

    def receive_halo(layer, chunk):
        @pl.when(sp > 0)
        def _():
            halo_copy(layer, chunk).wait_recv()
            for lane in range(groups):
                ext[chunk * groups + lane, :HALO, :] = halo_in[
                    layer, chunk, :, lane * LANES : (lane + 1) * LANES
                ].astype(jnp.float32)

        @pl.when(sp == 0)
        def _():
            for lane in range(groups):
                ext[chunk * groups + lane, :HALO, :] = jnp.zeros((HALO, LANES), jnp.float32)

    def convolve(layer, half, chunk, start, stop):
        base = spans[layer][half][0]
        blocks = []
        while start < stop:
            count = min(ROWS, stop - start)
            blocks.append((start, count))
            start += count

        @pl.loop(chunk * groups, (chunk + 1) * groups)
        def _(lane):
            here = pl.ds(pl.multiple_of(lane * LANES, LANES), LANES)
            bias = bias_ref[layer : layer + 1, here]
            for first_row, count in blocks:
                tiles = count // SUBLANES
                sums = [jnp.broadcast_to(bias, (SUBLANES, LANES))] * tiles
                for residue in range(SUBLANES):
                    begin = first_row + HALO - K + 1 + residue
                    held_taps = range(residue, K, SUBLANES)
                    weights = [taps[tap, layer : layer + 1, here] for tap in held_taps]
                    for index in range(tiles + len(weights) - 1):
                        at = begin + index * SUBLANES
                        window = ext[lane, at : at + SUBLANES, :]
                        for step, weight in enumerate(weights):
                            tile = index - step
                            if 0 <= tile < tiles:
                                sums[tile] = sums[tile] + window * weight
                total = jnp.concatenate(sums, axis=0)
                filt[first_row : first_row + count, here] = total
                inner = slice(first_row - base, first_row - base + count)
                part[half, chunk, 0, inner, :] += total
                part[half, chunk, 1, inner, :] += total * total

    lane_index = lax.broadcasted_iota(jnp.int32, (HALO, LANES), 1)

    def centre(layer, half, chunk):
        start, stop = spans[layer][half]

        for block in range((stop - start) // HALO):
            inner = slice(block * HALO, (block + 1) * HALO)
            rows = slice(start + block * HALO, start + (block + 1) * HALO)
            mean = jnp.sum(part[half, chunk, 0, inner, :], axis=1, keepdims=True) / CHUNK
            squares = jnp.sum(part[half, chunk, 1, inner, :], axis=1, keepdims=True)
            for lane in range(groups):
                at = chunk * CHUNK + lane * LANES
                cf[layer, my_y, chunk, rows, lane * LANES : (lane + 1) * LANES] = (
                    filt[rows, at : at + LANES] - mean
                ).astype(jnp.bfloat16)
            packed = jnp.where(
                lane_index == chunk, mean, jnp.where(lane_index == n_a + chunk, squares, 0.0)
            )
            if chunk:
                packed = packed + columns[half, inner, :]
            columns[half, inner, :] = packed

    def send_centred(layer, half, phase, chunk):
        ref = cf.at[layer, my_y, chunk, rows_of(spans[layer][half])]
        for step in range(1, n_y):
            launch(y_copy(phase, ref, step, chunk))

    def stat_copy(layer, half, step, owner, target):
        ref = stat.at[layer, half, owner, :, columns_of(spans[layer][half])]
        index = layer * 2 + half
        return remote(ref, ref, stat_sent.at[index], stat_recv.at[index], target)

    def send_stats(layer, half):
        stat[layer, half, me] = jnp.transpose(columns[half])[:stat_rows]
        for step in range(1, n_tp):
            launch(stat_copy(layer, half, step, me, lax.rem(me + step, n_tp)))

    def to_columns(rows):
        fill = jnp.zeros((LANES - rows.shape[0], padded), jnp.float32)
        return jnp.transpose(jnp.concatenate((rows, fill), axis=0))

    def settle(layer, half):
        wait_bytes(stats_of(layer, half), stat_recv.at[layer * 2 + half])
        totals = jnp.sum(stat[layer, half], axis=0)
        mean_row = jnp.sum(totals[:n_a], axis=0, keepdims=True) * CHUNK / total_chans
        square_row = jnp.sum(totals[n_a : 2 * n_a], axis=0, keepdims=True) / total_chans
        rstd_row = lax.rsqrt(square_row - mean_row * mean_row + epsilon)
        rows = [rstd_row]
        for step in range(n_y):
            means = stat[layer, half, y_origin(step) * CORES + core]
            rows.append((means[:n_a] - mean_row) * rstd_row)
        columns[half] = to_columns(jnp.concatenate(rows, axis=0))

    def activate(layer, half, step, chunk):
        start, stop = spans[layer][half]
        origin = y_origin(step)
        owner = origin * CORES + core

        at = 1 + step * n_a + chunk
        gains = 0.5 * chan[origin, 0, layer : layer + 1, chunk * CHUNK : (chunk + 1) * CHUNK]
        biases = 0.5 * chan[origin, 1, layer : layer + 1, chunk * CHUNK : (chunk + 1) * CHUNK]
        for block in range((stop - start) // HALO):
            inner = slice(block * HALO, (block + 1) * HALO)
            rows = slice(start + block * HALO, start + (block + 1) * HALO)
            rstd = jnp.broadcast_to(columns[half, inner, 0:1], (HALO, LANES))
            shift = jnp.broadcast_to(columns[half, inner, at : at + 1], (HALO, LANES))
            for lane in range(groups):
                cols = slice(lane * LANES, (lane + 1) * LANES)
                values = cf[layer, origin, chunk, rows, cols].astype(jnp.float32) * rstd + shift
                values = values * gains[:, cols] + biases[:, cols]
                ag[layer, owner, chunk, rows, cols] = (values + values * jnp.tanh(values)).astype(
                    jnp.bfloat16
                )

    def own_activated(layer, half, phase):
        for chunk in range(n_a):
            activate(layer, half, 0, chunk)
            launch(f_copy(phase, ag.at[layer], 0, chunk, me, spans[layer][half]))

    def arrive(layer, half, phase, chunk):
        for step in range(1, n_y):
            owner = y_origin(step) * CORES + core
            ref = cf.at[layer, y_origin(step), chunk, rows_of(spans[layer][half])]
            y_copy(phase, ref, step, chunk).wait_recv()
            activate(layer, half, step, chunk)
            launch(f_copy(phase, ag.at[layer], step, chunk, owner, spans[layer][half]))

    def from_next_door(layer, half, phase):
        rows = rows_of(spans[layer][half])
        wait_bytes(ag.at[layer, sibling, :, rows], own_recv.at[phase])

    def from_sibling(layer, half, phase, chunk, step):
        owner = y_origin(step) * CORES + 1 - core
        f_copy(phase, ag.at[layer], step, chunk, owner, spans[layer][half]).wait_recv()

    def mix(layer, half, parts, first=False, last=False):
        rows = slice(*spans[layer][half])
        if not first:
            total = acco[rows, :]
        elif layer == 0:
            total = x_in[rows, pl.ds(pl.multiple_of(me * feats, LANES), feats)].astype(jnp.float32)
        else:
            total = res[rows, :]
        for owner, chunk in parts:
            start = pl.multiple_of(owner * chans + chunk * CHUNK, LANES)
            total = total + dot_nt(
                ag[layer, owner, chunk, rows, :], wo[layer, :, pl.ds(start, CHUNK)]
            )
        if last:
            out_ref[rows, :] = total.astype(jnp.bfloat16)
        else:
            acco[rows, :] = total

    everything = range(n_a)
    others = range(1, n_y)

    def own(chunks):
        return [(me, chunk) for chunk in chunks]

    def next_door(chunks):
        return [(sibling, chunk) for chunk in chunks]

    def across(chunks):
        return [(y_origin(step) * CORES + core, chunk) for step in others for chunk in chunks]

    def relayed(chunks):
        return [(y_origin(step) * CORES + 1 - core, chunk) for step in others for chunk in chunks]

    def branch_start(layer, half, phase):
        own_activated(layer, half, phase)
        for chunk in everything[:-1]:
            arrive(layer, half, phase, chunk)
        mix(layer, half, own(everything) + across(everything[:-1]), True)

    def branch_end(layer, half, phase, early=False):
        parts = next_door(everything)
        if not early:
            from_next_door(layer, half, phase)
            mix(layer, half, parts)
            parts = []
        arrive(layer, half, phase, n_a - 1)
        if early:
            from_next_door(layer, half, phase)
        for step in others:
            for chunk in everything[:-1]:
                from_sibling(layer, half, phase, chunk, step)
        mix(layer, half, parts + across(everything[-1:]) + relayed(everything[:-1]))
        for step in others:
            from_sibling(layer, half, phase, n_a - 1, step)

    def sent_branch(layer, half, phase):
        rows = rows_of(spans[layer][half])
        wait_bytes(ag.at[layer, pl.ds(0, 2 * n_y - 1), :, rows], sent.at[phase])
        wait_bytes(stats_of(layer, half), stat_sent.at[layer * 2 + half])

    def sent_stream(half):
        rows = rows_of(spans[0][half])
        wait_bytes(sg.at[pl.ds(0, 2 * n_y - 1), :, rows], sent.at[2 + half])
        wait_bytes(squares_of(half), square_sent.at[half])

    def square_copy(half, step, owner, target):
        ref = square.at[half, owner, :, columns_of(spans[0][half])]
        return remote(ref, ref, square_sent.at[half], square_recv.at[half], target)

    def send_stream(half):
        span = spans[0][half]
        rows = slice(*span)
        squares = jnp.zeros((span[1] - span[0], LANES), jnp.float32)
        for lead in ((0, 1), (1, n_f)):
            block = slice(lead[0] * CHUNK, lead[1] * CHUNK)
            total = acco[rows, block]
            for owner, last in relayed(everything[-1:]):
                start = pl.multiple_of(owner * chans + last * CHUNK, LANES)
                total = total + dot_nt(
                    ag[0, owner, last, rows, :], wo[0, block, pl.ds(start, CHUNK)]
                )
            rounded = total.astype(jnp.bfloat16).astype(jnp.float32)
            res[rows, block] = rounded
            for chunk in range(*lead):
                first = pl.multiple_of(me * feats + chunk * CHUNK, LANES)
                at = (chunk - lead[0]) * CHUNK
                values = rounded[:, at : at + CHUNK]
                sg[me, chunk, rows, :] = (values * gain_ref[1:2, pl.ds(first, CHUNK)]).astype(
                    jnp.bfloat16
                )
                for lane in range(groups):
                    part = values[:, lane * LANES : (lane + 1) * LANES]
                    squares = squares + part * part
                if chunk == n_f - 1:
                    send_squares(half, squares)
                ref = sg.at[me, chunk, rows_of(span)]
                for step in others:
                    launch(y_copy(2 + half, ref, step, chunk))
                launch(f_copy(2 + half, sg, 0, chunk, me, span))

    def send_squares(half, squares):
        span = spans[0][half]
        count = span[1] - span[0]
        if count < padded:
            fill = jnp.zeros((padded - count, LANES), jnp.float32)
            squares = jnp.concatenate((squares, fill), axis=0)
        row = jnp.sum(jnp.transpose(squares), axis=0, keepdims=True)
        square[half, me] = row
        for step in range(1, n_tp):
            launch(square_copy(half, step, me, lax.rem(me + step, n_tp)))

    def rescale(half):
        wait_bytes(squares_of(half), square_recv.at[half])
        totals = jnp.sum(square[half], axis=0) / width
        start, stop = spans[0][half]
        spread = jnp.transpose(
            jnp.broadcast_to(0.5 * lax.rsqrt(totals + epsilon), (LANES, padded))
        )
        scale[start:stop, :] = spread[: stop - start]

    def project(half, owner, chunks, first, blocks=None):
        rows = slice(*spans[0][half])
        for block in range(n_a) if blocks is None else blocks:
            total = None if first else accp[rows, held(block)]
            for chunk in chunks:
                start = pl.multiple_of(owner * feats + chunk * CHUNK, LANES)
                product = dot_nt(
                    sg[owner, chunk, rows, :], wp[1, block, :, pl.ds(start, CHUNK)]
                )
                total = product if total is None else total + product
            accp[rows, held(block)] = total

    def own_stream(half):
        project(half, me, range(n_f), True)

    def sibling_stream(half):
        wait_bytes(sg.at[sibling, :, rows_of(spans[0][half])], own_recv.at[2 + half])
        project(half, sibling, range(n_f), False)

    def arrive_stream(half, chunk):
        for step in range(1, n_y):
            origin = y_origin(step)
            owner = origin * CORES + core
            ref = sg.at[owner, chunk, rows_of(spans[0][half])]
            y_copy(2 + half, ref, step, chunk).wait_recv()
            launch(f_copy(2 + half, sg, step, chunk, owner, spans[0][half]))
            project(half, owner, (chunk,), False)

    def relayed_stream(half, chunk, blocks=None):
        for step in others:
            owner = y_origin(step) * CORES + 1 - core
            if blocks is None or blocks[0] == 0:
                f_copy(2 + half, sg, step, chunk, owner, spans[0][half]).wait_recv()
            project(half, owner, (chunk,), False, blocks)

    smalls[0].wait()
    x_copy(0).wait()
    prepare(0)
    for index in range(PIECES):
        cols = slice(index * piece, (index + 1) * piece)
        for copy in proj_copies(0, 0, index):
            copy.wait()
        if index < PIECES - 1:
            x_copy(index + 1).wait()
        if index == PIECES // 2:
            for chunk in range(1, n_a):
                for copy in proj_copies(0, chunk):
                    copy.start()
            out_copy(0).start()
        product = dot_nt(xg[:, cols], wp[0, 0, :, cols])
        if index < PIECES - 1:
            prepare(index + 1)
        if index:
            accp[:, held(0)] += product
        else:
            accp[:, held(0)] = product

    for first_row in range(0, tokens, ROWS):
        rows = slice(first_row, first_row + ROWS)
        scaling = lax.rsqrt(jnp.sum(norm_squares[rows, :], axis=1, keepdims=True) / width + epsilon)
        scale[rows, :] = jnp.broadcast_to(0.5 * scaling, (ROWS, LANES))

    for copy in smalls[1:]:
        copy.wait()
    pl.semaphore_wait(
        barrier,
        n_tp - 1 + jnp.where(sp > 0, 1, 0) + jnp.where(sp < n_sp - 1, 1, 0),
    )

    for chunk in everything:
        if chunk:
            for copy in proj_copies(0, chunk):
                copy.wait()
            accp[:, held(chunk)] = dot_nt(xg[...], wp[0, chunk])
        send_halo(0, chunk)
        gate_rows(chunk, 0, tokens - HALO)
        convolve(0, 0, chunk, *spans[0][0])
        centre(0, 0, chunk)
        if chunk == n_a - 1:
            send_stats(0, 0)
        send_centred(0, 0, 0, chunk)
        if chunk == 0:
            for step in others:
                launch(chan_copy(step, my_y))
    for chunk in everything:
        convolve(0, 1, chunk, ROWS, spans[0][1][1])
        receive_halo(0, chunk)
        convolve(0, 1, chunk, 0, ROWS)
        centre(0, 1, chunk)
        if chunk == n_a - 1:
            send_stats(0, 1)
        send_centred(0, 1, 1, chunk)
    for chunk in everything:
        for copy in proj_copies(1, chunk):
            copy.start()
    out_copy(1).start()
    for step in others:
        chan_copy(step, y_origin(step)).wait_recv()
    out_copy(0).wait()
    settle(0, 0)
    branch_start(0, 0, 0)
    branch_end(0, 0, 0)
    send_stream(0)
    settle(0, 1)
    branch_start(0, 1, 1)
    branch_end(0, 1, 1)
    send_stream(1)
    part[...] = jnp.zeros(part.shape, jnp.float32)
    for chunk in everything:
        for copy in proj_copies(1, chunk):
            copy.wait()
    own_stream(0)
    sibling_stream(0)
    for chunk in range(n_f):
        if chunk == 1:
            own_stream(1)
        if chunk == 2:
            sibling_stream(1)
        if chunk == n_f - 1:
            sent_branch(0, 0, 0)
            sent_branch(0, 1, 1)
            rescale(0)
        arrive_stream(0, chunk)
        if chunk:
            relayed_stream(0, chunk - 1)
    for chunk in everything:
        relayed_stream(0, n_f - 1, (chunk,))
        send_halo(1, chunk)
        gate_rows(chunk, split, tokens - HALO)
        convolve(1, 0, chunk, *spans[1][0])
        centre(1, 0, chunk)
    send_stats(1, 0)
    for chunk in everything:
        send_centred(1, 0, 4, chunk)
    for chunk in range(n_f):
        if chunk == n_f - 1:
            rescale(1)
        arrive_stream(1, chunk)
        if chunk:
            relayed_stream(1, chunk - 1)
    for chunk in everything:
        relayed_stream(1, n_f - 1, (chunk,))
        gate_rows(chunk, 0, split)
        convolve(1, 1, chunk, HALO, spans[1][1][1])
        receive_halo(1, chunk)
        convolve(1, 1, chunk, 0, HALO)
        centre(1, 1, chunk)
        if chunk == n_a - 1:
            send_stats(1, 1)
        send_centred(1, 1, 5, chunk)
    out_copy(1).wait()
    settle(1, 0)
    own_activated(1, 0, 4)
    for chunk in everything:
        arrive(1, 0, 4, chunk)
    mix(1, 0, own(everything) + across(everything), True)
    from_next_door(1, 0, 4)
    for chunk in everything:
        for step in others:
            from_sibling(1, 0, 4, chunk, step)
    mix(1, 0, next_door(everything) + relayed(everything), False, True)
    sent_stream(0)
    sent_stream(1)
    settle(1, 1)
    branch_start(1, 1, 5)
    sent_branch(1, 0, 4)
    branch_end(1, 1, 5, True)
    mix(1, 1, relayed(everything[-1:]), False, True)

    @pl.when(sp < n_sp - 1)
    def _():
        for layer in range(LAYERS):
            wait_bytes(halo_out.at[layer], halo_sent.at[layer])

    sent_branch(1, 1, 5)
    for step in others:
        wait_bytes(chan.at[my_y], chan_sent.at[step - 1])


def fused(mesh, stream, norm_gain, value_weight, gate_weight, conv_kernel, conv_bias,
          channel_gain, channel_bias, out_weight):
    n_tp, n_sp = mesh.shape["tp"], mesh.shape["sp"]
    width, tokens = stream.shape
    chans, feats = value_weight.shape[1], out_weight.shape[1]
    split = (tokens // 2 - HALO) // HALO * HALO
    n_y = n_tp // CORES
    n_a, n_f = chans // CHUNK, feats // CHUNK
    fits = (
        n_tp % CORES == 0
        and chans % CHUNK == 0
        and feats % CHUNK == 0
        and width % (PIECES * CHUNK) == 0
        and tokens % ROWS == 0
        and split % ROWS == 0
        and tokens >= 4 * ROWS
        and LAYERS == 2
        and n_tp <= 8
        and 2 * n_a <= SUBLANES
        and 1 + n_y * n_a <= LANES
    )
    if not fits:
        return local(stream, norm_gain, value_weight, gate_weight, conv_kernel, conv_bias,
                     channel_gain, channel_bias, out_weight)
    padded = -(-(tokens - split) // LANES) * LANES
    f32, bf16 = jnp.float32, jnp.bfloat16
    dma = pltpu.SemaphoreType.DMA
    out = pl.pallas_call(
        functools.partial(kernel, n_tp, n_sp, split),
        out_shape=jax.ShapeDtypeStruct((tokens, feats), bf16),
        in_specs=[pl.BlockSpec(memory_space=pl.ANY)] * 9,
        out_specs=pl.BlockSpec(memory_space=pltpu.VMEM),
        scratch_shapes=[
            pltpu.VMEM((LAYERS, width), f32),
            pltpu.VMEM((K, LAYERS, chans), f32),
            pltpu.VMEM((LAYERS, chans), f32),
            pltpu.VMEM((n_y, 2, LAYERS, chans), f32),
            pltpu.VMEM((LAYERS, n_a, 2 * CHUNK, width), bf16),
            pltpu.VMEM((LAYERS, feats, chans * n_tp), bf16),
            pltpu.VMEM((tokens, width), bf16),
            pltpu.VMEM((tokens, width), bf16),
            pltpu.VMEM((chans // LANES, HALO + tokens, LANES), f32),
            pltpu.VMEM((tokens, chans), f32),
            pltpu.VMEM((tokens, LANES), f32),
            pltpu.VMEM((tokens, LANES), f32),
            pltpu.VMEM((2, n_a, 2, padded, LANES), f32),
            pltpu.VMEM((2, padded, LANES), f32),
            pltpu.VMEM((LAYERS, n_a, HALO, CHUNK), bf16),
            pltpu.VMEM((LAYERS, n_a, HALO, CHUNK), bf16),
            pltpu.VMEM((LAYERS, 2, n_tp, 4 if 2 * n_a <= 4 else SUBLANES, padded), f32),
            pltpu.VMEM((2, n_tp, 1, padded), f32),
            pltpu.VMEM((LAYERS, n_y, n_a, tokens, CHUNK), bf16),
            pltpu.VMEM((LAYERS, n_tp, n_a, tokens, CHUNK), bf16),
            pltpu.VMEM((n_tp, n_f, tokens, CHUNK), bf16),
            pltpu.VMEM((tokens, 2 * chans), f32),
            pltpu.VMEM((tokens, feats), f32),
            pltpu.VMEM((tokens, feats), f32),
            dma((5,)),
            dma((2 * PIECES,)),
            dma((LAYERS * n_a,)),
            dma((LAYERS,)),
            dma((6,)),
            dma((LAYERS * 2,)),
            dma((2,)),
            dma((n_y - 1,)),
            dma((LAYERS,)),
            dma((n_y - 1,)),
            dma((LAYERS, n_a)),
            dma((LAYERS * 2,)),
            dma((2,)),
            dma((4 * n_a + 2 * n_f, n_y - 1)),
            dma((6,)),
            dma((4 * n_a + 2 * n_f, n_y - 1)),
        ],
        compiler_params=pltpu.CompilerParams(
            collective_id=0, has_side_effects=True, vmem_limit_bytes=50 * 1024 * 1024
        ),
    )(*(
        pltpu.with_memory_space_constraint(value, pltpu.HBM)
        for value in (
            stream.T, norm_gain, jnp.transpose(conv_kernel, (2, 0, 1)), conv_bias, channel_gain,
            channel_bias, value_weight, gate_weight, out_weight,
        )
    ))
    return out.T


def solution(mesh):
    placed = (
        P(None, ("grp", "sp")),
        P(),
        P(None, "tp", None),
        P(None, "tp", None),
        P(None, "tp", None),
        P(None, "tp"),
        P(None, "tp"),
        P(None, "tp"),
        P(None, "tp", None),
    )
    return jax.shard_map(
        functools.partial(fused, mesh), mesh=mesh, in_specs=placed, out_specs=P("tp", ("grp", "sp")), check_vma=False
    )
```

```python
import functools

import jax
import jax.numpy as jnp
from jax import lax
from jax.experimental import pallas as pl
from jax.experimental.pallas import tpu as pltpu
from jax.sharding import PartitionSpec as P

K = 31
LAYERS = 2


epsilon = 1e-06


def shifted(value, axis, steps):
    count = lax.axis_size(axis)
    initial, last = (max(0, -steps), min(count, count - steps))
    return lax.ppermute(value, axis, [(source, source + steps) for source in range(initial, last)])


def depthwise(signal, kernel):
    out = lax.conv_general_dilated(
        signal[None],
        kernel[:, None, :],
        (1,),
        [(0, 0)],
        dimension_numbers=("NCW", "OIW", "NCW"),
        feature_group_count=kernel.shape[0],
        precision=lax.Precision.HIGHEST,
    )
    return out[0]


def norm_project(whole, gain, weights):
    scaling = lax.rsqrt(jnp.mean(whole * whole, axis=0, keepdims=True) + epsilon)
    normed = (whole * scaling * gain[:, None]).astype(jnp.bfloat16)
    return jnp.dot(weights, normed, preferred_element_type=jnp.float32)


def local(
    stream,
    norm_gain,
    value_weight,
    gate_weight,
    conv_kernel,
    conv_bias,
    channel_gain,
    channel_bias,
    out_weight,
):
    shard_channels = value_weight.shape[1]
    total_channels = shard_channels * lax.axis_size("tp")
    shard_features = out_weight.shape[1]
    tokens_here = stream.shape[1]
    row_start = lax.axis_index("tp") * shard_features
    whole = stream.astype(jnp.float32)
    current = lax.dynamic_slice_in_dim(whole, row_start, shard_features, 0)
    layer_out = stream
    for layer in range(LAYERS):
        both_weights = jnp.concatenate((value_weight[layer], gate_weight[layer]), axis=0)
        if layer == 0:
            projected = norm_project(whole, norm_gain[layer], both_weights)
        else:
            gathered = lax.all_gather(layer_out, "tp", axis=0, tiled=True).astype(jnp.float32)
            projected = norm_project(gathered, norm_gain[layer], both_weights)
        gated = (projected[:shard_channels] * jax.nn.sigmoid(projected[shard_channels:])).astype(
            jnp.bfloat16
        )
        earlier = shifted(gated[:, tokens_here - (K - 1) :], "sp", 1)
        extended = jnp.concatenate((earlier, gated), axis=1).astype(jnp.float32)
        filtered = depthwise(extended, conv_kernel[layer]) + conv_bias[layer][:, None]
        first_sum, square_sum = lax.psum(
            (
                jnp.sum(filtered, axis=0, keepdims=True),
                jnp.sum(filtered * filtered, axis=0, keepdims=True),
            ),
            "tp",
        )
        row_mean = first_sum / total_channels
        centred = filtered - row_mean
        spread = square_sum / total_channels - row_mean * row_mean
        activated = jax.nn.silu(
            centred * lax.rsqrt(spread + epsilon) * channel_gain[layer][:, None]
            + channel_bias[layer][:, None]
        ).astype(jnp.bfloat16)

        def accumulate(total, piece, start, weights=out_weight[layer]):
            weight_cols = lax.dynamic_slice_in_dim(weights, start, piece.shape[0], 1)
            return total + jnp.dot(weight_cols, piece, preferred_element_type=jnp.float32)

        zero_branch = jnp.zeros((shard_features, tokens_here), jnp.float32)
        branch = accumulate(
            zero_branch, lax.all_gather(activated, "tp", axis=0, tiled=True), jnp.int32(0)
        )
        layer_out = (current + branch).astype(jnp.bfloat16)
        current = layer_out.astype(jnp.float32)
    return layer_out


MESH = pl.DeviceIdType.MESH
LANES = 128
SUBLANES = 8
CHUNK = 256
HALO = 32
ROWS = 64
CORES = 2
PIECES = 4


def dot_nt(left, right):
    return lax.dot_general(
        left, right, (((1,), (1,)), ((), ())), preferred_element_type=jnp.float32
    )


def kernel(
    n_tp,
    n_sp,
    split,
    x_hbm,
    gain_hbm,
    taps_hbm,
    bias_hbm,
    chan_gain_hbm,
    chan_bias_hbm,
    wv_ref,
    wg_ref,
    ow_ref,
    out_ref,
    gain_ref,
    taps,
    bias_ref,
    chan,
    wp,
    wo,
    x_in,
    xg,
    ext,
    filt,
    norm_squares,
    scale,
    part,
    columns,
    halo_out,
    halo_in,
    stat,
    square,
    cf,
    ag,
    sg,
    accp,
    acco,
    res,
    small_sem,
    x_sem,
    wp_sem,
    wo_sem,
    sent,
    stat_sent,
    square_sent,
    chan_sent,
    halo_sent,
    chan_recv,
    halo_recv,
    stat_recv,
    square_recv,
    y_recv,
    own_recv,
    f_recv,
):
    tokens, width = x_in.shape
    chans = wv_ref.shape[1]
    feats = ow_ref.shape[1]
    total_chans = chans * n_tp
    n_y = n_tp // CORES
    piece = width // PIECES
    padded = stat.shape[-1]
    stat_rows = stat.shape[-2]
    n_a, n_f = chans // CHUNK, feats // CHUNK
    groups = CHUNK // LANES
    spans = (
        ((split, tokens), (0, split)),
        ((split + HALO, tokens), (0, split + HALO)),
    )
    me = lax.axis_index("tp")
    sp = lax.axis_index("sp")
    my_y, core = me // CORES, me % CORES
    sibling = my_y * CORES + (1 - core)

    def tp_id(index):
        return {"tp": index}

    smalls = [
        pltpu.make_async_copy(source, target, small_sem.at[index])
        for index, (source, target) in enumerate((
            (gain_hbm, gain_ref),
            (taps_hbm, taps),
            (bias_hbm, bias_ref),
            (chan_gain_hbm, chan.at[my_y, 0]),
            (chan_bias_hbm, chan.at[my_y, 1]),
        ))
    ]

    def x_copy(index):
        cols = pl.ds(index * piece, piece)
        return pltpu.make_async_copy(x_hbm.at[:, cols], x_in.at[:, cols], x_sem.at[index])

    def proj_copies(layer, chunk, index=None):
        rows = pl.ds(chunk * CHUNK, CHUNK)
        cols = slice(None) if index is None else pl.ds(index * piece, piece)
        return [
            pltpu.make_async_copy(
                ref.at[layer, rows, cols],
                wp.at[layer, chunk, pl.ds(half * CHUNK, CHUNK), cols],
                wp_sem.at[layer * n_a + chunk] if index is None else x_sem.at[PIECES + index],
            )
            for half, ref in enumerate((wv_ref, wg_ref))
        ]

    def out_copy(layer):
        return pltpu.make_async_copy(ow_ref.at[layer], wo.at[layer], wo_sem.at[layer])

    smalls[0].start()
    for index in range(PIECES):
        x_copy(index).start()
        for copy in proj_copies(0, 0, index):
            copy.start()
    for copy in smalls[1:]:
        copy.start()

    barrier = pltpu.get_barrier_semaphore()
    for step in range(1, n_tp):
        pl.semaphore_signal(
            barrier, inc=1, device_id=tp_id(lax.rem(me + step, n_tp)), device_id_type=MESH
        )

    @pl.when(sp > 0)
    def _():
        pl.semaphore_signal(barrier, inc=1, device_id={"sp": sp - 1}, device_id_type=MESH)

    @pl.when(sp < n_sp - 1)
    def _():
        pl.semaphore_signal(barrier, inc=1, device_id={"sp": sp + 1}, device_id_type=MESH)

    part[...] = jnp.zeros(part.shape, jnp.float32)
    columns[...] = jnp.zeros(columns.shape, jnp.float32)

    def remote(source, target, send, recv, device):
        return pltpu.make_async_remote_copy(
            src_ref=source,
            dst_ref=target,
            send_sem=send,
            recv_sem=recv,
            device_id=tp_id(device),
            device_id_type=MESH,
        )

    def launch(copy):
        copy.start()

    def wait_bytes(ref, semaphore):
        pltpu.make_async_copy(ref, ref, semaphore).wait()

    def rows_of(span):
        return pl.ds(span[0], span[1] - span[0])

    def columns_of(span):
        return pl.ds(0, -(-(span[1] - span[0]) // LANES) * LANES)

    def stats_of(layer, half):
        return stat.at[layer, half, pl.ds(0, n_tp - 1), :, columns_of(spans[layer][half])]

    def squares_of(half):
        return square.at[half, pl.ds(0, n_tp - 1), :, columns_of(spans[0][half])]

    def y_peer(step):
        return lax.rem(my_y + step, n_y)

    def y_origin(step):
        return lax.rem(my_y + n_y - step, n_y)

    def slot(phase, chunk):
        return phase * n_a + max(0, min(phase, 4) - 2) * (n_f - n_a) + chunk

    def y_copy(phase, ref, step, chunk):
        target = y_peer(step) * CORES + core
        return remote(
            ref, ref, sent.at[phase], y_recv.at[slot(phase, chunk), step - 1], target
        )

    def f_copy(phase, buf, step, chunk, owner, span):
        ref = buf.at[owner, chunk, rows_of(span)]
        if step == 0:
            return remote(ref, ref, sent.at[phase], own_recv.at[phase], sibling)
        index = slot(phase, chunk)
        return remote(
            ref, ref, sent.at[phase], f_recv.at[index, step - 1], sibling
        )

    def chan_copy(step, slot):
        target = y_peer(step) * CORES + core
        return remote(chan.at[slot], chan.at[slot], chan_sent.at[step - 1], chan_recv.at[step - 1], target)

    def prepare(index):
        gains = gain_ref[0:1, index * piece : (index + 1) * piece]
        for first_row in range(0, tokens, ROWS):
            rows = slice(first_row, first_row + ROWS)
            squares = norm_squares[rows, :] if index else None
            for lane in range(piece // LANES):
                here = slice(index * piece + lane * LANES, index * piece + (lane + 1) * LANES)
                values = x_in[rows, here].astype(jnp.float32)
                squares = values * values if squares is None else squares + values * values
                xg[rows, here] = (values * gains[:, lane * LANES : (lane + 1) * LANES]).astype(
                    jnp.bfloat16
                )
            norm_squares[rows, :] = squares

    def held(chunk):
        return slice(chunk * 2 * CHUNK, (chunk + 1) * 2 * CHUNK)

    def gate(chunk, first_row, count):
        rows = pl.ds(first_row, count)
        halved = scale[rows, :]
        start = chunk * 2 * CHUNK
        pieces = []
        for lane in range(groups):
            at = start + lane * LANES
            value = accp[rows, at : at + LANES] * halved
            gates = accp[rows, at + CHUNK : at + CHUNK + LANES] * halved
            gated = (value + value * jnp.tanh(gates)).astype(jnp.bfloat16)
            ext[chunk * groups + lane, pl.ds(first_row + HALO, count), :] = gated.astype(
                jnp.float32
            )
            pieces.append(gated)
        return pieces

    def gate_rows(chunk, start, stop):
        for first_row in range(start, stop, HALO):
            gate(chunk, first_row, HALO)

    def halo_copy(layer, chunk):
        return pltpu.make_async_remote_copy(
            src_ref=halo_out.at[layer, chunk],
            dst_ref=halo_in.at[layer, chunk],
            send_sem=halo_sent.at[layer],
            recv_sem=halo_recv.at[layer, chunk],
            device_id={"sp": lax.rem(sp + 1, n_sp)},
            device_id_type=MESH,
        )

    def send_halo(layer, chunk):
        for lane, gated in enumerate(gate(chunk, tokens - HALO, HALO)):
            halo_out[layer, chunk, :, lane * LANES : (lane + 1) * LANES] = gated

        @pl.when(sp < n_sp - 1)
        def _():
            halo_copy(layer, chunk).start()

    def receive_halo(layer, chunk):
        @pl.when(sp > 0)
        def _():
            halo_copy(layer, chunk).wait_recv()
            for lane in range(groups):
                ext[chunk * groups + lane, :HALO, :] = halo_in[
                    layer, chunk, :, lane * LANES : (lane + 1) * LANES
                ].astype(jnp.float32)

        @pl.when(sp == 0)
        def _():
            for lane in range(groups):
                ext[chunk * groups + lane, :HALO, :] = jnp.zeros((HALO, LANES), jnp.float32)

    def convolve(layer, half, chunk, start, stop):
        base = spans[layer][half][0]
        blocks = []
        while start < stop:
            count = min(ROWS, stop - start)
            blocks.append((start, count))
            start += count

        @pl.loop(chunk * groups, (chunk + 1) * groups)
        def _(lane):
            here = pl.ds(pl.multiple_of(lane * LANES, LANES), LANES)
            bias = bias_ref[layer : layer + 1, here]
            for first_row, count in blocks:
                tiles = count // SUBLANES
                sums = [jnp.broadcast_to(bias, (SUBLANES, LANES))] * tiles
                for residue in range(SUBLANES):
                    begin = first_row + HALO - K + 1 + residue
                    held_taps = range(residue, K, SUBLANES)
                    weights = [taps[tap, layer : layer + 1, here] for tap in held_taps]
                    for index in range(tiles + len(weights) - 1):
                        at = begin + index * SUBLANES
                        window = ext[lane, at : at + SUBLANES, :]
                        for step, weight in enumerate(weights):
                            tile = index - step
                            if 0 <= tile < tiles:
                                sums[tile] = sums[tile] + window * weight
                total = jnp.concatenate(sums, axis=0)
                filt[first_row : first_row + count, here] = total
                inner = slice(first_row - base, first_row - base + count)
                part[half, chunk, 0, inner, :] += total
                part[half, chunk, 1, inner, :] += total * total

    lane_index = lax.broadcasted_iota(jnp.int32, (HALO, LANES), 1)

    def centre(layer, half, chunk):
        start, stop = spans[layer][half]

        for block in range((stop - start) // HALO):
            inner = slice(block * HALO, (block + 1) * HALO)
            rows = slice(start + block * HALO, start + (block + 1) * HALO)
            mean = jnp.sum(part[half, chunk, 0, inner, :], axis=1, keepdims=True) / CHUNK
            squares = jnp.sum(part[half, chunk, 1, inner, :], axis=1, keepdims=True)
            for lane in range(groups):
                at = chunk * CHUNK + lane * LANES
                cf[layer, my_y, chunk, rows, lane * LANES : (lane + 1) * LANES] = (
                    filt[rows, at : at + LANES] - mean
                ).astype(jnp.bfloat16)
            packed = jnp.where(
                lane_index == chunk, mean, jnp.where(lane_index == n_a + chunk, squares, 0.0)
            )
            if chunk:
                packed = packed + columns[half, inner, :]
            columns[half, inner, :] = packed

    def send_centred(layer, half, phase, chunk):
        ref = cf.at[layer, my_y, chunk, rows_of(spans[layer][half])]
        for step in range(1, n_y):
            launch(y_copy(phase, ref, step, chunk))

    def stat_copy(layer, half, step, owner, target):
        ref = stat.at[layer, half, owner, :, columns_of(spans[layer][half])]
        index = layer * 2 + half
        return remote(ref, ref, stat_sent.at[index], stat_recv.at[index], target)

    def send_stats(layer, half):
        stat[layer, half, me] = jnp.transpose(columns[half])[:stat_rows]
        for step in range(1, n_tp):
            launch(stat_copy(layer, half, step, me, lax.rem(me + step, n_tp)))

    def to_columns(rows):
        fill = jnp.zeros((LANES - rows.shape[0], padded), jnp.float32)
        return jnp.transpose(jnp.concatenate((rows, fill), axis=0))

    def settle(layer, half):
        wait_bytes(stats_of(layer, half), stat_recv.at[layer * 2 + half])
        totals = jnp.sum(stat[layer, half], axis=0)
        mean_row = jnp.sum(totals[:n_a], axis=0, keepdims=True) * CHUNK / total_chans
        square_row = jnp.sum(totals[n_a : 2 * n_a], axis=0, keepdims=True) / total_chans
        rstd_row = lax.rsqrt(square_row - mean_row * mean_row + epsilon)
        rows = [rstd_row]
        for step in range(n_y):
            means = stat[layer, half, y_origin(step) * CORES + core]
            rows.append((means[:n_a] - mean_row) * rstd_row)
        columns[half] = to_columns(jnp.concatenate(rows, axis=0))

    def activate(layer, half, step, chunk):
        start, stop = spans[layer][half]
        origin = y_origin(step)
        owner = origin * CORES + core

        at = 1 + step * n_a + chunk
        gains = 0.5 * chan[origin, 0, layer : layer + 1, chunk * CHUNK : (chunk + 1) * CHUNK]
        biases = 0.5 * chan[origin, 1, layer : layer + 1, chunk * CHUNK : (chunk + 1) * CHUNK]
        for block in range((stop - start) // HALO):
            inner = slice(block * HALO, (block + 1) * HALO)
            rows = slice(start + block * HALO, start + (block + 1) * HALO)
            rstd = jnp.broadcast_to(columns[half, inner, 0:1], (HALO, LANES))
            shift = jnp.broadcast_to(columns[half, inner, at : at + 1], (HALO, LANES))
            for lane in range(groups):
                cols = slice(lane * LANES, (lane + 1) * LANES)
                values = cf[layer, origin, chunk, rows, cols].astype(jnp.float32) * rstd + shift
                values = values * gains[:, cols] + biases[:, cols]
                ag[layer, owner, chunk, rows, cols] = (values + values * jnp.tanh(values)).astype(
                    jnp.bfloat16
                )

    def own_activated(layer, half, phase):
        for chunk in range(n_a):
            activate(layer, half, 0, chunk)
            launch(f_copy(phase, ag.at[layer], 0, chunk, me, spans[layer][half]))

    def arrive(layer, half, phase, chunk):
        for step in range(1, n_y):
            owner = y_origin(step) * CORES + core
            ref = cf.at[layer, y_origin(step), chunk, rows_of(spans[layer][half])]
            y_copy(phase, ref, step, chunk).wait_recv()
            activate(layer, half, step, chunk)
            launch(f_copy(phase, ag.at[layer], step, chunk, owner, spans[layer][half]))

    def from_next_door(layer, half, phase):
        rows = rows_of(spans[layer][half])
        wait_bytes(ag.at[layer, sibling, :, rows], own_recv.at[phase])

    def from_sibling(layer, half, phase, chunk, step):
        owner = y_origin(step) * CORES + 1 - core
        f_copy(phase, ag.at[layer], step, chunk, owner, spans[layer][half]).wait_recv()

    def mix(layer, half, parts, first=False, last=False):
        rows = slice(*spans[layer][half])
        if not first:
            total = acco[rows, :]
        elif layer == 0:
            total = x_in[rows, pl.ds(pl.multiple_of(me * feats, LANES), feats)].astype(jnp.float32)
        else:
            total = res[rows, :]
        for owner, chunk in parts:
            start = pl.multiple_of(owner * chans + chunk * CHUNK, LANES)
            total = total + dot_nt(
                ag[layer, owner, chunk, rows, :], wo[layer, :, pl.ds(start, CHUNK)]
            )
        if last:
            out_ref[rows, :] = total.astype(jnp.bfloat16)
        else:
            acco[rows, :] = total

    everything = range(n_a)
    others = range(1, n_y)

    def own(chunks):
        return [(me, chunk) for chunk in chunks]

    def next_door(chunks):
        return [(sibling, chunk) for chunk in chunks]

    def across(chunks):
        return [(y_origin(step) * CORES + core, chunk) for step in others for chunk in chunks]

    def relayed(chunks):
        return [(y_origin(step) * CORES + 1 - core, chunk) for step in others for chunk in chunks]

    def branch_start(layer, half, phase):
        own_activated(layer, half, phase)
        for chunk in everything[:-1]:
            arrive(layer, half, phase, chunk)
        mix(layer, half, own(everything) + across(everything[:-1]), True)

    def branch_end(layer, half, phase, early=False):
        parts = next_door(everything)
        if not early:
            from_next_door(layer, half, phase)
            mix(layer, half, parts)
            parts = []
        arrive(layer, half, phase, n_a - 1)
        if early:
            from_next_door(layer, half, phase)
        for step in others:
            for chunk in everything[:-1]:
                from_sibling(layer, half, phase, chunk, step)
        mix(layer, half, parts + across(everything[-1:]) + relayed(everything[:-1]))
        for step in others:
            from_sibling(layer, half, phase, n_a - 1, step)

    def sent_branch(layer, half, phase):
        rows = rows_of(spans[layer][half])
        wait_bytes(ag.at[layer, pl.ds(0, 2 * n_y - 1), :, rows], sent.at[phase])
        wait_bytes(stats_of(layer, half), stat_sent.at[layer * 2 + half])

    def sent_stream(half):
        rows = rows_of(spans[0][half])
        wait_bytes(sg.at[pl.ds(0, 2 * n_y - 1), :, rows], sent.at[2 + half])
        wait_bytes(squares_of(half), square_sent.at[half])

    def square_copy(half, step, owner, target):
        ref = square.at[half, owner, :, columns_of(spans[0][half])]
        return remote(ref, ref, square_sent.at[half], square_recv.at[half], target)

    def send_stream(half):
        span = spans[0][half]
        rows = slice(*span)
        squares = jnp.zeros((span[1] - span[0], LANES), jnp.float32)
        for lead in ((0, 1), (1, n_f)):
            block = slice(lead[0] * CHUNK, lead[1] * CHUNK)
            total = acco[rows, block]
            for owner, last in relayed(everything[-1:]):
                start = pl.multiple_of(owner * chans + last * CHUNK, LANES)
                total = total + dot_nt(
                    ag[0, owner, last, rows, :], wo[0, block, pl.ds(start, CHUNK)]
                )
            rounded = total.astype(jnp.bfloat16).astype(jnp.float32)
            res[rows, block] = rounded
            for chunk in range(*lead):
                first = pl.multiple_of(me * feats + chunk * CHUNK, LANES)
                at = (chunk - lead[0]) * CHUNK
                values = rounded[:, at : at + CHUNK]
                sg[me, chunk, rows, :] = (values * gain_ref[1:2, pl.ds(first, CHUNK)]).astype(
                    jnp.bfloat16
                )
                for lane in range(groups):
                    part = values[:, lane * LANES : (lane + 1) * LANES]
                    squares = squares + part * part
                if chunk == n_f - 1:
                    send_squares(half, squares)
                ref = sg.at[me, chunk, rows_of(span)]
                for step in others:
                    launch(y_copy(2 + half, ref, step, chunk))
                launch(f_copy(2 + half, sg, 0, chunk, me, span))

    def send_squares(half, squares):
        span = spans[0][half]
        count = span[1] - span[0]
        if count < padded:
            fill = jnp.zeros((padded - count, LANES), jnp.float32)
            squares = jnp.concatenate((squares, fill), axis=0)
        row = jnp.sum(jnp.transpose(squares), axis=0, keepdims=True)
        square[half, me] = row
        for step in range(1, n_tp):
            launch(square_copy(half, step, me, lax.rem(me + step, n_tp)))

    def rescale(half):
        wait_bytes(squares_of(half), square_recv.at[half])
        totals = jnp.sum(square[half], axis=0) / width
        start, stop = spans[0][half]
        spread = jnp.transpose(
            jnp.broadcast_to(0.5 * lax.rsqrt(totals + epsilon), (LANES, padded))
        )
        scale[start:stop, :] = spread[: stop - start]

    def project(half, owner, chunks, first, blocks=None):
        rows = slice(*spans[0][half])
        for block in range(n_a) if blocks is None else blocks:
            total = None if first else accp[rows, held(block)]
            for chunk in chunks:
                start = pl.multiple_of(owner * feats + chunk * CHUNK, LANES)
                product = dot_nt(
                    sg[owner, chunk, rows, :], wp[1, block, :, pl.ds(start, CHUNK)]
                )
                total = product if total is None else total + product
            accp[rows, held(block)] = total

    def own_stream(half):
        project(half, me, range(n_f), True)

    def sibling_stream(half):
        wait_bytes(sg.at[sibling, :, rows_of(spans[0][half])], own_recv.at[2 + half])
        project(half, sibling, range(n_f), False)

    def arrive_stream(half, chunk):
        for step in range(1, n_y):
            origin = y_origin(step)
            owner = origin * CORES + core
            ref = sg.at[owner, chunk, rows_of(spans[0][half])]
            y_copy(2 + half, ref, step, chunk).wait_recv()
            launch(f_copy(2 + half, sg, step, chunk, owner, spans[0][half]))
            project(half, owner, (chunk,), False)

    def relayed_stream(half, chunk, blocks=None):
        for step in others:
            owner = y_origin(step) * CORES + 1 - core
            if blocks is None or blocks[0] == 0:
                f_copy(2 + half, sg, step, chunk, owner, spans[0][half]).wait_recv()
            project(half, owner, (chunk,), False, blocks)

    smalls[0].wait()
    x_copy(0).wait()
    prepare(0)
    for index in range(PIECES):
        cols = slice(index * piece, (index + 1) * piece)
        for copy in proj_copies(0, 0, index):
            copy.wait()
        if index < PIECES - 1:
            x_copy(index + 1).wait()
        if index == PIECES // 2:
            for chunk in range(1, n_a):
                for copy in proj_copies(0, chunk):
                    copy.start()
            out_copy(0).start()
        product = dot_nt(xg[:, cols], wp[0, 0, :, cols])
        if index < PIECES - 1:
            prepare(index + 1)
        if index:
            accp[:, held(0)] += product
        else:
            accp[:, held(0)] = product

    for first_row in range(0, tokens, ROWS):
        rows = slice(first_row, first_row + ROWS)
        scaling = lax.rsqrt(jnp.sum(norm_squares[rows, :], axis=1, keepdims=True) / width + epsilon)
        scale[rows, :] = jnp.broadcast_to(0.5 * scaling, (ROWS, LANES))

    for copy in smalls[1:]:
        copy.wait()
    pl.semaphore_wait(
        barrier,
        n_tp - 1 + jnp.where(sp > 0, 1, 0) + jnp.where(sp < n_sp - 1, 1, 0),
    )

    for chunk in everything:
        if chunk:
            for copy in proj_copies(0, chunk):
                copy.wait()
            accp[:, held(chunk)] = dot_nt(xg[...], wp[0, chunk])
        send_halo(0, chunk)
        gate_rows(chunk, 0, tokens - HALO)
        convolve(0, 0, chunk, *spans[0][0])
        centre(0, 0, chunk)
        if chunk == n_a - 1:
            send_stats(0, 0)
        send_centred(0, 0, 0, chunk)
        if chunk == 0:
            for step in others:
                launch(chan_copy(step, my_y))
    for chunk in everything:
        convolve(0, 1, chunk, ROWS, spans[0][1][1])
        receive_halo(0, chunk)
        convolve(0, 1, chunk, 0, ROWS)
        centre(0, 1, chunk)
        if chunk == n_a - 1:
            send_stats(0, 1)
        send_centred(0, 1, 1, chunk)
    for chunk in everything:
        for copy in proj_copies(1, chunk):
            copy.start()
    out_copy(1).start()
    for step in others:
        chan_copy(step, y_origin(step)).wait_recv()
    out_copy(0).wait()
    settle(0, 0)
    branch_start(0, 0, 0)
    branch_end(0, 0, 0)
    send_stream(0)
    settle(0, 1)
    branch_start(0, 1, 1)
    branch_end(0, 1, 1)
    send_stream(1)
    part[...] = jnp.zeros(part.shape, jnp.float32)
    for chunk in everything:
        for copy in proj_copies(1, chunk):
            copy.wait()
    own_stream(0)
    sibling_stream(0)
    for chunk in range(n_f):
        if chunk == 1:
            own_stream(1)
        if chunk == 2:
            sibling_stream(1)
        if chunk == n_f - 1:
            sent_branch(0, 0, 0)
            sent_branch(0, 1, 1)
            rescale(0)
        arrive_stream(0, chunk)
        if chunk:
            relayed_stream(0, chunk - 1)
    for chunk in everything:
        relayed_stream(0, n_f - 1, (chunk,))
        send_halo(1, chunk)
        gate_rows(chunk, split, tokens - HALO)
        convolve(1, 0, chunk, *spans[1][0])
        centre(1, 0, chunk)
    send_stats(1, 0)
    for chunk in everything:
        send_centred(1, 0, 4, chunk)
    for chunk in range(n_f):
        if chunk == n_f - 1:
            rescale(1)
        arrive_stream(1, chunk)
        if chunk:
            relayed_stream(1, chunk - 1)
    for chunk in everything:
        relayed_stream(1, n_f - 1, (chunk,))
        gate_rows(chunk, 0, split)
        convolve(1, 1, chunk, HALO, spans[1][1][1])
        receive_halo(1, chunk)
        convolve(1, 1, chunk, 0, HALO)
        centre(1, 1, chunk)
        if chunk == n_a - 1:
            send_stats(1, 1)
        send_centred(1, 1, 5, chunk)
    out_copy(1).wait()
    settle(1, 0)
    own_activated(1, 0, 4)
    for chunk in everything:
        arrive(1, 0, 4, chunk)
    mix(1, 0, own(everything) + across(everything), True)
    from_next_door(1, 0, 4)
    for chunk in everything:
        for step in others:
            from_sibling(1, 0, 4, chunk, step)
    mix(1, 0, next_door(everything) + relayed(everything), False, True)
    sent_stream(0)
    sent_stream(1)
    settle(1, 1)
    branch_start(1, 1, 5)
    sent_branch(1, 0, 4)
    branch_end(1, 1, 5, True)
    mix(1, 1, relayed(everything[-1:]), False, True)

    @pl.when(sp < n_sp - 1)
    def _():
        for layer in range(LAYERS):
            wait_bytes(halo_out.at[layer], halo_sent.at[layer])

    sent_branch(1, 1, 5)
    for step in others:
        wait_bytes(chan.at[my_y], chan_sent.at[step - 1])


def fused(mesh, stream, norm_gain, value_weight, gate_weight, conv_kernel, conv_bias,
          channel_gain, channel_bias, out_weight):
    n_tp, n_sp = mesh.shape["tp"], mesh.shape["sp"]
    width, tokens = stream.shape
    chans, feats = value_weight.shape[1], out_weight.shape[1]
    split = (tokens // 2 - HALO) // HALO * HALO
    n_y = n_tp // CORES
    n_a, n_f = chans // CHUNK, feats // CHUNK
    fits = (
        n_tp % CORES == 0
        and chans % CHUNK == 0
        and feats % CHUNK == 0
        and width % (PIECES * CHUNK) == 0
        and tokens % ROWS == 0
        and split % ROWS == 0
        and tokens >= 4 * ROWS
        and LAYERS == 2
        and n_tp <= 8
        and 2 * n_a <= SUBLANES
        and 1 + n_y * n_a <= LANES
    )
    if not fits:
        return local(stream, norm_gain, value_weight, gate_weight, conv_kernel, conv_bias,
                     channel_gain, channel_bias, out_weight)
    padded = -(-(tokens - split) // LANES) * LANES
    f32, bf16 = jnp.float32, jnp.bfloat16
    dma = pltpu.SemaphoreType.DMA
    out = pl.pallas_call(
        functools.partial(kernel, n_tp, n_sp, split),
        out_shape=jax.ShapeDtypeStruct((tokens, feats), bf16),
        in_specs=[pl.BlockSpec(memory_space=pl.ANY)] * 9,
        out_specs=pl.BlockSpec(memory_space=pltpu.VMEM),
        scratch_shapes=[
            pltpu.VMEM((LAYERS, width), f32),
            pltpu.VMEM((K, LAYERS, chans), f32),
            pltpu.VMEM((LAYERS, chans), f32),
            pltpu.VMEM((n_y, 2, LAYERS, chans), f32),
            pltpu.VMEM((LAYERS, n_a, 2 * CHUNK, width), bf16),
            pltpu.VMEM((LAYERS, feats, chans * n_tp), bf16),
            pltpu.VMEM((tokens, width), bf16),
            pltpu.VMEM((tokens, width), bf16),
            pltpu.VMEM((chans // LANES, HALO + tokens, LANES), f32),
            pltpu.VMEM((tokens, chans), f32),
            pltpu.VMEM((tokens, LANES), f32),
            pltpu.VMEM((tokens, LANES), f32),
            pltpu.VMEM((2, n_a, 2, padded, LANES), f32),
            pltpu.VMEM((2, padded, LANES), f32),
            pltpu.VMEM((LAYERS, n_a, HALO, CHUNK), bf16),
            pltpu.VMEM((LAYERS, n_a, HALO, CHUNK), bf16),
            pltpu.VMEM((LAYERS, 2, n_tp, 4 if 2 * n_a <= 4 else SUBLANES, padded), f32),
            pltpu.VMEM((2, n_tp, 1, padded), f32),
            pltpu.VMEM((LAYERS, n_y, n_a, tokens, CHUNK), bf16),
            pltpu.VMEM((LAYERS, n_tp, n_a, tokens, CHUNK), bf16),
            pltpu.VMEM((n_tp, n_f, tokens, CHUNK), bf16),
            pltpu.VMEM((tokens, 2 * chans), f32),
            pltpu.VMEM((tokens, feats), f32),
            pltpu.VMEM((tokens, feats), f32),
            dma((5,)),
            dma((2 * PIECES,)),
            dma((LAYERS * n_a,)),
            dma((LAYERS,)),
            dma((6,)),
            dma((LAYERS * 2,)),
            dma((2,)),
            dma((n_y - 1,)),
            dma((LAYERS,)),
            dma((n_y - 1,)),
            dma((LAYERS, n_a)),
            dma((LAYERS * 2,)),
            dma((2,)),
            dma((4 * n_a + 2 * n_f, n_y - 1)),
            dma((6,)),
            dma((4 * n_a + 2 * n_f, n_y - 1)),
        ],
        compiler_params=pltpu.CompilerParams(
            collective_id=0, has_side_effects=True, vmem_limit_bytes=50 * 1024 * 1024
        ),
    )(*(
        pltpu.with_memory_space_constraint(value, pltpu.HBM)
        for value in (
            stream.T, norm_gain, jnp.transpose(conv_kernel, (2, 0, 1)), conv_bias, channel_gain,
            channel_bias, value_weight, gate_weight, out_weight,
        )
    ))
    return out.T


def solution(mesh):
    placed = (
        P(None, ("grp", "sp")),
        P(),
        P(None, "tp", None),
        P(None, "tp", None),
        P(None, "tp", None),
        P(None, "tp"),
        P(None, "tp"),
        P(None, "tp"),
        P(None, "tp", None),
    )
    return jax.shard_map(
        functools.partial(fused, mesh), mesh=mesh, in_specs=placed, out_specs=P("tp", ("grp", "sp")), check_vma=False
    )
```
